256 devices in a mesh: sp: 32 (over z, x), tp: 8 (over y, core).
Axes of the slice: x: 4, y: 4, z: 8, core: 2. Of those that a mesh axis runs over, the one named last changes fastest.
Arguments:
- tokens: bfloat16 [8192, 1024], P(('sp', 'tp')), may hold values from -6 to 6
- doc_ids: int32 [8192], P('sp'), may hold values from 0 to 31, never falling along the last dimension, each value on 1 to 4608 neighbouring positions
- down_query: bfloat16 [1024, 256], P('sp'), may hold values from -0.1875 to 0.1875
- down_key: bfloat16 [1024, 256], P('sp'), may hold values from -0.1875 to 0.1875
- down_rotary: bfloat16 [1024, 32], P('sp'), may hold values from -0.1875 to 0.1875
- query_gain: float32 [256], replicated, may hold values from 0.1 to 1.9
- key_gain: float32 [256], replicated, may hold values from 0.1 to 1.9
- up_query: bfloat16 [256, 1536], P('sp', 'tp'), may hold values from -0.375 to 0.375
- up_key: bfloat16 [256, 1024], P('sp', 'tp'), may hold values from -0.375 to 0.375
- up_value: bfloat16 [256, 1024], P('sp', 'tp'), may hold values from -0.375 to 0.375
- output_weight: bfloat16 [1024, 1024], P('tp', 'sp'), may hold values from -0.1875 to 0.1875
- out_gain: float32 [1024], replicated, may hold values from 0.1 to 1.9
Outputs:
- mixed: bfloat16 [8192, 1024], P(('sp', 'tp'))
- log_sums: float32 [8192, 16], P('sp', 'tp')
The draws below stay inside these ranges and needn't reach their ends.
Inputs may be any that keep to these rules, and one draw needn't show every extreme that they name: doc_ids never fall along the sequence and run from 0 to at most the number of devices along sp minus one; each document has 1 to 4608 positions, and one document has exactly that many.
All inputs are finite; a program needn't handle non-finite values.
Results may differ from the reference program's by a relative error of at most 0.02.
Values may be sent and summed in bfloat16 or wider, within the bound.
A program may use at most 64 MiB of HBM per device.

```python
import math
import jax
import jax.numpy as jnp
import numpy as np
from jax import lax

D = 1024
HEADS = 16
Q_RANK = 256
KV_RANK = 256
NOPE = 64
ROPE = 32
VDIM = 64
TOK_DEV = 256
TOKENS = 8192
N_SP = 32


def block_scale(key, extent, pieces, least, high):
    def one(position, shards_of):
        draws = jax.random.uniform(jax.random.fold_in(jax.random.fold_in(key, 6), position), (shards_of,), jnp.float32, least / len(pieces), high / len(pieces))
        return jnp.repeat(jnp.exp(draws), extent[position] // shards_of).reshape((-1,) + (1,) * (len(extent) - position - 1))

    level = one(*pieces[0])
    for cut in pieces[1:]:
        level = level * one(*cut)
    return level


def profile(number_of, total, bound, skew):
    portions = [(1 << 20) // math.isqrt(standing ** skew) + 1 for standing in range(2, number_of + 1)]
    rest, given = total - bound - (number_of - 1), [1] * (number_of - 1)
    while rest > 0:
        movable = [i for i in range(number_of - 1) if given[i] < bound]
        pool, budget = sum([portions[i] for i in movable]), rest
        for i in movable:
            more = min(bound - given[i], max(1, budget * portions[i] // pool), rest)
            given[i] = given[i] + more
            rest = rest - more
    return np.array([bound] + given)


def uneven_parts(key, count, total, bound, lean):
    if count == 2:
        one = jax.random.randint(key, (), max(1, total - bound), min(bound, total - 1) + 1)
        return jnp.stack([one, total - one])
    lengths = jnp.asarray(profile(count, total, bound, lean), jnp.int32)
    twos = (count - 1) // 2
    source_of, sink = lengths[1:1 + 2 * twos:2], lengths[2:2 + 2 * twos:2]
    room = jnp.minimum(source_of - 1, bound - sink)
    moved = jax.random.randint(jax.random.fold_in(key, 1), (twos,), 0, 1 << 20) % (room + 1)
    lengths = lengths.at[1:1 + 2 * twos:2].set(source_of - moved).at[2:2 + 2 * twos:2].set(sink + moved)
    return lengths[jax.random.permutation(jax.random.fold_in(key, 2), count)]


def normal_values(own_key, shape, width, bound, split=(), kind=jnp.bfloat16):
    values = width * jax.random.normal(own_key, shape, jnp.float32)
    if split:
        values = values * block_scale(own_key, shape, split, -0.22, 0.18)
    return jnp.clip(values, -bound, bound).astype(kind)


def setup_inputs(seed: int = 0) -> dict:
    seeds = jax.random.split(jax.random.key(seed), 13)
    return {
        "tokens": normal_values(seeds[0], (TOKENS, D), 1.0, 6.0, ((0, 256),)),
        "doc_ids": jnp.searchsorted(jnp.cumsum(uneven_parts(seeds[1], N_SP, TOKENS, TOK_DEV * N_SP // 2 + 2 * TOK_DEV, 2)), jnp.arange(TOKENS), side="right").astype(jnp.int32),
        "down_query": normal_values(seeds[2], (D, Q_RANK), D ** -0.5, 0.1875, ((0, 32),)),
        "down_key": normal_values(seeds[3], (D, KV_RANK), D ** -0.5, 0.1875, ((0, 32),)),
        "down_rotary": normal_values(seeds[4], (D, ROPE), D ** -0.5, 0.1875, ((0, 32),)),
        "query_gain": jnp.clip(1.0 + 0.18 * jax.random.normal(seeds[5], (Q_RANK,), jnp.float32), 0.1, 1.9),
        "key_gain": jnp.clip(1.0 + 0.18 * jax.random.normal(seeds[6], (KV_RANK,), jnp.float32), 0.1, 1.9),
        "up_query": normal_values(seeds[7], (Q_RANK, HEADS * (NOPE + ROPE)), Q_RANK ** -0.5, 0.375, ((0, 32), (1, 8))),
        "up_key": normal_values(seeds[8], (KV_RANK, HEADS * NOPE), KV_RANK ** -0.5, 0.375, ((0, 32), (1, 8))),
        "up_value": normal_values(seeds[9], (KV_RANK, HEADS * VDIM), KV_RANK ** -0.5, 0.375, ((0, 32), (1, 8))),
        "output_weight": normal_values(seeds[10], (HEADS * VDIM, D), (HEADS * VDIM) ** -0.5, 0.1875, ((0, 8), (1, 32))),
        "out_gain": jnp.clip(1.0 + 0.18 * jax.random.normal(seeds[11], (D,), jnp.float32), 0.1, 1.9),
    }


NEG_BIG = -1e+30
THETA = 10000.0
EPS = 1e-06

def settle(quantity):
    return lax.optimization_barrier(quantity.astype(jnp.bfloat16))

def rms_gain(summed, gain_vector):
    widened = settle(summed).astype(jnp.float32)
    scaled = widened * lax.rsqrt(lax.optimization_barrier(jnp.mean(widened * widened, axis=-1, keepdims=True)) + EPS)
    return (scaled * gain_vector).astype(jnp.bfloat16)

def rotate(vectors, positions):
    half_width = vectors.shape[-1] // 2
    inverse = THETA ** (-jnp.arange(half_width, dtype=jnp.float32) / half_width)
    angles = positions.astype(jnp.float32)[:, None] * inverse[None, :]
    angles = angles.reshape((vectors.shape[0],) + (1,) * (vectors.ndim - 2) + (half_width,))
    cosine_part = jnp.cos(angles)
    sine_part = jnp.sin(angles)
    widened = vectors.astype(jnp.float32)
    front_half = widened[..., :half_width]
    back_half = widened[..., half_width:]
    return jnp.concatenate([front_half * cosine_part - back_half * sine_part, back_half * cosine_part + front_half * sine_part], axis=-1).astype(jnp.bfloat16)

def reference(tokens, doc_ids, down_query, down_key, down_rotary, query_gain, key_gain, up_query, up_key, up_value, output_weight, out_gain):
    highest = lax.Precision.HIGHEST
    positions = jnp.arange(TOKENS, dtype=jnp.int32)
    query_latent = rms_gain(jnp.dot(tokens, down_query, preferred_element_type=jnp.float32), query_gain)
    key_latent = rms_gain(jnp.dot(tokens, down_key, preferred_element_type=jnp.float32), key_gain)
    key_turned = rotate(settle(jnp.dot(tokens, down_rotary, preferred_element_type=jnp.float32)), positions)
    queries = settle(jnp.dot(query_latent, up_query, preferred_element_type=jnp.float32))
    queries = queries.reshape(TOKENS, HEADS, NOPE + ROPE)
    query_plain = queries[..., :NOPE]
    query_turned = rotate(queries[..., NOPE:], positions)
    key_plain = settle(jnp.dot(key_latent, up_key, preferred_element_type=jnp.float32)).reshape(TOKENS, HEADS, NOPE)
    values = settle(jnp.dot(key_latent, up_value, preferred_element_type=jnp.float32)).reshape(TOKENS, HEADS, VDIM)
    score_scale = 1.0 / math.sqrt(NOPE + ROPE)
    plain_wide = key_plain.astype(jnp.float32)
    turned_wide = key_turned.astype(jnp.float32)
    values_wide = values.astype(jnp.float32)

    def one_block(block_parts):
        plain_block, turned_block, docs_block = block_parts
        scores = jnp.einsum('qhd,khd->hqk', plain_block.astype(jnp.float32), plain_wide, precision=highest)
        scores = scores + jnp.einsum('qhr,kr->hqk', turned_block.astype(jnp.float32), turned_wide, precision=highest)
        scores = scores * score_scale
        same_doc = (docs_block[:, None] == doc_ids[None, :])[None]
        top_score = lax.optimization_barrier(jnp.max(jnp.where(same_doc, scores, NEG_BIG), axis=-1, keepdims=True))
        weights = jnp.where(same_doc, jnp.exp(scores - top_score), 0.0)
        weight_sum = lax.optimization_barrier(jnp.sum(weights, axis=-1))
        mixed_rows = jnp.einsum('hqk,khv->qhv', settle(weights).astype(jnp.float32), values_wide, precision=highest)
        mixed_rows = mixed_rows / weight_sum.T[:, :, None]
        return (mixed_rows, (top_score[..., 0] + jnp.log(weight_sum)).T)
    blocks = (query_plain.reshape(N_SP, TOK_DEV, HEADS, NOPE), query_turned.reshape(N_SP, TOK_DEV, HEADS, ROPE), doc_ids.reshape(N_SP, TOK_DEV))
    mixed_rows, log_sums = lax.map(one_block, blocks)
    attended = mixed_rows.reshape(TOKENS, HEADS * VDIM).astype(jnp.bfloat16)
    log_sums = log_sums.reshape(TOKENS, HEADS)
    projected = jnp.dot(attended, output_weight, preferred_element_type=jnp.float32)
    return (rms_gain(projected, out_gain), log_sums)
```

```python
import functools
import math

import jax
import jax.numpy as jnp
import numpy as np
from jax import lax
from jax.experimental import pallas as pl
from jax.experimental.pallas import tpu as pltpu
from jax.sharding import PartitionSpec as P

NOPE = 64
ROPE = 32
VDIM = 64
THETA = 10000.0
EPS = 1e-06
MASKED = -1e30
MESH = pl.DeviceIdType.MESH
F32 = jnp.float32
BF16 = jnp.bfloat16
NX, NY, NZ = 4, 4, 8
NEAR = (0, 1, 7, 2, 6, 3, 5, 4)
ZPOS = {rel: pos for pos, rel in enumerate(NEAR)}


def dot(a, b):
    return jnp.dot(a, b, preferred_element_type=F32)


def dot_t(a, b):
    return lax.dot_general(a, b, (((1,), (1,)), ((), ())), preferred_element_type=F32)


def rms(values, gain):
    wide = values.astype(F32)
    scale = lax.rsqrt(jnp.mean(wide * wide, axis=-1, keepdims=True) + EPS)
    return (wide * scale * gain).astype(BF16)


def tables(n, block, heads):
    half = ROPE // 2
    inverse = np.float32(THETA) ** (-np.arange(half, dtype=np.float32) / np.float32(half))
    inverse = inverse.astype(np.float32).astype(np.float64)[None, :]

    def turn(positions):
        angles = positions.astype(np.float64)[:, None] * inverse
        both = np.zeros((len(positions), 256), np.float32)
        both[:, :ROPE] = np.tile(np.cos(angles), (1, 2))
        both[:, 128 : 128 + ROPE] = np.tile(np.sin(angles), (1, 2))
        return both

    width = NOPE + ROPE
    pick = np.zeros((heads * width, heads * 384), np.float32)
    eye = np.arange(NOPE)
    rot = np.arange(ROPE)
    low = np.arange(half)
    for head in range(heads):
        pick[head * width + eye, head * 384 + (head % 2) * NOPE + eye] = 1
        pick[head * width + NOPE + rot, head * 384 + 128 + rot] = 1
        pick[head * width + NOPE + half + low, head * 384 + 256 + low] = -1
        pick[head * width + NOPE + low, head * 384 + 256 + half + low] = 1
    pick_key = np.zeros((ROPE, 256), np.float32)
    pick_key[rot, rot] = 1
    pick_key[half + low, 128 + low] = -1
    pick_key[low, 128 + half + low] = 1
    return turn(np.arange(block)), turn(np.arange(n) * block), pick, pick_key


def kernel(
    n, ntp, heads,
    tokens, docs, down_q, down_k, down_r, gain_q, gain_k, up_q, up_k, up_v, out_wt, gain_o,
    turn_in, turn_block, pick, pick_key,
    out, log_out,
    tok, w, wr, uq, up, wo, uq_flat, up_flat, ql, kown, koth, ks, tab, kdoc, qdoc, sel, qs,
    sbuf, vbuf, top_s, sum_s, acc_s, att, prod, part, got_core, got_y, send_y,
    loc, s_tok, r_tok, s_w, r_w, s_wr, r_wr, s_uq, r_uq, s_up, r_up, s_wo, r_wo,
    s_q, r_q, s_a, r_a, s_z, r_z, s_b, r_b, s_d, r_d, s_f, r_f,
):
    me = lax.axis_index("sp")
    t = lax.axis_index("tp")
    z, x = me // NX, lax.rem(me, NX)
    y, core = t // 2, lax.rem(t, 2)
    own, width = tokens.shape
    block = ntp * own
    rows_all = heads * block

    def wrap(v, size):
        return lax.rem(v + size, size)

    def dev(dz=0, dx=0, dy=0, c=None):
        c = core if c is None else c
        zz = wrap(z + dz, NZ) if dz else z
        xx = wrap(x + dx, NX) if dx else x
        yy = wrap(y + dy, NY) if dy else y
        return (zz * NX + xx, yy * 2 + c)

    def dev_b(d):
        bx, by = dev(dx=d), dev(dy=d)
        return (jnp.where(core == 0, by[0], bx[0]), jnp.where(core == 0, by[1], bx[1]))

    c_dev = dev(c=1 - core)

    def rc(src, dst, s, r, device):
        return pltpu.make_async_remote_copy(
            src_ref=src, dst_ref=dst, send_sem=s, recv_sem=r, device_id=device, device_id_type=MESH
        )

    sends = []

    def send(make, which=None):
        make().start()
        sends.append((make, which))

    c_tok = pltpu.make_async_copy(tokens, tok.at[core], loc.at[0])
    c_tok.start()

    @pl.when(core == 0)
    def _():
        pltpu.make_async_copy(down_k, w.at[z, x], loc.at[1]).start()

    @pl.when(core == 1)
    def _():
        pltpu.make_async_copy(down_q, w.at[z, x], loc.at[1]).start()

    c_w = pltpu.make_async_copy(down_k, w.at[z, x], loc.at[1])
    c_wr = pltpu.make_async_copy(down_r, wr.at[z, x], loc.at[2])
    nq, nk = up_q.shape[1], up_k.shape[1]
    c_uq = pltpu.make_async_copy(up_q, uq.at[z, x], loc.at[3])
    c_up = [
        pltpu.make_async_copy(up_k, up.at[z, x, :, pl.ds(0, nk)], loc.at[4]),
        pltpu.make_async_copy(up_v, up.at[z, x, :, pl.ds(nk, nk)], loc.at[5]),
    ]
    c_wo = pltpu.make_async_copy(out_wt, wo.at[z, x], loc.at[6])
    c_tab = pltpu.make_async_copy(turn_in, tab, loc.at[7])
    c_sel = pltpu.make_async_copy(pick, sel, loc.at[8])
    for copy in [c_wr, c_uq] + c_up + [c_wo, c_tab, c_sel]:
        copy.start()

    barrier = pltpu.get_barrier_semaphore()
    others = [dev(dz=d) for d in range(1, NZ)] + [dev(dx=d) for d in range(1, NX)]
    others += [dev(dy=d) for d in range(1, NY)] + [dev(dy=d, c=1 - core) for d in range(NY)]
    for device in others:
        pl.semaphore_signal(barrier, inc=1, device_id=device, device_id_type=MESH)

    down = lax.broadcasted_iota(jnp.int32, (block, block), 0)
    across = lax.broadcasted_iota(jnp.int32, (block, block), 1)
    doc_row = jnp.broadcast_to(docs[...].astype(F32), (block, block))
    doc_col = jnp.sum(jnp.where(down == across, doc_row, 0.0), axis=-1, keepdims=True)
    lane = lax.broadcasted_iota(jnp.int32, (block, 128), 1)
    in_docs = (lane >= ROPE) & (lane < ROPE + n)
    same = doc_col == (lane - ROPE).astype(F32)
    kdoc[...] = jnp.where(in_docs & same, 1.0, 0.0)
    qdoc[...] = jnp.where(in_docs & jnp.logical_not(same), MASKED, 0.0)
    c_tab.wait()
    block_turn = turn_block[pl.ds(me, 1), :]
    cos_a, sin_a = block_turn[:, :128], block_turn[:, 128:]
    cos_b, sin_b = tab[:, :128], tab[:, 128:]
    tab[:, :128] = cos_a * cos_b - sin_a * sin_b
    tab[:, 128:] = sin_a * cos_b + cos_a * sin_b

    for copy in [c_w, c_wr, c_tok, c_uq] + c_up + [c_wo, c_sel]:
        copy.wait()
    pl.semaphore_wait(barrier, len(others))

    class Gather:
        def __init__(self, ref, s, r, which=None):
            self.ref, self.s, self.r, self.which = ref, s, r, which

        def start_z(self):
            for d in NEAR[1:]:
                send(lambda d=d: rc(self.ref.at[z, x], self.ref.at[z, x], self.s.at[d], self.r.at[d], dev(dz=d)), self.which)

        def start_x(self, d):
            for k in (1, 3, 2):
                def make(k=k):
                    ref = self.ref.at[wrap(z - d, NZ), x]
                    return rc(ref, ref, self.s.at[8 * k + d], self.r.at[8 * k + d], dev(dx=k))
                send(make, self.which)

        def from_z(self, d):
            ref = self.ref.at[wrap(z - d, NZ), x]
            rc(ref, ref, self.s.at[d], self.r.at[d], c_dev).wait_recv()

        def from_x(self, d, k):
            ref = self.ref.at[wrap(z - d, NZ), wrap(x - k, NX)]
            rc(ref, ref, self.s.at[8 * k + d], self.r.at[8 * k + d], c_dev).wait_recv()

        def start_all_x(self):
            for d in NEAR[1:]:
                self.from_z(d)
            for k in (1, 3, 2):
                def make(k=k):
                    ref = self.ref.at[:, x]
                    return rc(ref, ref, self.s.at[8 * k], self.r.at[8 * k], dev(dx=k))
                send(make, self.which)

        def from_all_x(self):
            for k in (1, 3, 2):
                ref = self.ref.at[:, wrap(x - k, NX)]
                rc(ref, ref, self.s.at[8 * k], self.r.at[8 * k], c_dev).wait_recv()

    g_w = Gather(w, s_w, r_w)
    g_wr = Gather(wr, s_wr, r_wr, 0)
    g_uq = Gather(uq, s_uq, r_uq)
    g_up = Gather(up, s_up, r_up)
    g_wo = Gather(wo, s_wo, r_wo)

    g_w.start_z()
    g_w.start_x(0)

    @pl.when(core == 0)
    def _():
        g_wr.start_z()
        g_wr.start_x(0)

    send(lambda: rc(tok.at[core], tok.at[core], s_tok.at[0], r_tok.at[0], c_dev))
    g_up.start_z()
    g_uq.start_z()
    for d in NEAR[1:]:
        g_w.from_z(d)
        g_w.start_x(d)

        @pl.when(core == 0)
        def _():
            g_wr.from_z(d)
            g_wr.start_x(d)

    g_up.start_all_x()
    g_uq.start_all_x()
    g_wo.start_z()

    rc(tok.at[1 - core], tok.at[1 - core], s_tok.at[0], r_tok.at[0], c_dev).wait_recv()
    gain = jnp.where(core == 0, gain_k[...], gain_q[...])
    for d in NEAR:
        for k in (1, 3, 2):
            g_w.from_x(d, k)

    chip_tokens = tok[...].reshape(2 * own, width)
    raw = dot(chip_tokens, w[...].reshape(width, w.shape[-1])).astype(BF16)
    lat = rms(raw, gain)

    @pl.when(core == 0)
    def _():
        for d in NEAR:
            for k in (1, 3, 2):
                g_wr.from_x(d, k)
        rotary = dot(chip_tokens, wr[...].reshape(width, ROPE)).astype(BF16)
        both = dot(rotary, pick_key[...])
        rows = pl.ds(pl.multiple_of(y * (2 * own), 2 * own), 2 * own)
        turned = both[:, :128] * tab[rows, :128] + both[:, 128:] * tab[rows, 128:] + kdoc[rows, :]
        for stripe in range(2):
            first = stripe * own
            half = own // 2
            parts = [
                lat[first + s * half : first + (s + 1) * half, h * 128 : (h + 1) * 128]
                for s in range(2)
                for h in range(2)
            ]
            packed = turned[first : first + half] + pltpu.roll(turned[first + half : first + own], 64, 1)
            parts.append(packed.astype(BF16))
            for i, tile in enumerate(parts):
                if stripe == 0:
                    kown[0, 0, 0, i] = tile
                else:
                    ks[i] = tile
        for k in (1, 3, 2):
            here = kown.at[0, 0, 0]
            there = kown.at[0, 0, (-k) % 4]
            send(lambda k=k: rc(kown.at[0, 0, 0], kown.at[0, 0, (-k) % 4], s_a.at[k], r_a.at[(-k) % 4], dev(dx=k)), 0)
            send(lambda k=k: rc(ks, kown.at[0, 0, (-k) % 4], s_a.at[4 + k], r_a.at[(-k) % 4], dev(dy=k, c=1)), 0)
        send(lambda: rc(ks, kown.at[0, 0, 0], s_a.at[4], r_a.at[0], dev(c=1)), 0)

    @pl.when(core == 1)
    def _():
        ql[y] = lat
        send(lambda: rc(ql.at[y], ql.at[y], s_q.at[0], r_q.at[0], dev(c=0)), 1)
        for k in (1, 3, 2):
            for c in range(2):
                send(lambda k=k, c=c: rc(ql.at[y], ql.at[y], s_q.at[4 * c + k], r_q.at[k], dev(dy=k, c=c)), 1)

    def z_recv(pos):
        if pos == 7:
            for half in range(2):
                ref = kown.at[0, 7, pl.ds(2 * half, 2)]
                rc(ref, ref, s_z.at[0], r_z.at[7 + half], c_dev).wait_recv()
        else:
            ref = kown.at[0, pos]
            rc(ref, ref, s_z.at[0], r_z.at[pos], c_dev).wait_recv()

    def z_send(slot, src_pos, d, total, pieces=None):
        pos = ZPOS[(-total) % NZ]
        if pieces is None:
            send(lambda: rc(kown.at[0, src_pos], kown.at[0, pos], s_z.at[slot], r_z.at[pos], dev(dz=d)))
        else:
            part_of = pl.ds(2 * pieces, 2)
            send(lambda: rc(kown.at[0, src_pos, part_of], kown.at[0, 7, part_of], s_z.at[slot], r_z.at[7 + pieces], dev(dz=d)))

    def b_send(pos):
        send(lambda: rc(kown.at[0, pos], kown.at[3, pos], s_b.at[pos], r_b.at[24 + pos], dev_b(1)))
        send(lambda: rc(kown.at[0, pos], kown.at[1, pos], s_b.at[8 + pos], r_b.at[8 + pos], dev_b(-1)))

    def d_send(b, pos):
        send(lambda: rc(kown.at[b, pos], koth.at[b, pos], s_d.at[8 * b + pos], r_d.at[8 * b + pos], c_dev))

    def d_recv(b, pos):
        ref = koth.at[b, pos]
        rc(ref, ref, s_d.at[8 * b + pos], r_d.at[8 * b + pos], c_dev).wait_recv()

    def first_row():
        @pl.when(core == 1)
        def _():
            ref = kown.at[0, 0, 0]
            rc(ref, ref, s_a.at[0], r_a.at[0], c_dev).wait_recv()

        for k in (1, 3, 2):
            ref = kown.at[0, 0, k]
            rc(ref, ref, s_a.at[0], r_a.at[k], c_dev).wait_recv()
        z_send(0, 0, 2, 2)
        z_send(1, 0, -2, -2)
        z_send(2, 0, 1, 1)
        z_send(3, 0, -1, -1)
        b_send(0)
        d_send(0, 0)

    def z_row(pos):
        z_recv(pos)
        if NEAR[pos] == 6:
            z_send(4, pos, 1, 3)
            z_send(5, pos, 2, 4, 0)
        if NEAR[pos] == 2:
            z_send(6, pos, -1, -3)
            z_send(7, pos, -2, -4, 1)
        b_send(pos)
        d_send(0, pos)

    def b_row(b, pos):
        ref = kown.at[b, pos]
        rc(ref, ref, s_b.at[0], r_b.at[8 * b + pos], c_dev).wait_recv()
        half = 0 if b == 3 else 1
        part_of = pl.ds(2 * half, 2)
        send(
            lambda: rc(
                kown.at[b, pos, part_of], kown.at[2, pos, part_of],
                s_b.at[16 + 8 * half + pos], r_b.at[16 * half + pos], dev_b(1 if b == 3 else -1),
            )
        )
        d_send(b, pos)

    def far_row(pos):
        for half in range(2):
            ref = kown.at[2, pos, pl.ds(2 * half, 2)]
            rc(ref, ref, s_b.at[0], r_b.at[16 * half + pos], c_dev).wait_recv()
        d_send(2, pos)

    first_row()
    g_up.from_all_x()
    g_uq.from_all_x()
    for j in range(n):
        up_flat[j * 8 : (j + 1) * 8, :] = up[j // NX, j % NX]
        uq_flat[j * 8 : (j + 1) * 8, :] = uq[j // NX, j % NX]
    for k in range(NY):
        def wait_q(k=k):
            ref = ql.at[wrap(y - k, NY)]
            rc(ref, ref, s_q.at[0], r_q.at[k], c_dev).wait_recv()
        if k == 0:
            pl.when(core == 0)(wait_q)
        else:
            wait_q()

    scale = 1.0 / math.sqrt(NOPE + ROPE)
    factor = scale * math.log2(math.e)
    projected = dot(ql[...].reshape(block, ql.shape[-1]), uq_flat[...]).astype(BF16)
    for head in range(heads):
        laid = dot(projected, sel[:, head * 384 : (head + 1) * 384])
        turned = (laid[:, 128:256] * tab[:, :128] + laid[:, 256:] * tab[:, 128:]) * factor + qdoc[...]
        plain = (laid[:, :128] * factor).astype(BF16)
        rows = pl.ds(head * block, block)
        qs[0, rows, :128] = plain
        qs[1, rows, :128] = plain
        qs[0, rows, 128:] = turned.astype(BF16)
        qs[1, rows, 128:] = pltpu.roll(turned, 64, 1).astype(BF16)

    def score(ref, b, h, par):
        for s in range(2):
            def tiles(i):
                return ref[b, 4 * h : 4 * h + 4, :, i].reshape(256, 128)

            kv = dot(jnp.concatenate([tiles(2 * s), tiles(2 * s + 1)], axis=1), up_flat[...]).astype(BF16)
            keys = jnp.concatenate([kv[:, :nk], tiles(4)], axis=1)
            vbuf[par, s * 256 : (s + 1) * 256, :] = kv[:, nk:]
            sbuf[par, s] = dot_t(qs[s], keys)

    step = 128

    def weigh(par, first):
        for r in range(0, rows_all, step):
            rows = pl.ds(r, step)
            parts = [sbuf[par, s, rows, h * 128 : (h + 1) * 128] for s in range(2) for h in range(2)]
            most = jnp.maximum(jnp.maximum(parts[0], parts[1]), jnp.maximum(parts[2], parts[3]))
            most = jnp.max(most, axis=-1, keepdims=True)
            if first:
                new = jnp.broadcast_to(most, (step, 128))
            else:
                old = top_s[rows, :]
                new = jnp.maximum(old, most)
                alpha = jnp.exp2(old - new)
            weights = [jnp.exp2(p - new) for p in parts]
            total = (weights[0] + weights[1]) + (weights[2] + weights[3])
            mixed = dot(jnp.concatenate([p.astype(BF16) for p in weights], axis=1), vbuf[par])
            top_s[rows, :] = new
            if first:
                sum_s[rows, :] = total
                acc_s[rows, :] = mixed
            else:
                sum_s[rows, :] = sum_s[rows, :] * alpha + total
                acc_s[rows, :] = acc_s[rows, :] * alpha + mixed

    groups = []
    for b, h in ((0, 0), (0, 1), (1, 0), (3, 0), (1, 1), (3, 1), (2, 0), (2, 1)):
        groups.append((kown, b, h))
        groups.append((koth, b, h))
    events = {
        0: [lambda p=p: z_row(p) for p in (1, 2, 3, 4)],
        1: [lambda: b_row(1, 0), lambda: b_row(3, 0), lambda: z_row(5), lambda: z_row(6)],
        2: [lambda: z_row(7), lambda: b_row(1, 1), lambda: b_row(3, 1)],
        3: [lambda: b_row(1, 2), lambda: b_row(3, 2), g_wo.start_all_x],
        4: [lambda: b_row(1, 3), lambda: b_row(3, 3)],
        5: [lambda: b_row(1, 4), lambda: b_row(3, 4), lambda: far_row(0)],
        6: [lambda: b_row(1, 5), lambda: b_row(3, 5), lambda: far_row(1)],
        7: [lambda: b_row(1, 6), lambda: b_row(3, 6), lambda: far_row(2)],
        8: [lambda: b_row(1, 7), lambda: b_row(3, 7), lambda: far_row(3)],
        9: [lambda: far_row(4)],
        10: [lambda: far_row(5)],
        11: [lambda: far_row(6), lambda: far_row(7)],
    }
    for j, (ref, b, h) in enumerate(groups):
        for event in events.get(j, ()):
            event()
        if ref is koth:
            for pos in range(4 * h, 4 * h + 4):
                d_recv(b, pos)
        score(ref, b, h, j % 2)
        if j > 0:
            weigh((j - 1) % 2, j == 1)
    weigh((len(groups) - 1) % 2, False)

    head_lane = lax.broadcasted_iota(jnp.int32, (block, nk), 1) // VDIM
    attended = jnp.zeros((block, nk), F32)
    sums = []
    for head in range(heads):
        rows = pl.ds(head * block, block)
        weight_sum = jnp.sum(sum_s[rows, :], axis=-1, keepdims=True)
        attended = jnp.where(head_lane == head, acc_s[rows, :] / weight_sum, attended)
        sums.append(top_s[rows, :1] * math.log(2.0) + jnp.log(weight_sum))
    log_out[...] = jnp.concatenate(sums, axis=1)
    att[...] = attended.astype(BF16)

    g_wo.from_all_x()
    whole = dot_t(att[...], wo[...].reshape(width, nk))
    prod[...] = whole.reshape(NY, 2, own, width)

    def f_c(k):
        return rc(part.at[k], got_core.at[k], s_f.at[k], r_f.at[k], c_dev)

    def f_y(k):
        return rc(send_y.at[k], got_y.at[k], s_f.at[NY + k], r_f.at[NY + k], dev(dy=k))

    order = (2, 1, 3, 0)
    for k in order:
        part[k] = prod[wrap(y + k, NY), 1 - core].astype(BF16)
        send(lambda k=k: f_c(k))
    for k in order[:-1]:
        far = prod[wrap(y + k, NY), core]
        f_c(k).wait_recv()
        send_y[k] = (far + got_core[k].astype(F32)).astype(BF16)
        send(lambda k=k: f_y(k))
    near = prod[y, core]
    f_c(0).wait_recv()
    near = near + got_core[0].astype(F32)
    for k in order[:-1]:
        f_y(k).wait_recv()
        near = near + got_y[k].astype(F32)
    out[...] = rms(near.astype(BF16), gain_o[...])

    for make, which in sends:
        if which is None:
            make().wait_send()
    for c in range(2):
        @pl.when(core == c)
        def _():
            for make, which in sends:
                if which == c:
                    make().wait_send()


def on_device(n, ntp, tokens, doc_ids, down_q, down_k, down_r, gain_q, gain_k, up_q, up_k, up_v, out_w, gain_o):
    own, width = tokens.shape
    block = doc_ids.shape[0]
    heads = up_k.shape[1] // NOPE
    rank = down_k.shape[1]
    nq, nk, nv = up_q.shape[1], up_k.shape[1], up_v.shape[1]
    turn_in, turn_block, pick, pick_key = tables(n, block, heads)
    vmem = pl.BlockSpec(memory_space=pltpu.VMEM)
    hbm = pl.BlockSpec(memory_space=pl.ANY)
    dma = lambda k: pltpu.SemaphoreType.DMA((k,))
    v = lambda *shape, dtype=BF16: pltpu.VMEM(shape, dtype)
    rows = heads * block
    scratch = [
        v(2, own, width), v(NZ, NX, width // n, rank), v(NZ, NX, width // n, ROPE),
        v(NZ, NX, rank // n, nq), v(NZ, NX, rank // n, nk + nv), v(NZ, NX, width // n, nv),
        v(rank, nq), v(rank, nk + nv), v(NY, 2 * own, rank),
        v(4, NZ, 4, 5, own // 2, 128), v(4, NZ, 4, 5, own // 2, 128), v(5, own // 2, 128),
        v(block, 256, dtype=F32), v(block, 128, dtype=F32), v(block, 128, dtype=F32), v(*pick.shape),
        v(2, rows, 256),
        v(2, 2, rows, 256, dtype=F32), v(2, 512, nv),
        v(rows, 128, dtype=F32), v(rows, 128, dtype=F32), v(rows, 128, dtype=F32),
        v(block, nv), v(NY, 2, own, width, dtype=F32),
        v(NY, own, width), v(NY, own, width), v(NY, own, width), v(NY, own, width),
        dma(9), dma(1), dma(1), dma(32), dma(32), dma(32), dma(32), dma(32), dma(32), dma(32), dma(32), dma(32), dma(32),
        dma(8), dma(4), dma(8), dma(4), dma(8), dma(9), dma(32), dma(32), dma(32), dma(32), dma(8), dma(8),
    ]
    return pl.pallas_call(
        functools.partial(kernel, n, ntp, heads),
        out_shape=(
            jax.ShapeDtypeStruct((own, width), BF16),
            jax.ShapeDtypeStruct((block, heads), F32),
        ),
        in_specs=[hbm, vmem, hbm, hbm, hbm, vmem, vmem, hbm, hbm, hbm, hbm, vmem, hbm, vmem, hbm, vmem],
        out_specs=(vmem, vmem),
        scratch_shapes=scratch,
        compiler_params=pltpu.CompilerParams(
            collective_id=0, has_side_effects=True, vmem_limit_bytes=60 * 1024 * 1024
        ),
    )(
        tokens, doc_ids[None, :], down_q, down_k, down_r, gain_q[None, :], gain_k[None, :],
        up_q, up_k, up_v, out_w.T, gain_o[None, :],
        jnp.asarray(turn_in), jnp.asarray(turn_block), jnp.asarray(pick, BF16), jnp.asarray(pick_key, BF16),
    )


def solution(mesh):
    assert mesh.shape["tp"] == 2 * NY and mesh.shape["sp"] == NX * NZ
    placed = (
        P(("sp", "tp"), None), P("sp"), P("sp", None), P("sp", None), P("sp", None), P(), P(),
        P("sp", "tp"), P("sp", "tp"), P("sp", "tp"), P("tp", "sp"), P(),
    )
    return jax.shard_map(
        functools.partial(on_device, mesh.shape["sp"], mesh.shape["tp"]),
        mesh=mesh,
        in_specs=placed,
        out_specs=(P(("sp", "tp"), None), P("sp", "tp")),
        check_vma=False,
    )
```

```python
import functools
import math

import jax
import jax.numpy as jnp
import numpy as np
from jax import lax
from jax.experimental import pallas as pl
from jax.experimental.pallas import tpu as pltpu
from jax.sharding import PartitionSpec as P

NOPE = 64
ROPE = 32
VDIM = 64
THETA = 10000.0
EPS = 1e-06
MASKED = -1e30
MESH = pl.DeviceIdType.MESH
F32 = jnp.float32
BF16 = jnp.bfloat16
NX, NY, NZ = 4, 4, 8
NEAR = (0, 1, 7, 2, 6, 3, 5, 4)
ZPOS = {rel: pos for pos, rel in enumerate(NEAR)}


def dot(a, b):
    return jnp.dot(a, b, preferred_element_type=F32)


def dot_t(a, b):
    return lax.dot_general(a, b, (((1,), (1,)), ((), ())), preferred_element_type=F32)


def rms(values, gain):
    wide = values.astype(F32)
    scale = lax.rsqrt(jnp.mean(wide * wide, axis=-1, keepdims=True) + EPS)
    return (wide * scale * gain).astype(BF16)


def tables(n, block, heads):
    half = ROPE // 2
    inverse = np.float32(THETA) ** (-np.arange(half, dtype=np.float32) / np.float32(half))
    inverse = inverse.astype(np.float32).astype(np.float64)[None, :]

    def turn(positions):
        angles = positions.astype(np.float64)[:, None] * inverse
        both = np.zeros((len(positions), 256), np.float32)
        both[:, :ROPE] = np.tile(np.cos(angles), (1, 2))
        both[:, 128 : 128 + ROPE] = np.tile(np.sin(angles), (1, 2))
        return both

    width = NOPE + ROPE
    pick = np.zeros((heads * width, heads * 384), np.float32)
    eye = np.arange(NOPE)
    rot = np.arange(ROPE)
    low = np.arange(half)
    for head in range(heads):
        pick[head * width + eye, head * 384 + (head % 2) * NOPE + eye] = 1
        pick[head * width + NOPE + rot, head * 384 + 128 + rot] = 1
        pick[head * width + NOPE + half + low, head * 384 + 256 + low] = -1
        pick[head * width + NOPE + low, head * 384 + 256 + half + low] = 1
    pick_key = np.zeros((ROPE, 256), np.float32)
    pick_key[rot, rot] = 1
    pick_key[half + low, 128 + low] = -1
    pick_key[low, 128 + half + low] = 1
    return turn(np.arange(block)), turn(np.arange(n) * block), pick, pick_key


def kernel(
    n, ntp, heads,
    tokens, docs_in, down_q, down_k, down_r, gain_q, gain_k, up_q, up_k, up_v, out_wt, gain_o,
    turn_in, turn_block, pick, pick_key,
    out, log_out,
    docs, gain, gain_out, turn_me, sel_key,
    tok, w, wr, uq, up, wo, uq_flat, up_flat, ql, kown, koth, ks, tab, kdoc, qdoc, sel, qs,
    sbuf, vbuf, top_s, sum_s, acc_s, att, prod, part, got_core, got_y, send_y,
    loc, s_tok, r_tok, s_w, r_w, s_wr, r_wr, s_uq, r_uq, s_up, r_up, s_wo, r_wo,
    s_q, r_q, s_a, r_a, s_z, r_z, s_b, r_b, s_d, r_d, s_f, r_f,
):
    me = lax.axis_index("sp")
    t = lax.axis_index("tp")
    z, x = me // NX, lax.rem(me, NX)
    y, core = t // 2, lax.rem(t, 2)
    own, width = tokens.shape
    block = ntp * own
    rows_all = heads * block

    def wrap(v, size):
        return lax.rem(v + size, size)

    def dev(dz=0, dx=0, dy=0, c=None):
        c = core if c is None else c
        zz = wrap(z + dz, NZ) if dz else z
        xx = wrap(x + dx, NX) if dx else x
        yy = wrap(y + dy, NY) if dy else y
        return (zz * NX + xx, yy * 2 + c)

    def dev_b(d):
        bx, by = dev(dx=d), dev(dy=d)
        return (jnp.where(core == 0, by[0], bx[0]), jnp.where(core == 0, by[1], bx[1]))

    c_dev = dev(c=1 - core)

    def rc(src, dst, s, r, device):
        return pltpu.make_async_remote_copy(
            src_ref=src, dst_ref=dst, send_sem=s, recv_sem=r, device_id=device, device_id_type=MESH
        )

    def sent(ref, s):
        rc(ref, ref, s, s, c_dev).wait_send()

    def got(ref, r):
        rc(ref, ref, r, r, c_dev).wait_recv()

    barrier = pltpu.get_barrier_semaphore()
    others = [dev(dz=d) for d in range(1, NZ)] + [dev(dx=d) for d in range(1, NX)]
    others += [dev(dy=d) for d in range(1, NY)] + [dev(dy=d, c=1 - core) for d in range(NY)]
    for device in others:
        pl.semaphore_signal(barrier, inc=1, device_id=device, device_id_type=MESH)

    @pl.when(core == 0)
    def _():
        pltpu.make_async_copy(down_k, w.at[z, x], loc.at[1]).start()
        pltpu.make_async_copy(gain_k, gain, loc.at[9]).start()

    @pl.when(core == 1)
    def _():
        pltpu.make_async_copy(down_q, w.at[z, x], loc.at[1]).start()
        pltpu.make_async_copy(gain_q, gain, loc.at[9]).start()

    nq, nk = up_q.shape[1], up_k.shape[1]
    c_w = pltpu.make_async_copy(down_k, w.at[z, x], loc.at[1])
    c_gain = pltpu.make_async_copy(gain_k, gain, loc.at[9])
    c_docs = pltpu.make_async_copy(docs_in, docs, loc.at[10])
    c_tab = pltpu.make_async_copy(turn_in, tab, loc.at[7])
    c_me = pltpu.make_async_copy(turn_block.at[me], turn_me, loc.at[11])
    c_tok = pltpu.make_async_copy(tokens, tok.at[core], loc.at[0])
    c_wr = pltpu.make_async_copy(down_r, wr.at[z, x], loc.at[2])
    c_uq = pltpu.make_async_copy(up_q, uq.at[z, x], loc.at[3])
    c_up = [
        pltpu.make_async_copy(up_k, up.at[z, x, :, pl.ds(0, nk)], loc.at[4]),
        pltpu.make_async_copy(up_v, up.at[z, x, :, pl.ds(nk, nk)], loc.at[5]),
    ]
    c_wo = pltpu.make_async_copy(out_wt, wo.at[z, x], loc.at[6])
    c_sel = pltpu.make_async_copy(pick, sel, loc.at[8])
    c_key = pltpu.make_async_copy(pick_key, sel_key, loc.at[12])
    c_out = pltpu.make_async_copy(gain_o, gain_out, loc.at[13])
    for copy in [c_docs, c_tab, c_me, c_wr, c_tok, c_uq] + c_up + [c_key, c_wo, c_sel, c_out]:
        copy.start()

    down = lax.broadcasted_iota(jnp.int32, (block, block), 0)
    across = lax.broadcasted_iota(jnp.int32, (block, block), 1)
    c_docs.wait()
    doc_row = jnp.broadcast_to(docs[...].astype(F32), (block, block))
    doc_col = jnp.sum(jnp.where(down == across, doc_row, 0.0), axis=-1, keepdims=True)
    lane = lax.broadcasted_iota(jnp.int32, (block, 128), 1)
    in_docs = (lane >= ROPE) & (lane < ROPE + n)
    same = doc_col == (lane - ROPE).astype(F32)
    kdoc[...] = jnp.where(in_docs & same, 1.0, 0.0)
    qdoc[...] = jnp.where(in_docs & jnp.logical_not(same), MASKED, 0.0)
    c_tab.wait()
    c_me.wait()
    cos_a, sin_a = turn_me[:, :128], turn_me[:, 128:]
    cos_b, sin_b = tab[:, :128], tab[:, 128:]
    tab[:, :128] = cos_a * cos_b - sin_a * sin_b
    tab[:, 128:] = sin_a * cos_b + cos_a * sin_b

    for copy in [c_w, c_wr, c_tok, c_uq] + c_up + [c_key, c_gain]:
        copy.wait()
    pl.semaphore_wait(barrier, len(others))

    class Batch:
        def __init__(self, ref, s, r):
            self.ref, self.s, self.r = ref, s, r

        def start_z(self):
            here = self.ref.at[z, x]
            for d in NEAR[1:]:
                rc(here, here, self.s.at[0], self.r.at[0], dev(dz=d)).start()

        def start_x(self):
            got(self.ref.at[pl.ds(0, NZ - 1), x], self.r.at[0])
            column = self.ref.at[:, x]
            rc(column, column, self.s.at[1], self.r.at[1], dev(dx=1)).start()
            rc(column, column, self.s.at[1], self.r.at[2], dev(dx=-1)).start()

        def start_far(self):
            got(self.ref.at[:, wrap(x - 1, NX)], self.r.at[1])
            low = self.ref.at[pl.ds(0, NZ // 2), wrap(x - 1, NX)]
            rc(low, low, self.s.at[1], self.r.at[3], dev(dx=1)).start()
            got(self.ref.at[:, wrap(x + 1, NX)], self.r.at[2])
            high = self.ref.at[pl.ds(NZ // 2, NZ // 2), wrap(x + 1, NX)]
            rc(high, high, self.s.at[1], self.r.at[3], dev(dx=-1)).start()

        def finish(self):
            got(self.ref.at[:, wrap(x + 2, NX)], self.r.at[3])

        def drain(self):
            sent(self.ref.at[pl.ds(0, NZ - 1), x], self.s.at[0])
            sent(self.ref.at[pl.ds(0, NZ - 2)], self.s.at[1])

    class Pieces(Batch):
        def start_z(self):
            here = self.ref.at[z, x]
            for d in NEAR[1:]:
                rc(here, here, self.s.at[0], self.r.at[d], dev(dz=d)).start()

        def x_of(self, d):
            here = self.ref.at[wrap(z - d, NZ), x]
            if d > 0:
                got(here, self.r.at[d])
            rc(here, here, self.s.at[1], self.r.at[8 + d], dev(dx=1)).start()
            rc(here, here, self.s.at[1], self.r.at[16 + d], dev(dx=-1)).start()

        def far_of(self, d):
            low = self.ref.at[wrap(z - d, NZ), wrap(x - 1, NX)]
            high = self.ref.at[wrap(z - d, NZ), wrap(x + 1, NX)]
            got(low, self.r.at[8 + d])
            if d in (0, 7, 6, 5):
                rc(low, low, self.s.at[1], self.r.at[0], dev(dx=1)).start()
            got(high, self.r.at[16 + d])
            if d in (1, 2, 3, 4):
                rc(high, high, self.s.at[1], self.r.at[0], dev(dx=-1)).start()

        def finish(self):
            got(self.ref.at[:, wrap(x + 2, NX)], self.r.at[0])

    g_k = Pieces(w, s_w, r_w)
    g_q = Batch(w, s_w, r_w)
    g_wr = Batch(wr, s_wr, r_wr)
    g_uq = Batch(uq, s_uq, r_uq)
    g_up = Batch(up, s_up, r_up)
    g_wo = Batch(wo, s_wo, r_wo)
    here = tok.at[core]
    c_partner = rc(here, here, s_tok.at[0], r_tok.at[0], c_dev)

    @pl.when(core == 0)
    def _():
        g_k.start_z()
        g_k.x_of(0)
        g_wr.start_z()
        c_partner.start()
        g_up.start_z()
        g_uq.start_z()
        for d in (1, 7, 2, 6):
            g_k.x_of(d)
        g_k.far_of(0)
        for d in (3, 5):
            g_k.x_of(d)
        g_k.far_of(1)
        g_k.far_of(7)
        g_k.x_of(4)
        g_wr.start_x()
        for d in (2, 6, 3, 5, 4):
            g_k.far_of(d)
        g_wr.start_far()

    @pl.when(core == 1)
    def _():
        g_q.start_z()
        c_partner.start()
        g_up.start_z()
        g_uq.start_z()
        g_q.start_x()
        g_q.start_far()

    g_up.start_x()
    g_uq.start_x()
    got(tok.at[1 - core], r_tok.at[0])

    @pl.when(core == 0)
    def _():
        g_k.finish()
        g_wr.finish()

    @pl.when(core == 1)
    def _():
        g_q.finish()

    chip_tokens = tok[...].reshape(2 * own, width)
    raw = dot(chip_tokens, w[...].reshape(width, w.shape[-1])).astype(BF16)
    lat = rms(raw, gain[...])

    @pl.when(core == 0)
    def _():
        rotary = dot(chip_tokens, wr[...].reshape(width, ROPE)).astype(BF16)
        both = dot(rotary, sel_key[...])
        rows = pl.ds(pl.multiple_of(y * (2 * own), 2 * own), 2 * own)
        turned = both[:, :128] * tab[rows, :128] + both[:, 128:] * tab[rows, 128:] + kdoc[rows, :]
        for stripe in range(2):
            first = stripe * own
            half = own // 2
            parts = [
                lat[first + s * half : first + (s + 1) * half, h * 128 : (h + 1) * 128]
                for s in range(2)
                for h in range(2)
            ]
            packed = turned[first : first + half] + pltpu.roll(turned[first + half : first + own], 64, 1)
            parts.append(packed.astype(BF16))
            for i, tile in enumerate(parts):
                if stripe == 0:
                    kown[0, 0, 0, i] = tile
                else:
                    ks[i] = tile
        here = kown.at[0, 0, 0]
        rc(ks, here, s_a.at[1], r_a.at[0], dev(c=1)).start()
        for k in (2, 1, 3):
            there = kown.at[0, 0, (-k) % 4]
            rc(here, there, s_a.at[0], r_a.at[0], dev(dx=k)).start()
            rc(ks, there, s_a.at[1], r_a.at[0], dev(dy=k, c=1)).start()

    @pl.when(core == 1)
    def _():
        ql[y] = lat
        here = ql.at[y]
        for k in (2, 1, 3):
            for c in range(2):
                rc(here, here, s_q.at[c], r_q.at[0], dev(dy=k, c=c)).start()
        rc(here, here, s_q.at[0], r_q.at[0], dev(c=0)).start()

    def z_send(src_pos, d, total, pieces=None):
        pos = ZPOS[(-total) % NZ]
        part_of = pl.ds(0, 4) if pieces is None else pl.ds(2 * pieces, 2)
        rc(kown.at[0, src_pos, part_of], kown.at[0, pos, part_of], s_z.at[0], r_z.at[pos], dev(dz=d)).start()

    def b_send(pos):
        rc(kown.at[0, pos], kown.at[3, pos], s_b.at[0], r_b.at[24 + pos], dev_b(1)).start()
        rc(kown.at[0, pos], kown.at[1, pos], s_b.at[0], r_b.at[8 + pos], dev_b(-1)).start()

    def d_send(b, pos):
        rc(kown.at[b, pos], koth.at[b, pos], s_d.at[0], r_d.at[2 * b + pos // 4], c_dev).start()

    def first_row():
        @pl.when(core == 0)
        def _():
            got(kown.at[0, 0, pl.ds(1, 3)], r_a.at[0])

        @pl.when(core == 1)
        def _():
            got(kown.at[0, 0], r_a.at[0])

        z_send(0, 2, 2)
        z_send(0, -2, -2)
        z_send(0, 1, 1)
        z_send(0, -1, -1)
        b_send(0)
        d_send(0, 0)

    def z_row(pos):
        got(kown.at[0, pos], r_z.at[pos])
        if NEAR[pos] == 6:
            z_send(pos, 1, 3)
            z_send(pos, 2, 4, 0)
        if NEAR[pos] == 2:
            z_send(pos, -1, -3)
            z_send(pos, -2, -4, 1)
        b_send(pos)
        d_send(0, pos)

    def b_row(b, pos):
        got(kown.at[b, pos], r_b.at[8 * b + pos])
        half = 0 if b == 3 else 1
        part_of = pl.ds(2 * half, 2)
        rc(
            kown.at[b, pos, part_of], kown.at[2, pos, part_of], s_b.at[0], r_b.at[pos], dev_b(1 if b == 3 else -1)
        ).start()
        d_send(b, pos)

    def far_row(pos):
        got(kown.at[2, pos], r_b.at[pos])
        d_send(2, pos)

    first_row()
    g_up.start_far()
    g_uq.start_far()
    g_up.finish()
    g_uq.finish()
    for j in range(n):
        up_flat[j * 8 : (j + 1) * 8, :] = up[j // NX, j % NX]
        uq_flat[j * 8 : (j + 1) * 8, :] = uq[j // NX, j % NX]

    @pl.when(core == 0)
    def _():
        got(ql, r_q.at[0])

    @pl.when(core == 1)
    def _():
        got(ql.at[pl.ds(0, 3)], r_q.at[0])

    c_sel.wait()
    scale = 1.0 / math.sqrt(NOPE + ROPE)
    factor = scale * math.log2(math.e)
    projected = dot(ql[...].reshape(block, ql.shape[-1]), uq_flat[...]).astype(BF16)
    for head in range(heads):
        laid = dot(projected, sel[:, head * 384 : (head + 1) * 384])
        turned = (laid[:, 128:256] * tab[:, :128] + laid[:, 256:] * tab[:, 128:]) * factor + qdoc[...]
        plain = (laid[:, :128] * factor).astype(BF16)
        rows = pl.ds(head * block, block)
        qs[0, rows, :128] = plain
        qs[1, rows, :128] = plain
        qs[0, rows, 128:] = turned.astype(BF16)
        qs[1, rows, 128:] = pltpu.roll(turned, 64, 1).astype(BF16)

    def score(ref, b, h, par):
        for s in range(2):
            def tiles(i):
                return ref[b, 4 * h : 4 * h + 4, :, i].reshape(256, 128)

            kv = dot(jnp.concatenate([tiles(2 * s), tiles(2 * s + 1)], axis=1), up_flat[...]).astype(BF16)
            keys = jnp.concatenate([kv[:, :nk], tiles(4)], axis=1)
            vbuf[par, s * 256 : (s + 1) * 256, :] = kv[:, nk:]
            sbuf[par, s] = dot_t(qs[s], keys)

    step = 128

    def weigh(par, first):
        for r in range(0, rows_all, step):
            rows = pl.ds(r, step)
            parts = [sbuf[par, s, rows, h * 128 : (h + 1) * 128] for s in range(2) for h in range(2)]
            most = jnp.maximum(jnp.maximum(parts[0], parts[1]), jnp.maximum(parts[2], parts[3]))
            most = jnp.max(most, axis=-1, keepdims=True)
            if first:
                new = jnp.broadcast_to(most, (step, 128))
            else:
                old = top_s[rows, :]
                new = jnp.maximum(old, most)
                alpha = jnp.exp2(old - new)
            weights = [jnp.exp2(p - new) for p in parts]
            total = (weights[0] + weights[1]) + (weights[2] + weights[3])
            mixed = dot(jnp.concatenate([p.astype(BF16) for p in weights], axis=1), vbuf[par])
            top_s[rows, :] = new
            if first:
                sum_s[rows, :] = total
                acc_s[rows, :] = mixed
            else:
                sum_s[rows, :] = sum_s[rows, :] * alpha + total
                acc_s[rows, :] = acc_s[rows, :] * alpha + mixed

    groups = []
    for b, h in ((0, 0), (0, 1), (1, 0), (3, 0), (1, 1), (3, 1), (2, 0), (2, 1)):
        groups.append((kown, b, h))
        groups.append((koth, b, h))
    events = {
        0: [lambda p=p: z_row(p) for p in (1, 2, 3, 4)],
        1: [lambda: b_row(1, 0), lambda: b_row(3, 0), lambda: z_row(5), lambda: z_row(6)],
        2: [lambda: z_row(7), lambda: b_row(1, 1), lambda: b_row(3, 1)],
        3: [lambda: b_row(1, 2), lambda: b_row(3, 2), c_wo.wait, g_wo.start_z],
        4: [lambda: b_row(1, 3), lambda: b_row(3, 3)],
        5: [lambda: b_row(1, 4), lambda: b_row(3, 4), lambda: far_row(0)],
        6: [lambda: b_row(1, 5), lambda: b_row(3, 5), lambda: far_row(1)],
        7: [lambda: b_row(1, 6), lambda: b_row(3, 6), lambda: far_row(2)],
        8: [lambda: b_row(1, 7), lambda: b_row(3, 7), lambda: far_row(3)],
        9: [lambda: far_row(4), g_wo.start_x],
        10: [lambda: far_row(5)],
        11: [lambda: far_row(6), lambda: far_row(7)],
        13: [g_wo.start_far],
    }
    for j, (ref, b, h) in enumerate(groups):
        for event in events.get(j, ()):
            event()
        if ref is koth:
            got(koth.at[b, pl.ds(4 * h, 4)], r_d.at[2 * b + h])
        score(ref, b, h, j % 2)
        if j > 0:
            weigh((j - 1) % 2, j == 1)
    weigh((len(groups) - 1) % 2, False)

    head_lane = lax.broadcasted_iota(jnp.int32, (block, nk), 1) // VDIM
    attended = jnp.zeros((block, nk), F32)
    sums = []
    for head in range(heads):
        rows = pl.ds(head * block, block)
        weight_sum = jnp.sum(sum_s[rows, :], axis=-1, keepdims=True)
        attended = jnp.where(head_lane == head, acc_s[rows, :] / weight_sum, attended)
        log_sum = jnp.broadcast_to(top_s[rows, :1] * math.log(2.0) + jnp.log(weight_sum), (block, block))
        sums.append(jnp.sum(jnp.where(down == across, log_sum, 0.0), axis=0, keepdims=True))
    log_out[...] = jnp.concatenate(sums, axis=0)
    att[...] = attended.astype(BF16)

    g_wo.finish()
    whole = dot_t(att[...], wo[...].reshape(width, nk))
    prod[...] = whole.reshape(NY, 2, own, width)

    def f_c(k):
        return rc(part.at[k], got_core.at[k], s_f.at[0], r_f.at[k], c_dev)

    def f_y(k):
        return rc(send_y.at[k], got_y.at[k], s_f.at[1], r_f.at[NY + k], dev(dy=k))

    order = (2, 1, 3, 0)
    for k in order:
        part[k] = prod[wrap(y + k, NY), 1 - core].astype(BF16)
        f_c(k).start()
    for k in order[:-1]:
        far = prod[wrap(y + k, NY), core]
        f_c(k).wait_recv()
        send_y[k] = (far + got_core[k].astype(F32)).astype(BF16)
        f_y(k).start()
    near = prod[y, core]
    f_c(0).wait_recv()
    near = near + got_core[0].astype(F32)
    c_out.wait()
    for k in (1, 3, 2):
        f_y(k).wait_recv()
        near = near + got_y[k].astype(F32)
    out[...] = rms(near.astype(BF16), gain_out[...])

    for gather in (g_k, g_up, g_uq, g_wo):
        gather.drain()
    sent(tok.at[core], s_tok.at[0])
    sent(kown.at[0, pl.ds(0, 7)], s_z.at[0])
    sent(kown.at[pl.ds(0, 3)], s_b.at[0])
    sent(kown, s_d.at[0])
    sent(part, s_f.at[0])
    sent(send_y.at[pl.ds(1, 3)], s_f.at[1])

    @pl.when(core == 0)
    def _():
        g_wr.drain()
        sent(kown.at[0, 0, pl.ds(0, 3)], s_a.at[0])
        sent(kown.at[0, 0], s_a.at[1])

    @pl.when(core == 1)
    def _():
        sent(ql, s_q.at[0])
        sent(ql.at[pl.ds(0, 3)], s_q.at[1])


def on_device(n, ntp, tokens, doc_ids, down_q, down_k, down_r, gain_q, gain_k, up_q, up_k, up_v, out_w, gain_o):
    own, width = tokens.shape
    block = doc_ids.shape[0]
    heads = up_k.shape[1] // NOPE
    rank = down_k.shape[1]
    nq, nk, nv = up_q.shape[1], up_k.shape[1], up_v.shape[1]
    turn_in, turn_block, pick, pick_key = tables(n, block, heads)
    vmem = pl.BlockSpec(memory_space=pltpu.VMEM)
    hbm = pl.BlockSpec(memory_space=pl.ANY)
    dma = lambda k: pltpu.SemaphoreType.DMA((k,))
    v = lambda *shape, dtype=BF16: pltpu.VMEM(shape, dtype)
    rows = heads * block
    scratch = [
        pltpu.VMEM((1, block), jnp.int32), v(1, rank, dtype=F32), v(1, width, dtype=F32), v(1, 256, dtype=F32), v(ROPE, 256),
        v(2, own, width), v(NZ, NX, width // n, rank), v(NZ, NX, width // n, ROPE),
        v(NZ, NX, rank // n, nq), v(NZ, NX, rank // n, nk + nv), v(NZ, NX, width // n, nv),
        v(rank, nq), v(rank, nk + nv), v(NY, 2 * own, rank),
        v(4, NZ, 4, 5, own // 2, 128), v(4, NZ, 4, 5, own // 2, 128), v(5, own // 2, 128),
        v(block, 256, dtype=F32), v(block, 128, dtype=F32), v(block, 128, dtype=F32), v(*pick.shape),
        v(2, rows, 256),
        v(2, 2, rows, 256, dtype=F32), v(2, 512, nv),
        v(rows, 128, dtype=F32), v(rows, 128, dtype=F32), v(rows, 128, dtype=F32),
        v(block, nv), v(NY, 2, own, width, dtype=F32),
        v(NY, own, width), v(NY, own, width), v(NY, own, width), v(NY, own, width),
        dma(14), dma(1), dma(1), dma(2), dma(24), dma(2), dma(4), dma(2), dma(4), dma(2), dma(4), dma(2), dma(4),
        dma(2), dma(1), dma(2), dma(1), dma(1), dma(8), dma(1), dma(32), dma(1), dma(8), dma(2), dma(8),
    ]
    mixed, log_sums = pl.pallas_call(
        functools.partial(kernel, n, ntp, heads),
        out_shape=(
            jax.ShapeDtypeStruct((own, width), BF16),
            jax.ShapeDtypeStruct((heads, block), F32),
        ),
        in_specs=[hbm] * 16,
        out_specs=(vmem, vmem),
        scratch_shapes=scratch,
        compiler_params=pltpu.CompilerParams(
            collective_id=0, has_side_effects=True, vmem_limit_bytes=60 * 1024 * 1024
        ),
    )(
        tokens, doc_ids[None, :], down_q, down_k, down_r, gain_q[None, :], gain_k[None, :],
        up_q, up_k, up_v, out_w.T, gain_o[None, :],
        jnp.asarray(turn_in), jnp.asarray(turn_block[:, None, :]), jnp.asarray(pick, BF16), jnp.asarray(pick_key, BF16),
    )
    return mixed, log_sums.T


def solution(mesh):
    assert mesh.shape["tp"] == 2 * NY and mesh.shape["sp"] == NX * NZ
    placed = (
        P(("sp", "tp"), None), P("sp"), P("sp", None), P("sp", None), P("sp", None), P(), P(),
        P("sp", "tp"), P("sp", "tp"), P("sp", "tp"), P("tp", "sp"), P(),
    )
    return jax.shard_map(
        functools.partial(on_device, mesh.shape["sp"], mesh.shape["tp"]),
        mesh=mesh,
        in_specs=placed,
        out_specs=(P(("sp", "tp"), None), P("sp", "tp")),
        check_vma=False,
    )
```

```python
import functools
import math

import jax
import jax.numpy as jnp
import numpy as np
from jax import lax
from jax.experimental import pallas as pl
from jax.experimental.pallas import tpu as pltpu
from jax.sharding import PartitionSpec as P

NOPE = 64
ROPE = 32
VDIM = 64
THETA = 10000.0
EPS = 1e-06
MASKED = -1e30
MESH = pl.DeviceIdType.MESH
F32 = jnp.float32
BF16 = jnp.bfloat16
NX, NY, NZ = 4, 4, 8
NEAR = (0, 1, 7, 2, 6, 3, 5, 4)
ZPOS = {rel: pos for pos, rel in enumerate(NEAR)}


def dot(a, b):
    return jnp.dot(a, b, preferred_element_type=F32)


def dot_t(a, b):
    return lax.dot_general(a, b, (((1,), (1,)), ((), ())), preferred_element_type=F32)


def rms(values, gain):
    wide = values.astype(F32)
    scale = lax.rsqrt(jnp.mean(wide * wide, axis=-1, keepdims=True) + EPS)
    return (wide * scale * gain).astype(BF16)


def tables(n, block, heads):
    half = ROPE // 2
    inverse = np.float32(THETA) ** (-np.arange(half, dtype=np.float32) / np.float32(half))
    inverse = inverse.astype(np.float32).astype(np.float64)[None, :]

    def turn(positions):
        angles = positions.astype(np.float64)[:, None] * inverse
        both = np.zeros((len(positions), 256), np.float32)
        both[:, :ROPE] = np.tile(np.cos(angles), (1, 2))
        both[:, 128 : 128 + ROPE] = np.tile(np.sin(angles), (1, 2))
        return both

    width = NOPE + ROPE
    pick = np.zeros((heads * width, heads * 384), np.float32)
    eye = np.arange(NOPE)
    rot = np.arange(ROPE)
    low = np.arange(half)
    for head in range(heads):
        pick[head * width + eye, head * 384 + (head % 2) * NOPE + eye] = 1
        pick[head * width + NOPE + rot, head * 384 + 128 + rot] = 1
        pick[head * width + NOPE + half + low, head * 384 + 256 + low] = -1
        pick[head * width + NOPE + low, head * 384 + 256 + half + low] = 1
    pick_key = np.zeros((ROPE, 256), np.float32)
    pick_key[rot, rot] = 1
    pick_key[half + low, 128 + low] = -1
    pick_key[low, 128 + half + low] = 1
    mix = np.zeros((128, 128), np.float32)
    to = np.arange(128)
    mix[32 * (to // 8 % 4) + 8 * (to // 32) + to % 8, to] = 1
    return turn(np.arange(block)), turn(np.arange(n) * block), pick, pick_key, mix


def kernel(
    n, ntp, heads,
    tokens, docs_in, down_q, down_k, down_r, gain_q, gain_k, up_q, up_k, up_v, out_wt, gain_o,
    turn_in, turn_block, pick, pick_key, mix,
    out, log_out,
    docs, gain, gain_out, turn_me, sel_key, mix_in, tok_mix, wr_in, wr_flat,
    tok, w, wr, uq, up, wo, uq_flat, up_flat, ql, kown, koth, ks, tab, kdoc, qdoc, sel, qs,
    sbuf, kbuf, vbuf, top_s, sum_s, acc_s, att, prod, part, got_core, got_y, send_y,
    go, loc, s_tok, r_tok, s_w, r_w, s_wr, r_wr, s_uq, r_uq, s_up, r_up, s_wo, r_wo,
    s_q, r_q, s_a, r_a, s_z, r_z, s_b, r_b, s_d, r_d, s_f, r_f,
):
    me = lax.axis_index("sp")
    t = lax.axis_index("tp")
    z, x = me // NX, lax.rem(me, NX)
    y, core = t // 2, lax.rem(t, 2)
    own, width = tokens.shape
    block = ntp * own
    rows_all = heads * block

    def wrap(v, size):
        return lax.rem(v + size, size)

    def dev(dz=0, dx=0, dy=0, c=None):
        c = core if c is None else c
        zz = wrap(z + dz, NZ) if dz else z
        xx = wrap(x + dx, NX) if dx else x
        yy = wrap(y + dy, NY) if dy else y
        return (zz * NX + xx, yy * 2 + c)

    def dev_b(d):
        bx, by = dev(dx=d), dev(dy=d)
        return (jnp.where(core == 0, by[0], bx[0]), jnp.where(core == 0, by[1], bx[1]))

    c_dev = dev(c=1 - core)

    def rc(src, dst, s, r, device):
        return pltpu.make_async_remote_copy(
            src_ref=src, dst_ref=dst, send_sem=s, recv_sem=r, device_id=device, device_id_type=MESH
        )

    def sent(ref, s):
        rc(ref, ref, s, s, c_dev).wait_send()

    def got(ref, r):
        rc(ref, ref, r, r, c_dev).wait_recv()

    barrier = pltpu.get_barrier_semaphore()
    others = [dev(dz=d) for d in range(1, NZ)] + [dev(dx=d) for d in range(1, NX)]
    others += [dev(dy=d) for d in range(1, NY)] + [dev(dy=d, c=1 - core) for d in range(NY)]
    for device in others:
        pl.semaphore_signal(barrier, inc=1, device_id=device, device_id_type=MESH)

    @pl.when(core == 1)
    def _():
        pltpu.make_async_copy(down_k, w.at[z, x], loc.at[1]).start()
        pltpu.make_async_copy(gain_k, gain, loc.at[9]).start()

    @pl.when(core == 0)
    def _():
        pltpu.make_async_copy(down_q, w.at[z, x], loc.at[1]).start()
        pltpu.make_async_copy(gain_q, gain, loc.at[9]).start()

    nq, nk = up_q.shape[1], up_k.shape[1]
    c_w = pltpu.make_async_copy(down_k, w.at[z, x], loc.at[1])
    c_gain = pltpu.make_async_copy(gain_k, gain, loc.at[9])
    c_docs = pltpu.make_async_copy(docs_in, docs, loc.at[10])
    c_tab = pltpu.make_async_copy(turn_in, tab, loc.at[7])
    c_me = pltpu.make_async_copy(turn_block.at[me], turn_me, loc.at[11])
    c_tok = pltpu.make_async_copy(tokens, tok.at[core], loc.at[0])
    c_wr = pltpu.make_async_copy(down_r, wr_in, loc.at[2])
    c_mix = pltpu.make_async_copy(mix, mix_in, loc.at[14])
    c_uq = pltpu.make_async_copy(up_q, uq.at[z, x], loc.at[3])
    c_up = [
        pltpu.make_async_copy(up_k, up.at[z, x, :, pl.ds(0, nk)], loc.at[4]),
        pltpu.make_async_copy(up_v, up.at[z, x, :, pl.ds(nk, nk)], loc.at[5]),
    ]
    c_wo = pltpu.make_async_copy(out_wt, wo.at[z, x], loc.at[6])
    c_sel = pltpu.make_async_copy(pick, sel, loc.at[8])
    c_key = pltpu.make_async_copy(pick_key, sel_key, loc.at[12])
    c_out = pltpu.make_async_copy(gain_o, gain_out, loc.at[13])
    for copy in [c_docs, c_tab, c_me, c_wr, c_tok, c_uq] + c_up + [c_key, c_mix, c_wo, c_sel, c_out]:
        copy.start()

    down = lax.broadcasted_iota(jnp.int32, (block, block), 0)
    across = lax.broadcasted_iota(jnp.int32, (block, block), 1)
    c_docs.wait()
    doc_row = jnp.broadcast_to(docs[...].astype(F32), (block, block))
    doc_col = jnp.sum(jnp.where(down == across, doc_row, 0.0), axis=-1, keepdims=True)
    lane = lax.broadcasted_iota(jnp.int32, (block, 128), 1)
    in_docs = (lane >= ROPE) & (lane < ROPE + n)
    same = doc_col == (lane - ROPE).astype(F32)
    kdoc[...] = jnp.where(in_docs & same, 1.0, 0.0)
    qdoc[...] = jnp.where(in_docs & jnp.logical_not(same), MASKED, 0.0)
    c_tab.wait()
    c_me.wait()
    cos_a, sin_a = turn_me[:, :128], turn_me[:, 128:]
    cos_b, sin_b = tab[:, :128], tab[:, 128:]
    tab[:, :128] = cos_a * cos_b - sin_a * sin_b
    tab[:, 128:] = sin_a * cos_b + cos_a * sin_b

    rank = uq_flat.shape[0]
    c_wr.wait()
    wide_r = wr_in[...].astype(F32)
    wr[z, x] = jnp.concatenate([wide_r[8 * q : 8 * q + 8] for q in range(4)], axis=1)
    for copy in [c_w, c_tok, c_uq] + c_up + [c_key, c_mix, c_gain]:
        copy.wait()
    pl.semaphore_wait(barrier, len(others))

    class Gather:
        def __init__(self, ref, s, r):
            self.ref, self.s, self.r = ref, s, r

        def start_z(self):
            here = self.ref.at[z, x]
            for d in reversed(NEAR[1:]):
                rc(here, here, self.s.at[0], self.r.at[0], dev(dz=d)).start()

        def start_x(self):
            got(self.ref.at[pl.ds(0, NZ - 1), x], self.r.at[0])
            column = self.ref.at[:, x]
            for k in (2, 1, -1):
                rc(column, column, self.s.at[1], self.r.at[1], dev(dx=k)).start()

        def finish(self):
            got(self.ref.at[pl.ds(0, NZ - 2)], self.r.at[1])

        def drain(self):
            sent(self.ref.at[pl.ds(0, NZ - 1), 0], self.s.at[0])
            sent(self.ref.at[pl.ds(0, NZ - 2)], self.s.at[1])

    class Pieces(Gather):
        def start_z(self):
            here = self.ref.at[z, x]
            for d in reversed(NEAR[1:]):
                rc(here, here, self.s.at[0], self.r.at[d], dev(dz=d)).start()

        def pass_x(self, d):
            here = self.ref.at[wrap(z - d, NZ), x]
            if d > 0:
                got(here, self.r.at[d])
            for k in (2, 1, -1):
                rc(here, here, self.s.at[1], self.r.at[0], dev(dx=k)).start()

        def finish(self):
            got(self.ref.at[pl.ds(0, NZ - 2)], self.r.at[0])

    g_k = Pieces(w, s_w, r_w)
    g_wr = Pieces(wr, s_wr, r_wr)
    g_q = Gather(w, s_w, r_w)
    g_uq = Gather(uq, s_uq, r_uq)
    g_up = Gather(up, s_up, r_up)
    g_wo = Gather(wo, s_wo, r_wo)
    here = tok.at[core]
    c_partner = rc(here, here, s_tok.at[0], r_tok.at[0], c_dev)

    @pl.when(core == 1)
    def _():
        g_k.start_z()
        g_wr.start_z()
        g_k.pass_x(0)
        g_wr.pass_x(0)
        c_partner.start()
        for d in NEAR[1:]:
            g_k.pass_x(d)
            g_wr.pass_x(d)
            if d == 6:
                pl.semaphore_signal(go, inc=1, device_id=c_dev, device_id_type=MESH)
        g_up.start_z()
        g_uq.start_z()
        got(tok.at[1 - core], r_tok.at[0])
        both_tokens = tok[...].reshape(2 * own, width)
        for j in range(width // 128):
            cut = slice(j * 128, (j + 1) * 128)
            tok_mix[:, cut] = dot(both_tokens[:, cut], mix_in[...]).astype(BF16)
        g_wr.finish()
        packed = wr[...].reshape(rank, 128)
        for q in range(4):
            turned = (pltpu.roll(packed, 128 - 32 * q, 1) if q else packed).astype(BF16)
            for j in range(width // 128):
                wr_flat[j * 128 + q * 32 : j * 128 + (q + 1) * 32, :] = turned[j * 32 : (j + 1) * 32]
        g_k.finish()

    @pl.when(core == 0)
    def _():
        c_partner.start()
        pl.semaphore_wait(go, 1)
        g_q.start_z()
        g_up.start_z()
        g_uq.start_z()
        g_q.start_x()
        g_up.start_x()
        g_uq.start_x()
    def project():
        raw = dot(tok[...].reshape(2 * own, width), w[...].reshape(width, w.shape[-1])).astype(BF16)
        return rms(raw, gain[...])

    @pl.when(core == 1)
    def _():
        lat = project()
        rotary = dot(tok_mix[...], wr_flat[...])[:, :ROPE].astype(BF16)
        both = dot(rotary, sel_key[...])
        rows = pl.ds(pl.multiple_of(y * (2 * own), 2 * own), 2 * own)
        turned = both[:, :128] * tab[rows, :128] + both[:, 128:] * tab[rows, 128:] + kdoc[rows, :]
        half = own // 2
        for stripe in range(2):
            first = stripe * own
            parts = [
                lat[first + s * half : first + (s + 1) * half, h * 128 : (h + 1) * 128]
                for s in range(2)
                for h in range(2)
            ]
            packed = turned[first : first + half] + pltpu.roll(turned[first + half : first + own], 64, 1)
            parts.append(packed.astype(BF16))
            for i, tile in enumerate(parts):
                if stripe == 1:
                    kown[0, 0, 0, i] = tile
                else:
                    ks[i] = tile
        here = kown.at[0, 0, 0]
        rc(ks, here, s_a.at[1], r_a.at[0], dev(c=0)).start()
        for k in (2, 1, 3):
            there = kown.at[0, 0, (-k) % 4]
            rc(ks, there, s_a.at[1], r_a.at[0], dev(dx=k, c=0)).start()
            rc(here, there, s_a.at[0], r_a.at[0], dev(dy=k)).start()
        g_up.start_x()
        g_uq.start_x()

    def z_send(src_pos, d, total, pieces=None):
        pos = ZPOS[(-total) % NZ]
        part_of = pl.ds(0, 4) if pieces is None else pl.ds(2 * pieces, 2)
        rc(kown.at[0, src_pos, part_of], kown.at[0, pos, part_of], s_z.at[0], r_z.at[pos], dev(dz=d)).start()

    def b_send(pos):
        rc(kown.at[0, pos], kown.at[3, pos], s_b.at[0], r_b.at[24 + pos], dev_b(1)).start()
        rc(kown.at[0, pos], kown.at[1, pos], s_b.at[0], r_b.at[8 + pos], dev_b(-1)).start()

    def d_send(b, pos):
        rc(kown.at[b, pos], koth.at[b, pos], s_d.at[0], r_d.at[2 * b + pos // 4], c_dev).start()

    def first_row():
        @pl.when(core == 1)
        def _():
            got(kown.at[0, 0, pl.ds(1, 3)], r_a.at[0])

        @pl.when(core == 0)
        def _():
            got(kown.at[0, 0], r_a.at[0])

        z_send(0, 2, 2)
        z_send(0, -2, -2)
        z_send(0, 1, 1)
        z_send(0, -1, -1)
        b_send(0)
        d_send(0, 0)

    def z_row(pos):
        got(kown.at[0, pos], r_z.at[pos])
        if NEAR[pos] == 6:
            z_send(pos, 1, 3)
            z_send(pos, 2, 4, 0)
        if NEAR[pos] == 2:
            z_send(pos, -1, -3)
            z_send(pos, -2, -4, 1)
        b_send(pos)
        d_send(0, pos)

    def b_row(b, pos):
        got(kown.at[b, pos], r_b.at[8 * b + pos])
        half = 0 if b == 3 else 1
        part_of = pl.ds(2 * half, 2)
        rc(
            kown.at[b, pos, part_of], kown.at[2, pos, part_of], s_b.at[0], r_b.at[pos], dev_b(1 if b == 3 else -1)
        ).start()
        d_send(b, pos)

    def far_row(pos):
        got(kown.at[2, pos], r_b.at[pos])
        d_send(2, pos)

    first_row()

    @pl.when(core == 0)
    def _():
        got(tok.at[1 - core], r_tok.at[0])
        g_q.finish()
        ql[y] = project()
        here = ql.at[y]
        for k in (2, 1, 3):
            for c in range(2):
                rc(here, here, s_q.at[c], r_q.at[0], dev(dy=k, c=c)).start()
        rc(here, here, s_q.at[1], r_q.at[0], dev(c=1)).start()

    for pos in (1, 2, 3, 4):
        z_row(pos)
    g_up.finish()
    g_uq.finish()
    for j in range(n):
        up_flat[j * 8 : (j + 1) * 8, :] = up[j // NX, j % NX]
        uq_flat[j * 8 : (j + 1) * 8, :] = uq[j // NX, j % NX]

    @pl.when(core == 1)
    def _():
        got(ql, r_q.at[0])

    @pl.when(core == 0)
    def _():
        got(ql.at[pl.ds(0, 3)], r_q.at[0])

    c_sel.wait()
    scale = 1.0 / math.sqrt(NOPE + ROPE)
    factor = scale * math.log2(math.e)
    projected = dot(ql[...].reshape(block, ql.shape[-1]), uq_flat[...]).astype(BF16)
    for head in range(heads):
        laid = dot(projected, sel[:, head * 384 : (head + 1) * 384])
        turned = (laid[:, 128:256] * tab[:, :128] + laid[:, 256:] * tab[:, 128:]) * factor + qdoc[...]
        plain = (laid[:, :128] * factor).astype(BF16)
        rows = pl.ds(head * block, block)
        qs[0, rows, :128] = plain
        qs[1, rows, :128] = plain
        qs[0, rows, 128:] = turned.astype(BF16)
        qs[1, rows, 128:] = pltpu.roll(turned, 64, 1).astype(BF16)

    def tiles(ref, b, h, i):
        return ref[b, 4 * h : 4 * h + 4, :, i].reshape(256, 128)

    def expand(j):
        ref, b, h = groups[j]
        for s in range(2):
            lat = jnp.concatenate([tiles(ref, b, h, 2 * s), tiles(ref, b, h, 2 * s + 1)], axis=1)
            kv = dot(lat, up_flat[...]).astype(BF16)
            kbuf[j % 2, s] = kv[:, :nk]
            vbuf[j % 3, s * 256 : (s + 1) * 256, :] = kv[:, nk:]

    def score(j):
        ref, b, h = groups[j]
        rot = tiles(ref, b, h, 4)
        for s in range(2):
            sbuf[j % 2, s] = dot_t(qs[s], jnp.concatenate([kbuf[j % 2, s], rot], axis=1))

    step = 128

    def weigh(j):
        par, first = j % 2, j == 0
        for r in range(0, rows_all, step):
            rows = pl.ds(r, step)
            parts = [sbuf[par, s, rows, h * 128 : (h + 1) * 128] for s in range(2) for h in range(2)]
            most = jnp.maximum(jnp.maximum(parts[0], parts[1]), jnp.maximum(parts[2], parts[3]))
            most = jnp.max(most, axis=-1, keepdims=True)
            if first:
                new = jnp.broadcast_to(most, (step, 128))
            else:
                old = top_s[rows, :]
                new = jnp.maximum(old, most)
                alpha = jnp.exp2(old - new)
            weights = [jnp.exp2(p - new) for p in parts]
            total = (weights[0] + weights[1]) + (weights[2] + weights[3])
            mixed = dot(jnp.concatenate([p.astype(BF16) for p in weights], axis=1), vbuf[j % 3])
            top_s[rows, :] = new
            if first:
                sum_s[rows, :] = total
                acc_s[rows, :] = mixed
            else:
                sum_s[rows, :] = sum_s[rows, :] * alpha + total
                acc_s[rows, :] = acc_s[rows, :] * alpha + mixed

    groups = []
    for b, h in ((0, 0), (0, 1), (1, 0), (3, 0), (1, 1), (3, 1), (2, 0), (2, 1)):
        groups.append((kown, b, h))
        groups.append((koth, b, h))
    events = {
        1: [lambda: b_row(1, 0), lambda: b_row(3, 0), lambda: z_row(5), lambda: z_row(6)],
        2: [lambda: z_row(7), lambda: b_row(1, 1), lambda: b_row(3, 1)],
        3: [lambda: b_row(1, 2), lambda: b_row(3, 2), c_wo.wait, g_wo.start_z],
        4: [lambda: b_row(1, 3), lambda: b_row(3, 3)],
        5: [lambda: b_row(1, 4), lambda: b_row(3, 4), lambda: far_row(0)],
        6: [lambda: b_row(1, 5), lambda: b_row(3, 5), lambda: far_row(1)],
        7: [lambda: b_row(1, 6), lambda: b_row(3, 6), lambda: far_row(2)],
        8: [lambda: b_row(1, 7), lambda: b_row(3, 7), lambda: far_row(3)],
        9: [lambda: far_row(4), g_wo.start_x],
        10: [lambda: far_row(5)],
        11: [lambda: far_row(6), lambda: far_row(7)],
    }
    for j, (ref, b, h) in enumerate(groups):
        for event in events.get(j, ()):
            event()
        if ref is koth:
            got(koth.at[b, pl.ds(4 * h, 4)], r_d.at[2 * b + h])
        expand(j)
        if j >= 1:
            score(j - 1)
        if j >= 2:
            weigh(j - 2)
    last = len(groups) - 1
    score(last)
    weigh(last - 1)
    weigh(last)

    head_lane = lax.broadcasted_iota(jnp.int32, (block, nk), 1) // VDIM
    attended = jnp.zeros((block, nk), F32)
    sums = []
    for head in range(heads):
        rows = pl.ds(head * block, block)
        weight_sum = jnp.sum(sum_s[rows, :], axis=-1, keepdims=True)
        attended = jnp.where(head_lane == head, acc_s[rows, :] / weight_sum, attended)
        log_sum = jnp.broadcast_to(top_s[rows, :1] * math.log(2.0) + jnp.log(weight_sum), (block, block))
        sums.append(jnp.sum(jnp.where(down == across, log_sum, 0.0), axis=0, keepdims=True))
    log_out[...] = jnp.concatenate(sums, axis=0)
    att[...] = attended.astype(BF16)

    g_wo.finish()
    whole = dot_t(att[...], wo[...].reshape(width, nk))
    prod[...] = whole.reshape(NY, 2, own, width)

    def f_c(k):
        return rc(part.at[k], got_core.at[k], s_f.at[0], r_f.at[k], c_dev)

    def f_y(k):
        return rc(send_y.at[k], got_y.at[k], s_f.at[1], r_f.at[NY + k], dev(dy=k))

    order = (2, 1, 3, 0)
    for k in order:
        part[k] = prod[wrap(y + k, NY), 1 - core].astype(BF16)
        f_c(k).start()
    for k in order[:-1]:
        far = prod[wrap(y + k, NY), core]
        f_c(k).wait_recv()
        send_y[k] = (far + got_core[k].astype(F32)).astype(BF16)
        f_y(k).start()
    near = prod[y, core]
    f_c(0).wait_recv()
    near = near + got_core[0].astype(F32)
    c_out.wait()
    for k in (1, 3, 2):
        f_y(k).wait_recv()
        near = near + got_y[k].astype(F32)
    out[...] = rms(near.astype(BF16), gain_out[...])

    for gather in (g_up, g_uq, g_wo):
        gather.drain()
    sent(tok.at[core], s_tok.at[0])
    sent(kown.at[0, pl.ds(0, 7)], s_z.at[0])
    sent(kown.at[pl.ds(0, 3)], s_b.at[0])
    sent(kown, s_d.at[0])
    sent(part, s_f.at[0])
    sent(send_y.at[pl.ds(1, 3)], s_f.at[1])

    @pl.when(core == 1)
    def _():
        g_k.drain()
        g_wr.drain()
        sent(kown.at[0, 0, pl.ds(0, 3)], s_a.at[0])
        sent(kown.at[0, 0], s_a.at[1])

    @pl.when(core == 0)
    def _():
        g_q.drain()
        sent(ql, s_q.at[1])
        sent(ql.at[pl.ds(0, 3)], s_q.at[0])


def on_device(n, ntp, tokens, doc_ids, down_q, down_k, down_r, gain_q, gain_k, up_q, up_k, up_v, out_w, gain_o):
    own, width = tokens.shape
    block = doc_ids.shape[0]
    heads = up_k.shape[1] // NOPE
    rank = down_k.shape[1]
    nq, nk, nv = up_q.shape[1], up_k.shape[1], up_v.shape[1]
    turn_in, turn_block, pick, pick_key, mix = tables(n, block, heads)
    vmem = pl.BlockSpec(memory_space=pltpu.VMEM)
    hbm = pl.BlockSpec(memory_space=pl.ANY)
    dma = lambda k: pltpu.SemaphoreType.DMA((k,))
    v = lambda *shape, dtype=BF16: pltpu.VMEM(shape, dtype)
    rows = heads * block
    scratch = [
        pltpu.VMEM((1, block), jnp.int32), v(1, rank, dtype=F32), v(1, width, dtype=F32), v(1, 256, dtype=F32), v(ROPE, 256),
        v(128, 128), v(2 * own, width), v(width // n, ROPE), v(width, 128),
        v(2, own, width), v(NZ, NX, width // n, rank), v(NZ, NX, width // n // 4, 128, dtype=F32),
        v(NZ, NX, rank // n, nq), v(NZ, NX, rank // n, nk + nv), v(NZ, NX, width // n, nv),
        v(rank, nq), v(rank, nk + nv), v(NY, 2 * own, rank),
        v(4, NZ, 4, 5, own // 2, 128), v(4, NZ, 4, 5, own // 2, 128), v(5, own // 2, 128),
        v(block, 256, dtype=F32), v(block, 128, dtype=F32), v(block, 128, dtype=F32), v(*pick.shape),
        v(2, rows, 256),
        v(2, 2, rows, 256, dtype=F32), v(2, 2, 256, nk), v(3, 512, nv),
        v(rows, 128, dtype=F32), v(rows, 128, dtype=F32), v(rows, 128, dtype=F32),
        v(block, nv), v(NY, 2, own, width, dtype=F32),
        v(NY, own, width), v(NY, own, width), v(NY, own, width), v(NY, own, width),
        pltpu.SemaphoreType.REGULAR,
        dma(15), dma(1), dma(1), dma(2), dma(8), dma(2), dma(8), dma(2), dma(2), dma(2), dma(2), dma(2), dma(2),
        dma(2), dma(1), dma(2), dma(1), dma(1), dma(8), dma(1), dma(32), dma(1), dma(8), dma(2), dma(8),
    ]
    mixed, log_sums = pl.pallas_call(
        functools.partial(kernel, n, ntp, heads),
        out_shape=(
            jax.ShapeDtypeStruct((own, width), BF16),
            jax.ShapeDtypeStruct((heads, block), F32),
        ),
        in_specs=[hbm] * 17,
        out_specs=(vmem, vmem),
        scratch_shapes=scratch,
        compiler_params=pltpu.CompilerParams(
            collective_id=0, has_side_effects=True, vmem_limit_bytes=60 * 1024 * 1024
        ),
    )(
        tokens, doc_ids[None, :], down_q, down_k, down_r, gain_q[None, :], gain_k[None, :],
        up_q, up_k, up_v, out_w.T, gain_o[None, :],
        jnp.asarray(turn_in), jnp.asarray(turn_block[:, None, :]), jnp.asarray(pick, BF16), jnp.asarray(pick_key, BF16), jnp.asarray(mix, BF16),
    )
    return mixed, log_sums.T


def solution(mesh):
    assert mesh.shape["tp"] == 2 * NY and mesh.shape["sp"] == NX * NZ
    placed = (
        P(("sp", "tp"), None), P("sp"), P("sp", None), P("sp", None), P("sp", None), P(), P(),
        P("sp", "tp"), P("sp", "tp"), P("sp", "tp"), P("tp", "sp"), P(),
    )
    return jax.shard_map(
        functools.partial(on_device, mesh.shape["sp"], mesh.shape["tp"]),
        mesh=mesh,
        in_specs=placed,
        out_specs=(P(("sp", "tp"), None), P("sp", "tp")),
        check_vma=False,
    )
```

```python
import functools
import math

import jax
import jax.numpy as jnp
import numpy as np
from jax import lax
from jax.experimental import pallas as pl
from jax.experimental.pallas import tpu as pltpu
from jax.sharding import PartitionSpec as P

NOPE = 64
ROPE = 32
VDIM = 64
THETA = 10000.0
EPS = 1e-06
MASKED = -1e30
MESH = pl.DeviceIdType.MESH
F32 = jnp.float32
BF16 = jnp.bfloat16
NX, NY, NZ = 4, 4, 8
NEAR = (0, 1, 7, 2, 6, 3, 5, 4)
ZPOS = {rel: pos for pos, rel in enumerate(NEAR)}


def dot(a, b):
    return jnp.dot(a, b, preferred_element_type=F32)


def dot_t(a, b):
    return lax.dot_general(a, b, (((1,), (1,)), ((), ())), preferred_element_type=F32)


def rms(values, gain):
    wide = values.astype(F32)
    scale = lax.rsqrt(jnp.mean(wide * wide, axis=-1, keepdims=True) + EPS)
    return (wide * scale * gain).astype(BF16)


def tables(n, block, heads):
    half = ROPE // 2
    inverse = np.float32(THETA) ** (-np.arange(half, dtype=np.float32) / np.float32(half))
    inverse = inverse.astype(np.float32).astype(np.float64)[None, :]

    def turn(positions):
        angles = positions.astype(np.float64)[:, None] * inverse
        both = np.zeros((len(positions), 256), np.float32)
        both[:, :ROPE] = np.tile(np.cos(angles), (1, 2))
        both[:, 128 : 128 + ROPE] = np.tile(np.sin(angles), (1, 2))
        return both

    width = NOPE + ROPE
    pick = np.zeros((heads * width, heads * 384), np.float32)
    eye = np.arange(NOPE)
    rot = np.arange(ROPE)
    low = np.arange(half)
    for head in range(heads):
        pick[head * width + eye, head * 384 + (head % 2) * NOPE + eye] = 1
        pick[head * width + NOPE + rot, head * 384 + 128 + rot] = 1
        pick[head * width + NOPE + half + low, head * 384 + 256 + low] = -1
        pick[head * width + NOPE + low, head * 384 + 256 + half + low] = 1
    pick_key = np.zeros((ROPE, 256), np.float32)
    pick_key[rot, rot] = 1
    pick_key[half + low, 128 + low] = -1
    pick_key[low, 128 + half + low] = 1
    mix = np.zeros((128, 128), np.float32)
    to = np.arange(128)
    mix[32 * (to // 8 % 4) + 8 * (to // 32) + to % 8, to] = 1
    return turn(np.arange(block)), turn(np.arange(n) * block), pick, pick_key, mix


def kernel(
    n, ntp, heads,
    tokens, docs_in, down_q, down_k, down_r, gain_q, gain_k, up_q, up_k, up_v, out_wt, gain_o,
    turn_in, turn_block, pick, pick_key, mix,
    out, log_out,
    docs, gain, gain_out, turn_me, sel_key, mix_in, tok_mix, wr_in, wr_flat,
    tok, w, wr, uq, up, wo, uq_flat, up_flat, ql, kown, koth, ks, tab, kdoc, qdoc, sel, qs,
    sbuf, kbuf, vbuf, top_s, sum_s, acc_s, osend, oget, lget,
    go, loc, s_tok, r_tok, s_w, r_w, s_wr, r_wr, s_uq, r_uq, s_up, r_up, s_wo, r_wo,
    s_q, r_q, s_a, r_a, s_z, r_z, s_d, r_d, s_f, r_f,
):
    me = lax.axis_index("sp")
    t = lax.axis_index("tp")
    z, x = me // NX, lax.rem(me, NX)
    y, core = t // 2, lax.rem(t, 2)
    own, width = tokens.shape
    block = ntp * own
    rows_all = heads * block

    def wrap(v, size):
        return lax.rem(v + size, size)

    def dev(dz=0, dx=0, dy=0, c=None):
        c = core if c is None else c
        zz = wrap(z + dz, NZ) if dz else z
        xx = wrap(x + dx, NX) if dx else x
        yy = wrap(y + dy, NY) if dy else y
        return (zz * NX + xx, yy * 2 + c)

    c_dev = dev(c=1 - core)

    def rc(src, dst, s, r, device):
        return pltpu.make_async_remote_copy(
            src_ref=src, dst_ref=dst, send_sem=s, recv_sem=r, device_id=device, device_id_type=MESH
        )

    def sent(ref, s):
        rc(ref, ref, s, s, c_dev).wait_send()

    def got(ref, r):
        rc(ref, ref, r, r, c_dev).wait_recv()

    barrier = pltpu.get_barrier_semaphore()
    others = [dev(dz=d) for d in range(1, NZ)] + [dev(dx=d) for d in range(1, NX)]
    others += [dev(dz=d, c=1 - core) for d in range(1, NZ)]
    others += [dev(dy=d) for d in range(1, NY)] + [dev(dy=d, c=1 - core) for d in range(NY)]
    for device in others:
        pl.semaphore_signal(barrier, inc=1, device_id=device, device_id_type=MESH)

    @pl.when(core == 1)
    def _():
        pltpu.make_async_copy(down_k, w.at[z, x], loc.at[1]).start()
        pltpu.make_async_copy(gain_k, gain, loc.at[9]).start()

    @pl.when(core == 0)
    def _():
        pltpu.make_async_copy(down_q, w.at[z, x], loc.at[1]).start()
        pltpu.make_async_copy(gain_q, gain, loc.at[9]).start()

    nq, nk = up_q.shape[1], up_k.shape[1]
    c_w = pltpu.make_async_copy(down_k, w.at[z, x], loc.at[1])
    c_gain = pltpu.make_async_copy(gain_k, gain, loc.at[9])
    c_docs = pltpu.make_async_copy(docs_in, docs, loc.at[10])
    c_tab = pltpu.make_async_copy(turn_in, tab, loc.at[7])
    c_me = pltpu.make_async_copy(turn_block.at[me], turn_me, loc.at[11])
    c_tok = pltpu.make_async_copy(tokens, tok.at[core], loc.at[0])
    c_wr = pltpu.make_async_copy(down_r, wr_in, loc.at[2])
    c_mix = pltpu.make_async_copy(mix, mix_in, loc.at[14])
    c_uq = pltpu.make_async_copy(up_q, uq.at[0, z, x], loc.at[3])
    c_up = [
        pltpu.make_async_copy(up_k, up.at[0, z, x, :, pl.ds(0, nk)], loc.at[4]),
        pltpu.make_async_copy(up_v, up.at[0, z, x, :, pl.ds(nk, nk)], loc.at[5]),
    ]
    c_wo = pltpu.make_async_copy(out_wt, wo.at[y, core, z, x], loc.at[6])
    c_sel = pltpu.make_async_copy(pick, sel, loc.at[8])
    c_key = pltpu.make_async_copy(pick_key, sel_key, loc.at[12])
    c_out = pltpu.make_async_copy(gain_o, gain_out, loc.at[13])
    for copy in [c_docs, c_tab, c_me, c_wr, c_tok, c_uq] + c_up + [c_key, c_mix, c_wo, c_sel, c_out]:
        copy.start()

    down = lax.broadcasted_iota(jnp.int32, (block, block), 0)
    across = lax.broadcasted_iota(jnp.int32, (block, block), 1)
    c_docs.wait()
    doc_row = jnp.broadcast_to(docs[...].astype(F32), (block, block))
    doc_col = jnp.sum(jnp.where(down == across, doc_row, 0.0), axis=-1, keepdims=True)
    lane = lax.broadcasted_iota(jnp.int32, (block, 128), 1)
    in_docs = (lane >= ROPE) & (lane < ROPE + n)
    same = doc_col == (lane - ROPE).astype(F32)
    kdoc[...] = jnp.where(in_docs & same, 1.0, 0.0)
    qdoc[...] = jnp.where(in_docs & jnp.logical_not(same), MASKED, 0.0)
    c_tab.wait()
    c_me.wait()
    cos_a, sin_a = turn_me[:, :128], turn_me[:, 128:]
    cos_b, sin_b = tab[:, :128], tab[:, 128:]
    tab[:, :128] = cos_a * cos_b - sin_a * sin_b
    tab[:, 128:] = sin_a * cos_b + cos_a * sin_b

    rank = uq_flat.shape[1]
    c_wr.wait()
    wide_r = wr_in[...].astype(F32)
    wr[z, x] = jnp.concatenate([wide_r[8 * q : 8 * q + 8] for q in range(4)], axis=1)
    for copy in [c_w, c_tok, c_uq] + c_up + [c_key, c_mix, c_gain, c_wo]:
        copy.wait()
    pl.semaphore_wait(barrier, len(others))

    class Gather:
        def __init__(self, at, s, r):
            self.at, self.s, self.r = at, s, r

        def start_z(self):
            here = self.at(z, x)
            for d in reversed(NEAR[1:]):
                rc(here, here, self.s.at[0], self.r.at[0], dev(dz=d)).start()

        def start_x(self):
            got(self.at(pl.ds(0, NZ - 1), x), self.r.at[0])
            column = self.at(slice(None), x)
            for k in (2, 1, -1):
                rc(column, column, self.s.at[1], self.r.at[1], dev(dx=k)).start()

        def finish(self):
            got(self.at(pl.ds(0, NZ - 2), slice(None)), self.r.at[1])

        def drain(self):
            sent(self.at(pl.ds(0, NZ - 1), 0), self.s.at[0])
            sent(self.at(pl.ds(0, NZ - 2), slice(None)), self.s.at[1])

    class Pieces(Gather):
        def start_z(self):
            here = self.at(z, x)
            for d in reversed(NEAR[1:]):
                rc(here, here, self.s.at[0], self.r.at[d], dev(dz=d)).start()

        def pass_x(self, d):
            here = self.at(wrap(z - d, NZ), x)
            if d > 0:
                got(here, self.r.at[d])
            for k in (2, 1, -1):
                rc(here, here, self.s.at[1], self.r.at[0], dev(dx=k)).start()

        def finish(self):
            got(self.at(pl.ds(0, NZ - 2), slice(None)), self.r.at[0])

    g_k = Pieces(lambda i, j: w.at[i, j], s_w, r_w)
    g_wr = Pieces(lambda i, j: wr.at[i, j], s_wr, r_wr)
    g_q = Gather(lambda i, j: w.at[i, j], s_w, r_w)
    g_uq = Gather(lambda i, j: uq.at[0, i, j], s_uq, r_uq)
    g_up = Gather(lambda i, j: up.at[0, i, j], s_up, r_up)
    g_wo = Gather(lambda i, j: wo.at[:, core, i, j], s_wo, r_wo)

    def wo_y():
        here = wo.at[y, core, z, x]
        for k in (2, 1, 3):
            rc(here, here, s_wo.at[2], r_wo.at[2], dev(dy=k)).start()

    def wo_z():
        got(wo.at[pl.ds(0, 3), core, z, x], r_wo.at[2])
        g_wo.start_z()

    def wo_cross():
        g_wo.finish()
        here = wo.at[:, core]
        rc(here, here, s_wo.at[3], r_wo.at[3], c_dev).start()


    def heads_y(ref, g, s, r):
        g.finish()
        for k in (1, 3, 2):
            rel = -k % NY
            rc(ref.at[0], ref.at[rel], s.at[2], r.at[1 + rel], dev(dy=k)).start()

    def heads_in(rel):
        if rel:
            got(up.at[rel], r_up.at[1 + rel])
            got(uq.at[rel], r_uq.at[1 + rel])
        for j in range(n):
            up_flat[rel, j * 8 : (j + 1) * 8, :] = up[rel, j // NX, j % NX]
            uq_flat[rel, j * 8 : (j + 1) * 8, :] = uq[rel, j // NX, j % NX]

    here = tok.at[core]
    c_partner = rc(here, here, s_tok.at[0], r_tok.at[0], c_dev)

    @pl.when(core == 1)
    def _():
        g_k.start_z()
        g_wr.start_z()
        g_k.pass_x(0)
        g_wr.pass_x(0)
        c_partner.start()
        wo_y()
        g_up.start_z()
        g_uq.start_z()
        for d in NEAR[1:]:
            g_k.pass_x(d)
            g_wr.pass_x(d)
            if d == 6:
                pl.semaphore_signal(go, inc=1, device_id=c_dev, device_id_type=MESH)
        g_up.start_x()
        g_uq.start_x()
        wo_z()
        got(tok.at[1 - core], r_tok.at[0])
        both_tokens = tok[...].reshape(2 * own, width)
        for j in range(width // 128):
            cut = slice(j * 128, (j + 1) * 128)
            tok_mix[:, cut] = dot(both_tokens[:, cut], mix_in[...]).astype(BF16)
        g_wr.finish()
        packed = wr[...].reshape(rank, 128)
        for q in range(4):
            turned = (pltpu.roll(packed, 128 - 32 * q, 1) if q else packed).astype(BF16)
            for j in range(width // 128):
                wr_flat[j * 128 + q * 32 : j * 128 + (q + 1) * 32, :] = turned[j * 32 : (j + 1) * 32]
        g_k.finish()

    @pl.when(core == 0)
    def _():
        c_partner.start()
        wo_y()
        g_up.start_z()
        g_uq.start_z()
        pl.semaphore_wait(go, 1)
        g_q.start_z()
        g_up.start_x()
        g_uq.start_x()
        g_q.start_x()
        wo_z()

    def project():
        raw = dot(tok[...].reshape(2 * own, width), w[...].reshape(width, w.shape[-1])).astype(BF16)
        return rms(raw, gain[...])

    @pl.when(core == 1)
    def _():
        lat = project()
        rotary = dot(tok_mix[...], wr_flat[...])[:, :ROPE].astype(BF16)
        both = dot(rotary, sel_key[...])
        rows = pl.ds(pl.multiple_of(y * (2 * own), 2 * own), 2 * own)
        turned = both[:, :128] * tab[rows, :128] + both[:, 128:] * tab[rows, 128:] + kdoc[rows, :]
        half = own // 2
        for stripe in range(2):
            first = stripe * own
            parts = [
                lat[first + s * half : first + (s + 1) * half, h * 128 : (h + 1) * 128]
                for s in range(2)
                for h in range(2)
            ]
            packed = turned[first : first + half] + pltpu.roll(turned[first + half : first + own], 64, 1)
            parts.append(packed.astype(BF16))
            for i, tile in enumerate(parts):
                if stripe == 1:
                    kown[0, 0, i] = tile
                else:
                    ks[i] = tile
        here = kown.at[0, 0]
        rc(ks, here, s_z.at[1], r_z.at[2], dev(c=0)).start()
        for d in (4, 1, 7, 6, 2, 3, 5):
            pos = ZPOS[-d % NZ]
            there, sem = kown.at[0, pos], r_z.at[0 if pos < 4 else 1]
            rc(ks, there, s_z.at[1], sem, dev(dz=d, c=0)).start()
            rc(here, there, s_z.at[0], sem, dev(dz=d)).start()

    parts = ((0, 1), (1, 3), (4, 4))

    def a_send(p):
        first, length = parts[p]
        src = kown.at[0, pl.ds(first, length)]
        for k in (2, 1, 3):
            rel = -k % NX
            sem = r_a.at[0] if p == 0 else r_a.at[3 * p - 3 + rel]
            rc(src, kown.at[rel, pl.ds(first, length)], s_a.at[0], sem, dev(dx=k)).start()

    def cross(a, count, p):
        cut = pl.ds(*parts[p])
        src, dst = kown.at[pl.ds(a, count), cut], koth.at[pl.ds(a, count), cut]
        rc(src, dst, s_d.at[0], r_d.at[1 if p == 2 else 0], c_dev).start()

    def z_part(p):
        if p == 0:
            @pl.when(core == 0)
            def _():
                got(kown.at[0, 0], r_z.at[2])
        else:
            got(kown.at[0, pl.ds(*parts[p])], r_z.at[p - 1])
        a_send(p)
        cross(0, 1, p)

    def a_part(p):
        if p == 0:
            got(kown.at[pl.ds(1, 3), 0], r_a.at[0])
            cross(1, 3, 0)
        else:
            for rel in (1, 3, 2):
                got(kown.at[rel, pl.ds(*parts[p])], r_a.at[3 * p - 3 + rel])
                cross(rel, 1, p)

    z_part(0)

    @pl.when(core == 0)
    def _():
        got(tok.at[1 - core], r_tok.at[0])
        g_q.finish()
        ql[y] = project()
        here = ql.at[y]
        for k in (2, 1, 3):
            for c in range(2):
                rc(here, here, s_q.at[c], r_q.at[0], dev(dy=k, c=c)).start()
        rc(here, here, s_q.at[1], r_q.at[0], dev(c=1)).start()

    heads_y(up, g_up, s_up, r_up)
    heads_y(uq, g_uq, s_uq, r_uq)
    heads_in(0)
    a_part(0)
    z_part(1)
    z_part(2)
    a_part(1)
    g_wo.start_x()

    @pl.when(core == 1)
    def _():
        got(ql, r_q.at[0])

    @pl.when(core == 0)
    def _():
        got(ql.at[pl.ds(0, 3)], r_q.at[0])

    c_sel.wait()
    scale = 1.0 / math.sqrt(NOPE + ROPE)
    factor = scale * math.log2(math.e)

    def queries_of(rel):
        projected = dot(ql[...].reshape(block, ql.shape[-1]), uq_flat[rel]).astype(BF16)
        for head in range(heads):
            laid = dot(projected, sel[:, head * 384 : (head + 1) * 384])
            turned = (laid[:, 128:256] * tab[:, :128] + laid[:, 256:] * tab[:, 128:]) * factor + qdoc[...]
            plain = (laid[:, :128] * factor).astype(BF16)
            rows = pl.ds(head * block, block)
            qs[rel, 0, rows, :128] = plain
            qs[rel, 1, rows, :128] = plain
            qs[rel, 0, rows, 128:] = turned.astype(BF16)
            qs[rel, 1, rows, 128:] = pltpu.roll(turned, 64, 1).astype(BF16)

    def tiles(ref, h, i):
        return ref[:, 4 * h : 4 * h + 4, i].reshape(256, 128)

    def expand(j):
        ref, h, rel = groups[j]
        for s in range(2):
            lat = jnp.concatenate([tiles(ref, h, 2 * s), tiles(ref, h, 2 * s + 1)], axis=1)
            kv = dot(lat, up_flat[rel]).astype(BF16)
            kbuf[j % 2, s] = kv[:, :nk]
            vbuf[j % 3, s * 256 : (s + 1) * 256, :] = kv[:, nk:]

    def score(j):
        ref, h, rel = groups[j]
        rot = tiles(ref, h, 4)
        for s in range(2):
            sbuf[j % 2, s] = dot_t(qs[rel, s], jnp.concatenate([kbuf[j % 2, s], rot], axis=1))

    step = 128

    def weigh(j):
        par, first, pair = j % 2, j % 4 == 0, j // 4 % 2
        for r in range(0, rows_all, step):
            rows = pl.ds(r, step)
            parts = [sbuf[par, s, rows, h * 128 : (h + 1) * 128] for s in range(2) for h in range(2)]
            most = jnp.maximum(jnp.maximum(parts[0], parts[1]), jnp.maximum(parts[2], parts[3]))
            most = jnp.max(most, axis=-1, keepdims=True)
            if first:
                new = jnp.broadcast_to(most, (step, 128))
            else:
                old = top_s[pair, rows, :]
                new = jnp.maximum(old, most)
                alpha = jnp.exp2(old - new)
            weights = [jnp.exp2(p - new) for p in parts]
            total = (weights[0] + weights[1]) + (weights[2] + weights[3])
            mixed = dot(jnp.concatenate([p.astype(BF16) for p in weights], axis=1), vbuf[j % 3])
            top_s[pair, rows, :] = new
            if first:
                sum_s[pair, rows, :] = total
                acc_s[pair, rows, :] = mixed
            else:
                sum_s[pair, rows, :] = sum_s[pair, rows, :] * alpha + total
                acc_s[pair, rows, :] = acc_s[pair, rows, :] * alpha + mixed

    head_lane = lax.broadcasted_iota(jnp.int32, (block, nk), 1) // VDIM

    def close(i, rel):
        pair = i % 2
        outs, sums = [], []
        for head in range(heads):
            rows = pl.ds(head * block, block)
            weight_sum = jnp.sum(sum_s[pair, rows, :], axis=-1, keepdims=True)
            outs.append(acc_s[pair, rows, :] / weight_sum)
            log_sum = jnp.broadcast_to(top_s[pair, rows, :1] + jnp.log2(weight_sum), (block, block))
            sums.append(jnp.sum(jnp.where(down == across, log_sum, 0.0), axis=0, keepdims=True))
        osend[i] = jnp.where(head_lane == 0, outs[0], outs[1]).astype(BF16)
        slot = y * NY + wrap(y + rel, NY)
        lget[core, slot] = jnp.concatenate(sums, axis=0)
        oget[core, slot] = osend[i, pl.ds(pl.multiple_of(t * own, own), own), :]
        for k in (2, 1, 3, 0):
            for c in range(2):
                def go_to(c=c, k=k):
                    device = dev(dy=k, c=c)
                    rows = pl.ds(pl.multiple_of(device[1] * own, own), own)
                    rc(osend.at[i, rows], oget.at[core, slot], s_f.at[0], r_f.at[0], device).start()
                    rc(lget.at[core, slot], lget.at[core, slot], s_f.at[1], r_f.at[1], device).start()
                if k:
                    go_to()
                else:
                    pl.when(core != c)(go_to)

    order = (0, 1, 3, 2)
    groups = [(ref, h, rel) for rel in order for ref, h in ((kown, 0), (koth, 0), (kown, 1), (koth, 1))]
    events = {
        0: [lambda: queries_of(0)],
        1: [lambda: a_part(2)],
        3: [lambda: heads_in(1)],
        7: [lambda: heads_in(3)],
        11: [lambda: heads_in(2)],
        14: [wo_cross],
    }
    for j, (ref, h, rel) in enumerate(groups):
        for event in events.get(j, ()):
            event()
        if j == 1 or j == 3:
            got(koth.at[:, pl.ds(4 * h, 4)], r_d.at[h])
        expand(j)
        if j % 4 == 3 and j < 15:
            queries_of(groups[j + 1][2])
        if j >= 1:
            score(j - 1)
        if j >= 2:
            weigh(j - 2)
            if (j - 2) % 4 == 3:
                close((j - 2) // 4, groups[j - 2][2])
    last = len(groups) - 1
    score(last)
    weigh(last - 1)
    weigh(last)
    close(last // 4, groups[last][2])

    c_out.wait()
    got(lget.at[:, pl.ds(0, 14)], r_f.at[1])
    got(oget.at[:, pl.ds(0, 14)], r_f.at[0])
    spot = lax.broadcasted_iota(jnp.int32, (own, block), 0) + t * own
    spot = spot == lax.broadcasted_iota(jnp.int32, (own, block), 1)
    own_lane = lax.broadcasted_iota(jnp.int32, (own, nk), 1) // VDIM

    def column(row):
        return jnp.sum(jnp.where(spot, jnp.broadcast_to(row, (own, block)), 0.0), axis=-1, keepdims=True)

    got(wo.at[:, 0], r_wo.at[3])
    mixed = jnp.zeros((own, width), F32)
    for p in range(NY):
        merged = []
        for c in range(2):
            logs = [lget[c, q * NY + p] for q in range(NY)]
            most = jnp.maximum(jnp.maximum(logs[0], logs[1]), jnp.maximum(logs[2], logs[3]))
            shares = [jnp.exp2(log - most) for log in logs]
            whole = (shares[0] + shares[1]) + (shares[2] + shares[3])
            total = jnp.zeros((own, nk), F32)
            for q in range(NY):
                share = shares[q] / whole
                both = jnp.where(own_lane == 0, column(share[:1]), column(share[1:]))
                total = total + both * oget[c, q * NY + p].astype(F32)
            merged.append(total.astype(BF16))
        weights = jnp.concatenate([wo[p, c].reshape(width, nk) for c in range(2)], axis=1)
        mixed = mixed + dot_t(jnp.concatenate(merged, axis=1), weights)
    out[...] = rms(mixed.astype(BF16), gain_out[...])
    logs = [lget[core, q * NY + y] for q in range(NY)]
    most = jnp.maximum(jnp.maximum(logs[0], logs[1]), jnp.maximum(logs[2], logs[3]))
    shares = [jnp.exp2(log - most) for log in logs]
    whole = (shares[0] + shares[1]) + (shares[2] + shares[3])
    log_out[...] = most * math.log(2.0) + jnp.log(whole)

    for gather in (g_up, g_uq, g_wo):
        gather.drain()
    sent(up.at[pl.ds(0, 3)], s_up.at[2])
    sent(uq.at[pl.ds(0, 3)], s_uq.at[2])
    sent(wo.at[pl.ds(0, 3), core, 0, 0], s_wo.at[2])
    sent(wo.at[:, 0], s_wo.at[3])
    sent(tok.at[core], s_tok.at[0])
    sent(kown.at[pl.ds(0, 3)], s_a.at[0])
    sent(kown, s_d.at[0])
    sent(oget.at[:, pl.ds(0, 14)], s_f.at[0])
    sent(lget.at[:, pl.ds(0, 14)], s_f.at[1])

    @pl.when(core == 1)
    def _():
        g_k.drain()
        g_wr.drain()
        sent(kown.at[0, pl.ds(0, 7)], s_z.at[0])
        sent(kown.at[0], s_z.at[1])

    @pl.when(core == 0)
    def _():
        g_q.drain()
        sent(ql, s_q.at[1])
        sent(ql.at[pl.ds(0, 3)], s_q.at[0])


def on_device(n, ntp, tokens, doc_ids, down_q, down_k, down_r, gain_q, gain_k, up_q, up_k, up_v, out_w, gain_o):
    own, width = tokens.shape
    block = doc_ids.shape[0]
    heads = up_k.shape[1] // NOPE
    rank = down_k.shape[1]
    nq, nk, nv = up_q.shape[1], up_k.shape[1], up_v.shape[1]
    turn_in, turn_block, pick, pick_key, mix = tables(n, block, heads)
    vmem = pl.BlockSpec(memory_space=pltpu.VMEM)
    hbm = pl.BlockSpec(memory_space=pl.ANY)
    dma = lambda k: pltpu.SemaphoreType.DMA((k,))
    v = lambda *shape, dtype=BF16: pltpu.VMEM(shape, dtype)
    rows = heads * block
    scratch = [
        pltpu.VMEM((1, block), jnp.int32), v(1, rank, dtype=F32), v(1, width, dtype=F32), v(1, 256, dtype=F32), v(ROPE, 256),
        v(128, 128), v(2 * own, width), v(width // n, ROPE), v(width, 128),
        v(2, own, width), v(NZ, NX, width // n, rank), v(NZ, NX, width // n // 4, 128, dtype=F32),
        v(NY, NZ, NX, rank // n, nq), v(NY, NZ, NX, rank // n, nk + nv), v(NY, 2, NZ, NX, width // n, nv),
        v(NY, rank, nq), v(NY, rank, nk + nv), v(NY, 2 * own, rank),
        v(NX, NZ, 5, own // 2, 128), v(NX, NZ, 5, own // 2, 128), v(5, own // 2, 128),
        v(block, 256, dtype=F32), v(block, 128, dtype=F32), v(block, 128, dtype=F32), v(*pick.shape),
        v(NY, 2, rows, 256),
        v(2, 2, rows, 256, dtype=F32), v(2, 2, 256, nk), v(3, 512, nv),
        v(2, rows, 128, dtype=F32), v(2, rows, 128, dtype=F32), v(2, rows, 128, dtype=F32),
        v(NY, block, nv), v(2, NY * NY, own, nv), v(2, NY * NY, heads, block, dtype=F32),
        pltpu.SemaphoreType.REGULAR,
        dma(15), dma(1), dma(1), dma(2), dma(8), dma(2), dma(8), dma(3), dma(5), dma(3), dma(5), dma(4), dma(4),
        dma(2), dma(1), dma(1), dma(7), dma(2), dma(3), dma(1), dma(2), dma(2), dma(2),
    ]
    mixed, log_sums = pl.pallas_call(
        functools.partial(kernel, n, ntp, heads),
        out_shape=(
            jax.ShapeDtypeStruct((own, width), BF16),
            jax.ShapeDtypeStruct((heads, block), F32),
        ),
        in_specs=[hbm] * 17,
        out_specs=(vmem, vmem),
        scratch_shapes=scratch,
        compiler_params=pltpu.CompilerParams(
            collective_id=0, has_side_effects=True, vmem_limit_bytes=60 * 1024 * 1024
        ),
    )(
        tokens, doc_ids[None, :], down_q, down_k, down_r, gain_q[None, :], gain_k[None, :],
        up_q, up_k, up_v, out_w.T, gain_o[None, :],
        jnp.asarray(turn_in), jnp.asarray(turn_block[:, None, :]), jnp.asarray(pick, BF16), jnp.asarray(pick_key, BF16), jnp.asarray(mix, BF16),
    )
    return mixed, log_sums.T


def solution(mesh):
    assert mesh.shape["tp"] == 2 * NY and mesh.shape["sp"] == NX * NZ
    placed = (
        P(("sp", "tp"), None), P("sp"), P("sp", None), P("sp", None), P("sp", None), P(), P(),
        P("sp", "tp"), P("sp", "tp"), P("sp", "tp"), P("tp", "sp"), P(),
    )
    return jax.shard_map(
        functools.partial(on_device, mesh.shape["sp"], mesh.shape["tp"]),
        mesh=mesh,
        in_specs=placed,
        out_specs=(P(("sp", "tp"), None), P("sp", "tp")),
        check_vma=False,
    )
```

```python
import functools
import math

import jax
import jax.numpy as jnp
import numpy as np
from jax import lax
from jax.experimental import pallas as pl
from jax.experimental.pallas import tpu as pltpu
from jax.sharding import PartitionSpec as P

NOPE = 64
ROPE = 32
VDIM = 64
THETA = 10000.0
EPS = 1e-06
MASKED = -1e30
MESH = pl.DeviceIdType.MESH
F32 = jnp.float32
BF16 = jnp.bfloat16
NX, NY, NZ = 4, 4, 8
NEAR = (0, 1, 7, 2, 6, 3, 5, 4)
ZPOS = {rel: pos for pos, rel in enumerate(NEAR)}


def dot(a, b):
    return jnp.dot(a, b, preferred_element_type=F32)


def dot_t(a, b):
    return lax.dot_general(a, b, (((1,), (1,)), ((), ())), preferred_element_type=F32)


def rms(values, gain):
    wide = values.astype(F32)
    scale = lax.rsqrt(jnp.mean(wide * wide, axis=-1, keepdims=True) + EPS)
    return (wide * scale * gain).astype(BF16)


def tables(n, block, heads):
    half = ROPE // 2
    inverse = np.float32(THETA) ** (-np.arange(half, dtype=np.float32) / np.float32(half))
    inverse = inverse.astype(np.float32).astype(np.float64)[None, :]

    def turn(positions):
        angles = positions.astype(np.float64)[:, None] * inverse
        both = np.zeros((len(positions), 256), np.float32)
        both[:, :ROPE] = np.tile(np.cos(angles), (1, 2))
        both[:, 128 : 128 + ROPE] = np.tile(np.sin(angles), (1, 2))
        return both

    width = NOPE + ROPE
    pick = np.zeros((heads * width, heads * 384), np.float32)
    eye = np.arange(NOPE)
    rot = np.arange(ROPE)
    low = np.arange(half)
    for head in range(heads):
        pick[head * width + eye, head * 384 + (head % 2) * NOPE + eye] = 1
        pick[head * width + NOPE + rot, head * 384 + 128 + rot] = 1
        pick[head * width + NOPE + half + low, head * 384 + 256 + low] = -1
        pick[head * width + NOPE + low, head * 384 + 256 + half + low] = 1
    pick_key = np.zeros((ROPE, 256), np.float32)
    pick_key[rot, rot] = 1
    pick_key[half + low, 128 + low] = -1
    pick_key[low, 128 + half + low] = 1
    mix = np.zeros((128, 128), np.float32)
    to = np.arange(128)
    mix[32 * (to // 8 % 4) + 8 * (to // 32) + to % 8, to] = 1
    return turn(np.arange(block)), turn(np.arange(n) * block), pick, pick_key, mix


def kernel(
    n, ntp, heads,
    tokens, docs_in, down_q, down_k, down_r, gain_q, gain_k, up_q, up_k, up_v, out_wt, gain_o,
    turn_in, turn_block, pick, pick_key, mix,
    out, log_out,
    docs, gain, gain_out, turn_me, sel_key, mix_in, tok_mix, wr_in, wr_flat,
    tok, w, wr, uq, up, wo, uq_flat, up_flat, ql, kown, koth, ks, tab, kdoc, qdoc, sel, qs,
    sbuf, kbuf, vbuf, top_s, sum_s, acc_s, osend, oget, lget,
    go, loc, s_tok, r_tok, s_w, r_w, s_wr, r_wr, s_uq, r_uq, s_up, r_up, s_wo, r_wo,
    s_q, r_q, s_a, r_a, s_z, r_z, s_d, r_d, s_f, r_f,
):
    me = lax.axis_index("sp")
    t = lax.axis_index("tp")
    z, x = me // NX, lax.rem(me, NX)
    y, core = t // 2, lax.rem(t, 2)
    own, width = tokens.shape
    block = ntp * own
    rows_all = heads * block

    def wrap(v, size):
        return lax.rem(v + size, size)

    def dev(dz=0, dx=0, dy=0, c=None):
        c = core if c is None else c
        zz = wrap(z + dz, NZ) if dz else z
        xx = wrap(x + dx, NX) if dx else x
        yy = wrap(y + dy, NY) if dy else y
        return (zz * NX + xx, yy * 2 + c)

    c_dev = dev(c=1 - core)

    def rc(src, dst, s, r, device):
        return pltpu.make_async_remote_copy(
            src_ref=src, dst_ref=dst, send_sem=s, recv_sem=r, device_id=device, device_id_type=MESH
        )

    def sent(ref, s):
        rc(ref, ref, s, s, c_dev).wait_send()

    def got(ref, r):
        rc(ref, ref, r, r, c_dev).wait_recv()

    barrier = pltpu.get_barrier_semaphore()
    others = [dev(dz=d) for d in range(1, NZ)] + [dev(dx=d) for d in range(1, NX)]
    others += [dev(dz=d, c=1 - core) for d in range(1, NZ)]
    others += [dev(dy=d) for d in range(1, NY)] + [dev(dy=d, c=1 - core) for d in range(NY)]
    for device in others:
        pl.semaphore_signal(barrier, inc=1, device_id=device, device_id_type=MESH)

    @pl.when(core == 1)
    def _():
        pltpu.make_async_copy(down_k, w.at[z, x], loc.at[1]).start()
        pltpu.make_async_copy(gain_k, gain, loc.at[9]).start()

    @pl.when(core == 0)
    def _():
        pltpu.make_async_copy(down_q, w.at[z, x], loc.at[1]).start()
        pltpu.make_async_copy(gain_q, gain, loc.at[9]).start()

    nq, nk = up_q.shape[1], up_k.shape[1]
    c_w = pltpu.make_async_copy(down_k, w.at[z, x], loc.at[1])
    c_gain = pltpu.make_async_copy(gain_k, gain, loc.at[9])
    c_docs = pltpu.make_async_copy(docs_in, docs, loc.at[10])
    c_tab = pltpu.make_async_copy(turn_in, tab, loc.at[7])
    c_me = pltpu.make_async_copy(turn_block.at[me], turn_me, loc.at[11])
    c_tok = pltpu.make_async_copy(tokens, tok.at[core], loc.at[0])
    c_wr = pltpu.make_async_copy(down_r, wr_in, loc.at[2])
    c_mix = pltpu.make_async_copy(mix, mix_in, loc.at[14])
    c_uq = pltpu.make_async_copy(up_q, uq.at[0, z, x], loc.at[3])
    c_up = [
        pltpu.make_async_copy(up_k, up.at[0, z, x, :, pl.ds(0, nk)], loc.at[4]),
        pltpu.make_async_copy(up_v, up.at[0, z, x, :, pl.ds(nk, nk)], loc.at[5]),
    ]
    c_wo = pltpu.make_async_copy(out_wt, wo.at[y, core, z, x], loc.at[6])
    c_sel = pltpu.make_async_copy(pick, sel, loc.at[8])
    c_key = pltpu.make_async_copy(pick_key, sel_key, loc.at[12])
    c_out = pltpu.make_async_copy(gain_o, gain_out, loc.at[13])
    for copy in [c_docs, c_tab, c_me, c_wr, c_tok, c_uq] + c_up + [c_key, c_mix, c_wo, c_sel, c_out]:
        copy.start()

    down = lax.broadcasted_iota(jnp.int32, (block, block), 0)
    across = lax.broadcasted_iota(jnp.int32, (block, block), 1)
    c_docs.wait()
    doc_row = jnp.broadcast_to(docs[...].astype(F32), (block, block))
    doc_col = jnp.sum(jnp.where(down == across, doc_row, 0.0), axis=-1, keepdims=True)
    lane = lax.broadcasted_iota(jnp.int32, (block, 128), 1)
    in_docs = (lane >= ROPE) & (lane < ROPE + n)
    same = doc_col == (lane - ROPE).astype(F32)
    kdoc[...] = jnp.where(in_docs & same, 1.0, 0.0)
    qdoc[...] = jnp.where(in_docs & jnp.logical_not(same), MASKED, 0.0)
    c_tab.wait()
    c_me.wait()
    cos_a, sin_a = turn_me[:, :128], turn_me[:, 128:]
    cos_b, sin_b = tab[:, :128], tab[:, 128:]
    tab[:, :128] = cos_a * cos_b - sin_a * sin_b
    tab[:, 128:] = sin_a * cos_b + cos_a * sin_b

    rank = uq_flat.shape[1]
    c_wr.wait()
    wide_r = wr_in[...].astype(F32)
    wr[z, x] = jnp.concatenate([wide_r[8 * q : 8 * q + 8] for q in range(4)], axis=1)
    for copy in [c_w, c_tok, c_uq] + c_up + [c_key, c_mix, c_gain, c_wo]:
        copy.wait()
    pl.semaphore_wait(barrier, len(others))

    class Gather:
        def __init__(self, at, s, r):
            self.at, self.s, self.r = at, s, r

        def start_z(self):
            here = self.at(z, x)
            for d in reversed(NEAR[1:]):
                rc(here, here, self.s.at[0], self.r.at[0], dev(dz=d)).start()

        def start_x(self):
            got(self.at(pl.ds(0, NZ - 1), x), self.r.at[0])
            column = self.at(slice(None), x)
            for k in (2, 1, -1):
                rc(column, column, self.s.at[1], self.r.at[1], dev(dx=k)).start()

        def finish(self):
            got(self.at(pl.ds(0, NZ - 2), slice(None)), self.r.at[1])

        def drain(self):
            sent(self.at(pl.ds(0, NZ - 1), 0), self.s.at[0])
            sent(self.at(pl.ds(0, NZ - 2), slice(None)), self.s.at[1])

    class Pieces(Gather):
        def start_z(self):
            here = self.at(z, x)
            for d in reversed(NEAR[1:]):
                rc(here, here, self.s.at[0], self.r.at[d], dev(dz=d)).start()

        def pass_x(self, d):
            here = self.at(wrap(z - d, NZ), x)
            if d > 0:
                got(here, self.r.at[d])
            for k in (2, 1, -1):
                rc(here, here, self.s.at[1], self.r.at[0], dev(dx=k)).start()

        def finish(self):
            got(self.at(pl.ds(0, NZ - 2), slice(None)), self.r.at[0])

    g_k = Pieces(lambda i, j: w.at[i, j], s_w, r_w)
    g_wr = Pieces(lambda i, j: wr.at[i, j], s_wr, r_wr)
    g_q = Gather(lambda i, j: w.at[i, j], s_w, r_w)
    g_uq = Gather(lambda i, j: uq.at[0, i, j], s_uq, r_uq)
    g_up = Gather(lambda i, j: up.at[0, i, j], s_up, r_up)
    g_w0 = Gather(lambda i, j: wo.at[:, 0, i, j], s_wo, r_wo)
    g_w1 = Gather(lambda i, j: wo.at[y, 1, i, j], s_wo, r_wo)

    def wo_y():
        here = wo.at[y, 0, z, x]
        for k in (2, 1, 3):
            rc(here, here, s_wo.at[2], r_wo.at[2], dev(dy=k)).start()

    def wo_z():
        got(wo.at[pl.ds(0, 3), 0, z, x], r_wo.at[2])
        g_w0.start_z()

    def wo_last():
        pl.when(core == 0)(g_w0.start_x)

        @pl.when(core == 1)
        def _():
            g_w1.finish()
            here = wo.at[y, 1]
            for k in (2, 1, 3):
                rc(here, here, s_wo.at[2], r_wo.at[2], dev(dy=k)).start()

    def wo_cross():
        pl.when(core == 0)(g_w0.finish)

        @pl.when(core == 1)
        def _():
            got(wo.at[pl.ds(0, 3), 1], r_wo.at[2])

        here = wo.at[:, core]
        rc(here, here, s_wo.at[3], r_wo.at[3], c_dev).start()

    def heads_y(ref, g, s, r):
        g.finish()
        for k in (1, 3, 2):
            rel = -k % NY
            rc(ref.at[0], ref.at[rel], s.at[2], r.at[1 + rel], dev(dy=k)).start()

    def heads_in(rel):
        if rel:
            got(up.at[rel], r_up.at[1 + rel])
            got(uq.at[rel], r_uq.at[1 + rel])
        for j in range(n):
            up_flat[rel, j * 8 : (j + 1) * 8, :] = up[rel, j // NX, j % NX]
            uq_flat[rel, j * 8 : (j + 1) * 8, :] = uq[rel, j // NX, j % NX]

    here = tok.at[core]
    c_partner = rc(here, here, s_tok.at[0], r_tok.at[0], c_dev)

    @pl.when(core == 1)
    def _():
        g_k.start_z()
        g_wr.start_z()
        g_k.pass_x(0)
        g_wr.pass_x(0)
        c_partner.start()
        g_up.start_z()
        g_uq.start_z()
        g_w1.start_z()
        for d in NEAR[1:]:
            g_k.pass_x(d)
            g_wr.pass_x(d)
            if d == 6:
                pl.semaphore_signal(go, inc=1, device_id=c_dev, device_id_type=MESH)
        g_up.start_x()
        g_uq.start_x()
        g_w1.start_x()
        got(tok.at[1 - core], r_tok.at[0])
        both_tokens = tok[...].reshape(2 * own, width)
        for j in range(width // 128):
            cut = slice(j * 128, (j + 1) * 128)
            tok_mix[:, cut] = dot(both_tokens[:, cut], mix_in[...]).astype(BF16)
        g_wr.finish()
        packed = wr[...].reshape(rank, 128)
        for q in range(4):
            turned = (pltpu.roll(packed, 128 - 32 * q, 1) if q else packed).astype(BF16)
            for j in range(width // 128):
                wr_flat[j * 128 + q * 32 : j * 128 + (q + 1) * 32, :] = turned[j * 32 : (j + 1) * 32]
        g_k.finish()

    @pl.when(core == 0)
    def _():
        c_partner.start()
        wo_y()
        g_up.start_z()
        g_uq.start_z()
        pl.semaphore_wait(go, 1)
        g_q.start_z()
        g_up.start_x()
        g_uq.start_x()
        g_q.start_x()
        wo_z()

    def project():
        raw = dot(tok[...].reshape(2 * own, width), w[...].reshape(width, w.shape[-1])).astype(BF16)
        return rms(raw, gain[...])

    @pl.when(core == 1)
    def _():
        lat = project()
        rotary = dot(tok_mix[...], wr_flat[...])[:, :ROPE].astype(BF16)
        both = dot(rotary, sel_key[...])
        rows = pl.ds(pl.multiple_of(y * (2 * own), 2 * own), 2 * own)
        turned = both[:, :128] * tab[rows, :128] + both[:, 128:] * tab[rows, 128:] + kdoc[rows, :]
        half = own // 2
        for stripe in range(2):
            first = stripe * own
            parts = [
                lat[first + s * half : first + (s + 1) * half, h * 128 : (h + 1) * 128]
                for s in range(2)
                for h in range(2)
            ]
            packed = turned[first : first + half] + pltpu.roll(turned[first + half : first + own], 64, 1)
            parts.append(packed.astype(BF16))
            for i, tile in enumerate(parts):
                if stripe == 1:
                    kown[0, 0, i] = tile
                else:
                    ks[i] = tile
        here = kown.at[0, 0]
        rc(ks, here, s_z.at[1], r_z.at[2], dev(c=0)).start()
        for d in (4, 1, 7, 6, 2, 3, 5):
            pos = ZPOS[-d % NZ]
            there, sem = kown.at[0, pos], r_z.at[0 if pos < 4 else 1]
            rc(ks, there, s_z.at[1], sem, dev(dz=d, c=0)).start()
            rc(here, there, s_z.at[0], sem, dev(dz=d)).start()

    parts = ((0, 1), (1, 3), (4, 4))

    def a_send(p):
        first, length = parts[p]
        src = kown.at[0, pl.ds(first, length)]
        for k in (2, 1, 3):
            rel = -k % NX
            sem = r_a.at[0] if p == 0 else r_a.at[3 * p - 3 + rel]
            rc(src, kown.at[rel, pl.ds(first, length)], s_a.at[0], sem, dev(dx=k)).start()

    def cross(a, count, p):
        cut = pl.ds(*parts[p])
        src, dst = kown.at[pl.ds(a, count), cut], koth.at[pl.ds(a, count), cut]
        rc(src, dst, s_d.at[0], r_d.at[1 if p == 2 else 0], c_dev).start()

    def z_part(p):
        if p == 0:
            @pl.when(core == 0)
            def _():
                got(kown.at[0, 0], r_z.at[2])
        else:
            got(kown.at[0, pl.ds(*parts[p])], r_z.at[p - 1])
        a_send(p)
        cross(0, 1, p)

    def a_part(p):
        if p == 0:
            got(kown.at[pl.ds(1, 3), 0], r_a.at[0])
            cross(1, 3, 0)
        else:
            for rel in (1, 3, 2):
                got(kown.at[rel, pl.ds(*parts[p])], r_a.at[3 * p - 3 + rel])
                cross(rel, 1, p)

    z_part(0)

    @pl.when(core == 0)
    def _():
        got(tok.at[1 - core], r_tok.at[0])
        g_q.finish()
        ql[y] = project()
        here = ql.at[y]
        for k in (2, 1, 3):
            for c in range(2):
                rc(here, here, s_q.at[c], r_q.at[0], dev(dy=k, c=c)).start()
        rc(here, here, s_q.at[1], r_q.at[0], dev(c=1)).start()

    heads_y(up, g_up, s_up, r_up)
    heads_y(uq, g_uq, s_uq, r_uq)
    heads_in(0)
    a_part(0)
    z_part(1)
    z_part(2)
    a_part(1)

    @pl.when(core == 1)
    def _():
        got(ql, r_q.at[0])

    @pl.when(core == 0)
    def _():
        got(ql.at[pl.ds(0, 3)], r_q.at[0])

    c_sel.wait()
    scale = 1.0 / math.sqrt(NOPE + ROPE)
    factor = scale * math.log2(math.e)

    def queries_of(rel):
        projected = dot(ql[...].reshape(block, ql.shape[-1]), uq_flat[rel]).astype(BF16)
        for head in range(heads):
            laid = dot(projected, sel[:, head * 384 : (head + 1) * 384])
            turned = (laid[:, 128:256] * tab[:, :128] + laid[:, 256:] * tab[:, 128:]) * factor + qdoc[...]
            plain = (laid[:, :128] * factor).astype(BF16)
            rows = pl.ds(head * block, block)
            qs[rel, 0, rows, :128] = plain
            qs[rel, 1, rows, :128] = plain
            qs[rel, 0, rows, 128:] = turned.astype(BF16)
            qs[rel, 1, rows, 128:] = pltpu.roll(turned, 64, 1).astype(BF16)

    def tiles(ref, h, i):
        return ref[:, 4 * h : 4 * h + 4, i].reshape(256, 128)

    def expand(j):
        ref, h, rel = groups[j]
        for s in range(2):
            lat = jnp.concatenate([tiles(ref, h, 2 * s), tiles(ref, h, 2 * s + 1)], axis=1)
            kv = dot(lat, up_flat[rel]).astype(BF16)
            kbuf[j % 2, s] = kv[:, :nk]
            vbuf[j % 3, s * 256 : (s + 1) * 256, :] = kv[:, nk:]

    def score(j):
        ref, h, rel = groups[j]
        rot = tiles(ref, h, 4)
        for s in range(2):
            sbuf[j % 2, s] = dot_t(qs[rel, s], jnp.concatenate([kbuf[j % 2, s], rot], axis=1))

    step = 128

    def weigh(j):
        par, first, pair = j % 2, j % 4 == 0, j // 4 % 2
        for r in range(0, rows_all, step):
            rows = pl.ds(r, step)
            parts = [sbuf[par, s, rows, h * 128 : (h + 1) * 128] for s in range(2) for h in range(2)]
            most = jnp.maximum(jnp.maximum(parts[0], parts[1]), jnp.maximum(parts[2], parts[3]))
            most = jnp.max(most, axis=-1, keepdims=True)
            if first:
                new = jnp.broadcast_to(most, (step, 128))
            else:
                old = top_s[pair, rows, :]
                new = jnp.maximum(old, most)
                alpha = jnp.exp2(old - new)
            weights = [jnp.exp2(p - new) for p in parts]
            total = (weights[0] + weights[1]) + (weights[2] + weights[3])
            mixed = dot(jnp.concatenate([p.astype(BF16) for p in weights], axis=1), vbuf[j % 3])
            top_s[pair, rows, :] = new
            if first:
                sum_s[pair, rows, :] = total
                acc_s[pair, rows, :] = mixed
            else:
                sum_s[pair, rows, :] = sum_s[pair, rows, :] * alpha + total
                acc_s[pair, rows, :] = acc_s[pair, rows, :] * alpha + mixed

    head_lane = lax.broadcasted_iota(jnp.int32, (block, nk), 1) // VDIM

    def close(i, rel):
        pair = i % 2
        outs, sums = [], []
        for head in range(heads):
            rows = pl.ds(head * block, block)
            weight_sum = jnp.sum(sum_s[pair, rows, :], axis=-1, keepdims=True)
            outs.append(acc_s[pair, rows, :] / weight_sum)
            log_sum = jnp.broadcast_to(top_s[pair, rows, :1] + jnp.log2(weight_sum), (block, block))
            sums.append(jnp.sum(jnp.where(down == across, log_sum, 0.0), axis=0, keepdims=True))
        osend[i] = jnp.where(head_lane == 0, outs[0], outs[1]).astype(BF16)
        slot = y * NY + wrap(y + rel, NY)
        lget[core, slot] = jnp.concatenate(sums, axis=0)
        oget[core, slot] = osend[i, pl.ds(pl.multiple_of(t * own, own), own), :]
        for k in (2, 1, 3, 0):
            for c in range(2):
                def go_to(c=c, k=k):
                    device = dev(dy=k, c=c)
                    rows = pl.ds(pl.multiple_of(device[1] * own, own), own)
                    rc(osend.at[i, rows], oget.at[core, slot], s_f.at[0], r_f.at[0], device).start()
                    rc(lget.at[core, slot], lget.at[core, slot], s_f.at[1], r_f.at[1], device).start()
                if k:
                    go_to()
                else:
                    pl.when(core != c)(go_to)

    order = (0, 1, 3, 2)
    groups = [(ref, h, rel) for rel in order for ref, h in ((kown, 0), (koth, 0), (kown, 1), (koth, 1))]
    events = {
        0: [lambda: queries_of(0)],
        1: [lambda: a_part(2)],
        2: [wo_last],
        3: [lambda: heads_in(1)],
        7: [lambda: heads_in(3)],
        11: [lambda: heads_in(2)],
    }
    for j, (ref, h, rel) in enumerate(groups):
        for event in events.get(j, ()):
            event()
        if j == 1 or j == 3:
            got(koth.at[:, pl.ds(4 * h, 4)], r_d.at[h])
        expand(j)
        if j % 4 == 3 and j < 15:
            queries_of(groups[j + 1][2])
        if j >= 1:
            score(j - 1)
        if j >= 2:
            weigh(j - 2)
            if (j - 2) % 4 == 3:
                close((j - 2) // 4, groups[j - 2][2])
    last = len(groups) - 1
    score(last)
    weigh(last - 1)
    weigh(last)
    close(last // 4, groups[last][2])
    wo_cross()

    c_out.wait()
    got(lget.at[:, pl.ds(0, 14)], r_f.at[1])
    got(oget.at[:, pl.ds(0, 14)], r_f.at[0])
    spot = lax.broadcasted_iota(jnp.int32, (own, block), 0) + t * own
    spot = spot == lax.broadcasted_iota(jnp.int32, (own, block), 1)
    own_lane = lax.broadcasted_iota(jnp.int32, (own, nk), 1) // VDIM

    def column(row):
        return jnp.sum(jnp.where(spot, jnp.broadcast_to(row, (own, block)), 0.0), axis=-1, keepdims=True)

    got(wo.at[:, 0], r_wo.at[3])
    mixed = jnp.zeros((own, width), F32)
    for p in range(NY):
        merged = []
        for c in range(2):
            logs = [lget[c, q * NY + p] for q in range(NY)]
            most = jnp.maximum(jnp.maximum(logs[0], logs[1]), jnp.maximum(logs[2], logs[3]))
            shares = [jnp.exp2(log - most) for log in logs]
            whole = (shares[0] + shares[1]) + (shares[2] + shares[3])
            total = jnp.zeros((own, nk), F32)
            for q in range(NY):
                share = shares[q] / whole
                both = jnp.where(own_lane == 0, column(share[:1]), column(share[1:]))
                total = total + both * oget[c, q * NY + p].astype(F32)
            merged.append(total.astype(BF16))
        weights = jnp.concatenate([wo[p, c].reshape(width, nk) for c in range(2)], axis=1)
        mixed = mixed + dot_t(jnp.concatenate(merged, axis=1), weights)
    out[...] = rms(mixed.astype(BF16), gain_out[...])
    logs = [lget[core, q * NY + y] for q in range(NY)]
    most = jnp.maximum(jnp.maximum(logs[0], logs[1]), jnp.maximum(logs[2], logs[3]))
    shares = [jnp.exp2(log - most) for log in logs]
    whole = (shares[0] + shares[1]) + (shares[2] + shares[3])
    log_out[...] = most * math.log(2.0) + jnp.log(whole)

    for gather in (g_up, g_uq):
        gather.drain()
    sent(up.at[pl.ds(0, 3)], s_up.at[2])
    sent(uq.at[pl.ds(0, 3)], s_uq.at[2])
    sent(wo.at[:, 0], s_wo.at[3])
    sent(tok.at[core], s_tok.at[0])
    sent(kown.at[pl.ds(0, 3)], s_a.at[0])
    sent(kown, s_d.at[0])
    sent(oget.at[:, pl.ds(0, 14)], s_f.at[0])
    sent(lget.at[:, pl.ds(0, 14)], s_f.at[1])

    @pl.when(core == 1)
    def _():
        g_k.drain()
        g_wr.drain()
        g_w1.drain()
        sent(wo.at[pl.ds(0, 3), 1], s_wo.at[2])
        sent(kown.at[0, pl.ds(0, 7)], s_z.at[0])
        sent(kown.at[0], s_z.at[1])

    @pl.when(core == 0)
    def _():
        g_q.drain()
        g_w0.drain()
        sent(wo.at[pl.ds(0, 3), 0, 0, 0], s_wo.at[2])
        sent(ql, s_q.at[1])
        sent(ql.at[pl.ds(0, 3)], s_q.at[0])


def on_device(n, ntp, tokens, doc_ids, down_q, down_k, down_r, gain_q, gain_k, up_q, up_k, up_v, out_w, gain_o):
    own, width = tokens.shape
    block = doc_ids.shape[0]
    heads = up_k.shape[1] // NOPE
    rank = down_k.shape[1]
    nq, nk, nv = up_q.shape[1], up_k.shape[1], up_v.shape[1]
    turn_in, turn_block, pick, pick_key, mix = tables(n, block, heads)
    vmem = pl.BlockSpec(memory_space=pltpu.VMEM)
    hbm = pl.BlockSpec(memory_space=pl.ANY)
    dma = lambda k: pltpu.SemaphoreType.DMA((k,))
    v = lambda *shape, dtype=BF16: pltpu.VMEM(shape, dtype)
    rows = heads * block
    scratch = [
        pltpu.VMEM((1, block), jnp.int32), v(1, rank, dtype=F32), v(1, width, dtype=F32), v(1, 256, dtype=F32), v(ROPE, 256),
        v(128, 128), v(2 * own, width), v(width // n, ROPE), v(width, 128),
        v(2, own, width), v(NZ, NX, width // n, rank), v(NZ, NX, width // n // 4, 128, dtype=F32),
        v(NY, NZ, NX, rank // n, nq), v(NY, NZ, NX, rank // n, nk + nv), v(NY, 2, NZ, NX, width // n, nv),
        v(NY, rank, nq), v(NY, rank, nk + nv), v(NY, 2 * own, rank),
        v(NX, NZ, 5, own // 2, 128), v(NX, NZ, 5, own // 2, 128), v(5, own // 2, 128),
        v(block, 256, dtype=F32), v(block, 128, dtype=F32), v(block, 128, dtype=F32), v(*pick.shape),
        v(NY, 2, rows, 256),
        v(2, 2, rows, 256, dtype=F32), v(2, 2, 256, nk), v(3, 512, nv),
        v(2, rows, 128, dtype=F32), v(2, rows, 128, dtype=F32), v(2, rows, 128, dtype=F32),
        v(NY, block, nv), v(2, NY * NY, own, nv), v(2, NY * NY, heads, block, dtype=F32),
        pltpu.SemaphoreType.REGULAR,
        dma(15), dma(1), dma(1), dma(2), dma(8), dma(2), dma(8), dma(3), dma(5), dma(3), dma(5), dma(4), dma(4),
        dma(2), dma(1), dma(1), dma(7), dma(2), dma(3), dma(1), dma(2), dma(2), dma(2),
    ]
    mixed, log_sums = pl.pallas_call(
        functools.partial(kernel, n, ntp, heads),
        out_shape=(
            jax.ShapeDtypeStruct((own, width), BF16),
            jax.ShapeDtypeStruct((heads, block), F32),
        ),
        in_specs=[hbm] * 17,
        out_specs=(vmem, vmem),
        scratch_shapes=scratch,
        compiler_params=pltpu.CompilerParams(
            collective_id=0, has_side_effects=True, vmem_limit_bytes=60 * 1024 * 1024
        ),
    )(
        tokens, doc_ids[None, :], down_q, down_k, down_r, gain_q[None, :], gain_k[None, :],
        up_q, up_k, up_v, out_w.T, gain_o[None, :],
        jnp.asarray(turn_in), jnp.asarray(turn_block[:, None, :]), jnp.asarray(pick, BF16), jnp.asarray(pick_key, BF16), jnp.asarray(mix, BF16),
    )
    return mixed, log_sums.T


def solution(mesh):
    assert mesh.shape["tp"] == 2 * NY and mesh.shape["sp"] == NX * NZ
    placed = (
        P(("sp", "tp"), None), P("sp"), P("sp", None), P("sp", None), P("sp", None), P(), P(),
        P("sp", "tp"), P("sp", "tp"), P("sp", "tp"), P("tp", "sp"), P(),
    )
    return jax.shard_map(
        functools.partial(on_device, mesh.shape["sp"], mesh.shape["tp"]),
        mesh=mesh,
        in_specs=placed,
        out_specs=(P(("sp", "tp"), None), P("sp", "tp")),
        check_vma=False,
    )
```

```python
import functools
import math

import jax
import jax.numpy as jnp
import numpy as np
from jax import lax
from jax.experimental import pallas as pl
from jax.experimental.pallas import tpu as pltpu
from jax.sharding import PartitionSpec as P

NOPE = 64
ROPE = 32
VDIM = 64
THETA = 10000.0
EPS = 1e-06
MASKED = -1e30
MESH = pl.DeviceIdType.MESH
F32 = jnp.float32
BF16 = jnp.bfloat16
NX, NY, NZ = 4, 4, 8
NEAR = (0, 1, 7, 2, 6, 3, 5, 4)
ZPOS = {rel: pos for pos, rel in enumerate(NEAR)}


def dot(a, b):
    return jnp.dot(a, b, preferred_element_type=F32)


def dot_t(a, b):
    return lax.dot_general(a, b, (((1,), (1,)), ((), ())), preferred_element_type=F32)


def rms(values, gain):
    wide = values.astype(F32)
    scale = lax.rsqrt(jnp.mean(wide * wide, axis=-1, keepdims=True) + EPS)
    return (wide * scale * gain).astype(BF16)


def tables(n, block, heads):
    half = ROPE // 2
    inverse = np.float32(THETA) ** (-np.arange(half, dtype=np.float32) / np.float32(half))
    inverse = inverse.astype(np.float32).astype(np.float64)[None, :]

    def turn(positions):
        angles = positions.astype(np.float64)[:, None] * inverse
        both = np.zeros((len(positions), 256), np.float32)
        both[:, :ROPE] = np.tile(np.cos(angles), (1, 2))
        both[:, 128 : 128 + ROPE] = np.tile(np.sin(angles), (1, 2))
        return both

    width = NOPE + ROPE
    pick = np.zeros((heads * width, heads * 384), np.float32)
    eye = np.arange(NOPE)
    rot = np.arange(ROPE)
    low = np.arange(half)
    for head in range(heads):
        pick[head * width + eye, head * 384 + (head % 2) * NOPE + eye] = 1
        pick[head * width + NOPE + rot, head * 384 + 128 + rot] = 1
        pick[head * width + NOPE + half + low, head * 384 + 256 + low] = -1
        pick[head * width + NOPE + low, head * 384 + 256 + half + low] = 1
    pick_key = np.zeros((ROPE, 256), np.float32)
    pick_key[rot, rot] = 1
    pick_key[half + low, 128 + low] = -1
    pick_key[low, 128 + half + low] = 1
    mix = np.zeros((128, 128), np.float32)
    to = np.arange(128)
    mix[32 * (to // 8 % 4) + 8 * (to // 32) + to % 8, to] = 1
    return turn(np.arange(block)), turn(np.arange(n) * block), pick, pick_key, mix


def kernel(
    n, ntp, heads,
    tokens, docs_in, down_q, down_k, down_r, gain_q, gain_k, up_q, up_k, up_v, out_wt, gain_o,
    turn_in, turn_block, pick, pick_key, mix,
    out, log_out,
    docs, gain, gain_out, turn_me, sel_key, mix_in, tok_mix, wr_in, wr_flat,
    tok, w, wr, uq, up, wo, uq_flat, up_flat, ql, kown, koth, ks, tab, kdoc, qdoc, sel, qs,
    sbuf, kbuf, vbuf, top_s, sum_s, acc_s, osend, oget, lget,
    go, loc, s_tok, r_tok, s_w, r_w, s_wr, r_wr, s_uq, r_uq, s_up, r_up, s_wo, r_wo,
    s_q, r_q, s_a, r_a, s_z, r_z, s_d, r_d, s_f, r_f,
):
    me = lax.axis_index("sp")
    t = lax.axis_index("tp")
    z, x = me // NX, lax.rem(me, NX)
    y, core = t // 2, lax.rem(t, 2)
    own, width = tokens.shape
    block = ntp * own
    rows_all = heads * block

    def wrap(v, size):
        return lax.rem(v + size, size)

    def dev(dz=0, dx=0, dy=0, c=None):
        c = core if c is None else c
        zz = wrap(z + dz, NZ) if dz else z
        xx = wrap(x + dx, NX) if dx else x
        yy = wrap(y + dy, NY) if dy else y
        return (zz * NX + xx, yy * 2 + c)

    c_dev = dev(c=1 - core)

    def rc(src, dst, s, r, device):
        return pltpu.make_async_remote_copy(
            src_ref=src, dst_ref=dst, send_sem=s, recv_sem=r, device_id=device, device_id_type=MESH
        )

    def sent(ref, s):
        rc(ref, ref, s, s, c_dev).wait_send()

    def got(ref, r):
        rc(ref, ref, r, r, c_dev).wait_recv()

    barrier = pltpu.get_barrier_semaphore()
    others = [dev(dz=d) for d in range(1, NZ)] + [dev(dx=d) for d in range(1, NX)]
    others += [dev(dz=d, c=1 - core) for d in range(1, NZ)]
    others += [dev(dy=d) for d in range(1, NY)] + [dev(dy=d, c=1 - core) for d in range(NY)]
    for device in others:
        pl.semaphore_signal(barrier, inc=1, device_id=device, device_id_type=MESH)

    @pl.when(core == 1)
    def _():
        pltpu.make_async_copy(down_k, w.at[z, x], loc.at[1]).start()
        pltpu.make_async_copy(gain_k, gain, loc.at[9]).start()

    @pl.when(core == 0)
    def _():
        pltpu.make_async_copy(down_q, w.at[z, x], loc.at[1]).start()
        pltpu.make_async_copy(gain_q, gain, loc.at[9]).start()

    nq, nk = up_q.shape[1], up_k.shape[1]
    c_w = pltpu.make_async_copy(down_k, w.at[z, x], loc.at[1])
    c_gain = pltpu.make_async_copy(gain_k, gain, loc.at[9])
    c_docs = pltpu.make_async_copy(docs_in, docs, loc.at[10])
    c_tab = pltpu.make_async_copy(turn_in, tab, loc.at[7])
    c_me = pltpu.make_async_copy(turn_block.at[me], turn_me, loc.at[11])
    c_tok = pltpu.make_async_copy(tokens, tok.at[core], loc.at[0])
    c_wr = pltpu.make_async_copy(down_r, wr_in, loc.at[2])
    c_mix = pltpu.make_async_copy(mix, mix_in, loc.at[14])
    c_uq = pltpu.make_async_copy(up_q, uq.at[0, z, x], loc.at[3])
    c_up = [
        pltpu.make_async_copy(up_k, up.at[0, z, x, :, pl.ds(0, nk)], loc.at[4]),
        pltpu.make_async_copy(up_v, up.at[0, z, x, :, pl.ds(nk, nk)], loc.at[5]),
    ]
    c_wo = pltpu.make_async_copy(out_wt, wo.at[y, core, z, x], loc.at[6])
    c_sel = pltpu.make_async_copy(pick, sel, loc.at[8])
    c_key = pltpu.make_async_copy(pick_key, sel_key, loc.at[12])
    c_out = pltpu.make_async_copy(gain_o, gain_out, loc.at[13])
    for copy in [c_docs, c_tab, c_me, c_wr, c_tok, c_uq] + c_up + [c_key, c_mix, c_wo, c_sel, c_out]:
        copy.start()

    down = lax.broadcasted_iota(jnp.int32, (block, block), 0)
    across = lax.broadcasted_iota(jnp.int32, (block, block), 1)
    c_docs.wait()
    doc_row = jnp.broadcast_to(docs[...].astype(F32), (block, block))
    doc_col = jnp.sum(jnp.where(down == across, doc_row, 0.0), axis=-1, keepdims=True)
    lane = lax.broadcasted_iota(jnp.int32, (block, 128), 1)
    in_docs = (lane >= ROPE) & (lane < ROPE + n)
    same = doc_col == (lane - ROPE).astype(F32)
    kdoc[...] = jnp.where(in_docs & same, 1.0, 0.0)
    qdoc[...] = jnp.where(in_docs & jnp.logical_not(same), MASKED, 0.0)
    c_tab.wait()
    c_me.wait()
    cos_a, sin_a = turn_me[:, :128], turn_me[:, 128:]
    cos_b, sin_b = tab[:, :128], tab[:, 128:]
    tab[:, :128] = cos_a * cos_b - sin_a * sin_b
    tab[:, 128:] = sin_a * cos_b + cos_a * sin_b

    rank = uq_flat.shape[1]
    c_wr.wait()
    wide_r = wr_in[...].astype(F32)
    wr[z, x] = jnp.concatenate([wide_r[8 * q : 8 * q + 8] for q in range(4)], axis=1)
    for copy in [c_w, c_tok, c_uq] + c_up + [c_key, c_mix, c_gain, c_wo]:
        copy.wait()
    pl.semaphore_wait(barrier, len(others))

    class Gather:
        def __init__(self, at, s, r):
            self.at, self.s, self.r = at, s, r

        def start_z(self):
            here = self.at(z, x)
            for d in reversed(NEAR[1:]):
                rc(here, here, self.s.at[0], self.r.at[0], dev(dz=d)).start()

        def start_x(self):
            got(self.at(pl.ds(0, NZ - 1), x), self.r.at[0])
            column = self.at(slice(None), x)
            for k in (2, 1, -1):
                rc(column, column, self.s.at[1], self.r.at[1], dev(dx=k)).start()

        def finish(self):
            got(self.at(pl.ds(0, NZ - 2), slice(None)), self.r.at[1])

        def drain(self):
            sent(self.at(pl.ds(0, NZ - 1), 0), self.s.at[0])
            sent(self.at(pl.ds(0, NZ - 2), slice(None)), self.s.at[1])

    class Pieces(Gather):
        def start_z(self):
            here = self.at(z, x)
            for d in reversed(NEAR[1:]):
                rc(here, here, self.s.at[0], self.r.at[d], dev(dz=d)).start()

        def pass_x(self, d):
            here = self.at(wrap(z - d, NZ), x)
            if d > 0:
                got(here, self.r.at[d])
            for k in (2, 1, -1):
                rc(here, here, self.s.at[1], self.r.at[0], dev(dx=k)).start()

        def finish(self):
            got(self.at(pl.ds(0, NZ - 2), slice(None)), self.r.at[0])

    g_k = Pieces(lambda i, j: w.at[i, j], s_w, r_w)
    g_wr = Pieces(lambda i, j: wr.at[i, j], s_wr, r_wr)
    g_q = Gather(lambda i, j: w.at[i, j], s_w, r_w)
    g_uq = Gather(lambda i, j: uq.at[0, i, j], s_uq, r_uq)
    g_up = Gather(lambda i, j: up.at[0, i, j], s_up, r_up)
    g_w0 = Gather(lambda i, j: wo.at[:, 0, i, j], s_wo, r_wo)
    g_w1 = Gather(lambda i, j: wo.at[y, 1, i, j], s_wo, r_wo)

    def wo_y():
        here = wo.at[y, 0, z, x]
        for k in (2, 1, 3):
            rc(here, here, s_wo.at[2], r_wo.at[2], dev(dy=k)).start()

    def wo_z():
        got(wo.at[pl.ds(0, 3), 0, z, x], r_wo.at[2])
        g_w0.start_z()

    def wo_last():
        pl.when(core == 0)(g_w0.start_x)

        @pl.when(core == 1)
        def _():
            g_w1.finish()
            here = wo.at[y, 1]
            for k in (2, 1, 3):
                rc(here, here, s_wo.at[2], r_wo.at[2], dev(dy=k)).start()

    def wo_cross():
        pl.when(core == 0)(g_w0.finish)

        @pl.when(core == 1)
        def _():
            got(wo.at[pl.ds(0, 3), 1], r_wo.at[2])

        here = wo.at[:, core]
        rc(here, here, s_wo.at[3], r_wo.at[3], c_dev).start()

    def heads_y(steps):
        for k in steps:
            rel = -k % NY
            rc(up.at[0], up.at[rel], s_up.at[2], r_up.at[1 + rel], dev(dy=k)).start()
            rc(uq.at[0], uq.at[rel], s_uq.at[2], r_uq.at[1 + rel], dev(dy=k)).start()

    def heads_in(rel):
        if rel:
            got(up.at[rel], r_up.at[1 + rel])
            got(uq.at[rel], r_uq.at[1 + rel])
        for j in range(n):
            up_flat[rel, j * 8 : (j + 1) * 8, :] = up[rel, j // NX, j % NX]
            uq_flat[rel, j * 8 : (j + 1) * 8, :] = uq[rel, j // NX, j % NX]

    here = tok.at[core]
    c_partner = rc(here, here, s_tok.at[0], r_tok.at[0], c_dev)

    @pl.when(core == 1)
    def _():
        g_k.start_z()
        g_wr.start_z()
        g_k.pass_x(0)
        g_wr.pass_x(0)
        c_partner.start()
        g_up.start_z()
        g_uq.start_z()
        g_w1.start_z()
        for d in NEAR[1:]:
            g_k.pass_x(d)
            g_wr.pass_x(d)
            if d == 1:
                pl.semaphore_signal(go, inc=1, device_id=c_dev, device_id_type=MESH)
        g_up.start_x()
        g_uq.start_x()
        got(tok.at[1 - core], r_tok.at[0])
        both_tokens = tok[...].reshape(2 * own, width)
        for j in range(width // 128):
            cut = slice(j * 128, (j + 1) * 128)
            tok_mix[:, cut] = dot(both_tokens[:, cut], mix_in[...]).astype(BF16)
        g_wr.finish()
        packed = wr[...].reshape(rank, 128)
        for q in range(4):
            turned = (pltpu.roll(packed, 128 - 32 * q, 1) if q else packed).astype(BF16)
            for j in range(width // 128):
                wr_flat[j * 128 + q * 32 : j * 128 + (q + 1) * 32, :] = turned[j * 32 : (j + 1) * 32]
        g_k.finish()

    @pl.when(core == 0)
    def _():
        c_partner.start()
        wo_y()
        g_up.start_z()
        g_uq.start_z()
        pl.semaphore_wait(go, 1)
        g_q.start_z()
        g_q.start_x()
        g_up.start_x()
        g_uq.start_x()
        wo_z()

    def project():
        raw = dot(tok[...].reshape(2 * own, width), w[...].reshape(width, w.shape[-1])).astype(BF16)
        return rms(raw, gain[...])

    @pl.when(core == 1)
    def _():
        lat = project()
        rotary = dot(tok_mix[...], wr_flat[...])[:, :ROPE].astype(BF16)
        both = dot(rotary, sel_key[...])
        rows = pl.ds(pl.multiple_of(y * (2 * own), 2 * own), 2 * own)
        turned = both[:, :128] * tab[rows, :128] + both[:, 128:] * tab[rows, 128:] + kdoc[rows, :]
        half = own // 2
        for stripe in range(2):
            first = stripe * own
            parts = [
                lat[first + s * half : first + (s + 1) * half, h * 128 : (h + 1) * 128]
                for s in range(2)
                for h in range(2)
            ]
            packed = turned[first : first + half] + pltpu.roll(turned[first + half : first + own], 64, 1)
            parts.append(packed.astype(BF16))
            for i, tile in enumerate(parts):
                if stripe == 1:
                    kown[0, 0, i] = tile
                else:
                    ks[i] = tile
        here = kown.at[0, 0]
        rc(ks, here, s_z.at[1], r_z.at[2], dev(c=0)).start()
        for k in (2, 1, 3):
            rc(here, kown.at[-k % NX, 0], s_a.at[0], r_a.at[0], dev(dx=k)).start()
        for d in (4, 1, 7, 6, 2, 3, 5):
            pos = ZPOS[-d % NZ]
            rc(ks, kown.at[0, pos], s_z.at[1], r_z.at[0 if pos < 4 else 1], dev(dz=d, c=0)).start()

    parts = ((0, 1), (1, 3), (4, 4))

    def a_send(p):
        first, length = parts[p]
        src = kown.at[0, pl.ds(first, length)]
        for k in (2, 1, 3):
            rel = -k % NX
            sem = r_a.at[0] if p == 0 else r_a.at[3 * p - 3 + rel]
            rc(src, kown.at[rel, pl.ds(first, length)], s_a.at[0], sem, dev(dx=k)).start()

    def cross(a, count, p):
        cut = pl.ds(*parts[p])
        src, dst = kown.at[pl.ds(a, count), cut], koth.at[pl.ds(a, count), cut]
        rc(src, dst, s_d.at[0], r_d.at[1 if p == 2 else 0], c_dev).start()

    def z_part(p):
        if p == 0:
            got(kown.at[0, 0], r_z.at[2])
        else:
            got(kown.at[0, pl.ds(*parts[p])], r_z.at[p - 1])
        a_send(p)
        cross(0, 1, p)

    def a_part(p):
        if p == 0:
            got(kown.at[pl.ds(1, 3), 0], r_a.at[0])
            cross(1, 3, 0)
        else:
            for rel in (1, 3, 2):
                got(kown.at[rel, pl.ds(*parts[p])], r_a.at[3 * p - 3 + rel])
                cross(rel, 1, p)

    def rows_of(h):
        cut = pl.ds(1, 3) if h == 0 else pl.ds(4, 4)
        got(kown.at[:, cut], r_z.at[h])
        cut = pl.ds(4 * h, 4)
        rc(kown.at[:, cut], koth.at[:, cut], s_d.at[0], r_d.at[h], c_dev).start()

    @pl.when(core == 0)
    def _():
        z_part(0)
        got(tok.at[1 - core], r_tok.at[0])
        g_q.finish()
        ql[y] = project()
        here = ql.at[y]
        for k in (2, 1, 3):
            for c in range(2):
                rc(here, here, s_q.at[c], r_q.at[0], dev(dy=k, c=c)).start()
        rc(here, here, s_q.at[1], r_q.at[0], dev(c=1)).start()
        g_up.finish()
        g_uq.finish()
        heads_y((1, 3))
        a_part(0)
        z_part(1)
        z_part(2)
        heads_y((2,))

    @pl.when(core == 1)
    def _():
        g_up.finish()
        g_uq.finish()
        heads_y((1, 3))
        got(kown.at[pl.ds(1, 3), 0], r_a.at[0])
        for d in (1, 7, 6, 4, 3, 5, 2):
            pos = ZPOS[-d % NZ]
            rc(kown.at[:, 0], kown.at[:, pos], s_z.at[0], r_z.at[0 if pos < 4 else 1], dev(dz=d)).start()
        g_w1.start_x()

    heads_in(0)

    @pl.when(core == 0)
    def _():
        a_part(1)

    @pl.when(core == 1)
    def _():
        rows_of(0)
        heads_y((2,))

    @pl.when(core == 1)
    def _():
        got(ql, r_q.at[0])

    @pl.when(core == 0)
    def _():
        got(ql.at[pl.ds(0, 3)], r_q.at[0])

    c_sel.wait()
    scale = 1.0 / math.sqrt(NOPE + ROPE)
    factor = scale * math.log2(math.e)

    def queries_of(rel):
        projected = dot(ql[...].reshape(block, ql.shape[-1]), uq_flat[rel]).astype(BF16)
        for head in range(heads):
            laid = dot(projected, sel[:, head * 384 : (head + 1) * 384])
            turned = (laid[:, 128:256] * tab[:, :128] + laid[:, 256:] * tab[:, 128:]) * factor + qdoc[...]
            plain = (laid[:, :128] * factor).astype(BF16)
            rows = pl.ds(head * block, block)
            qs[rel, 0, rows, :128] = plain
            qs[rel, 1, rows, :128] = plain
            qs[rel, 0, rows, 128:] = turned.astype(BF16)
            qs[rel, 1, rows, 128:] = pltpu.roll(turned, 64, 1).astype(BF16)

    def tiles(ref, h, i):
        return ref[:, 4 * h : 4 * h + 4, i].reshape(256, 128)

    def expand(j):
        ref, h, rel = groups[j]
        for s in range(2):
            lat = jnp.concatenate([tiles(ref, h, 2 * s), tiles(ref, h, 2 * s + 1)], axis=1)
            kv = dot(lat, up_flat[rel]).astype(BF16)
            kbuf[j % 2, s] = kv[:, :nk]
            vbuf[j % 3, s * 256 : (s + 1) * 256, :] = kv[:, nk:]

    def score(j):
        ref, h, rel = groups[j]
        rot = tiles(ref, h, 4)
        for s in range(2):
            sbuf[j % 2, s] = dot_t(qs[rel, s], jnp.concatenate([kbuf[j % 2, s], rot], axis=1))

    step = 128

    def weigh(j):
        par, first, pair = j % 2, j % 4 == 0, j // 4 % 2
        for r in range(0, rows_all, step):
            rows = pl.ds(r, step)
            parts = [sbuf[par, s, rows, h * 128 : (h + 1) * 128] for s in range(2) for h in range(2)]
            most = jnp.maximum(jnp.maximum(parts[0], parts[1]), jnp.maximum(parts[2], parts[3]))
            most = jnp.max(most, axis=-1, keepdims=True)
            if first:
                new = jnp.broadcast_to(most, (step, 128))
            else:
                old = top_s[pair, rows, :]
                new = jnp.maximum(old, most)
                alpha = jnp.exp2(old - new)
            weights = [jnp.exp2(p - new) for p in parts]
            total = (weights[0] + weights[1]) + (weights[2] + weights[3])
            mixed = dot(jnp.concatenate([p.astype(BF16) for p in weights], axis=1), vbuf[j % 3])
            top_s[pair, rows, :] = new
            if first:
                sum_s[pair, rows, :] = total
                acc_s[pair, rows, :] = mixed
            else:
                sum_s[pair, rows, :] = sum_s[pair, rows, :] * alpha + total
                acc_s[pair, rows, :] = acc_s[pair, rows, :] * alpha + mixed

    head_lane = lax.broadcasted_iota(jnp.int32, (block, nk), 1) // VDIM

    def close(i, rel):
        pair = i % 2
        outs, sums = [], []
        for head in range(heads):
            rows = pl.ds(head * block, block)
            weight_sum = jnp.sum(sum_s[pair, rows, :], axis=-1, keepdims=True)
            outs.append(acc_s[pair, rows, :] / weight_sum)
            log_sum = jnp.broadcast_to(top_s[pair, rows, :1] + jnp.log2(weight_sum), (block, block))
            sums.append(jnp.sum(jnp.where(down == across, log_sum, 0.0), axis=0, keepdims=True))
        osend[i] = jnp.where(head_lane == 0, outs[0], outs[1]).astype(BF16)
        slot = y * NY + wrap(y + rel, NY)
        lget[core, slot] = jnp.concatenate(sums, axis=0)
        oget[core, slot] = osend[i, pl.ds(pl.multiple_of(t * own, own), own), :]
        for k in (2, 1, 3, 0):
            for c in range(2):
                def go_to(c=c, k=k):
                    device = dev(dy=k, c=c)
                    rows = pl.ds(pl.multiple_of(device[1] * own, own), own)
                    rc(osend.at[i, rows], oget.at[core, slot], s_f.at[0], r_f.at[0], device).start()
                    rc(lget.at[core, slot], lget.at[core, slot], s_f.at[1], r_f.at[1], device).start()
                if k:
                    go_to()
                else:
                    pl.when(core != c)(go_to)

    order = (0, 1, 3, 2)
    groups = [(ref, h, rel) for rel in order for ref, h in ((kown, 0), (koth, 0), (kown, 1), (koth, 1))]
    def second_half():
        pl.when(core == 0)(lambda: a_part(2))
        pl.when(core == 1)(lambda: rows_of(1))

    events = {
        0: [lambda: queries_of(0)],
        2: [second_half],
        3: [lambda: heads_in(1)],
        4: [wo_last],
        7: [lambda: heads_in(3)],
        11: [lambda: heads_in(2)],
    }
    for j, (ref, h, rel) in enumerate(groups):
        for event in events.get(j, ()):
            event()
        if j == 1 or j == 3:
            got(koth.at[:, pl.ds(4 * h, 4)], r_d.at[h])
        expand(j)
        if j % 4 == 3 and j < 15:
            queries_of(groups[j + 1][2])
        if j >= 1:
            score(j - 1)
        if j >= 2:
            weigh(j - 2)
            if (j - 2) % 4 == 3:
                close((j - 2) // 4, groups[j - 2][2])
    last = len(groups) - 1
    score(last)
    weigh(last - 1)
    weigh(last)
    close(last // 4, groups[last][2])
    wo_cross()

    c_out.wait()
    got(lget.at[:, pl.ds(0, 14)], r_f.at[1])
    got(oget.at[:, pl.ds(0, 14)], r_f.at[0])
    spot = lax.broadcasted_iota(jnp.int32, (own, block), 0) + t * own
    spot = spot == lax.broadcasted_iota(jnp.int32, (own, block), 1)
    own_lane = lax.broadcasted_iota(jnp.int32, (own, nk), 1) // VDIM

    def column(row):
        return jnp.sum(jnp.where(spot, jnp.broadcast_to(row, (own, block)), 0.0), axis=-1, keepdims=True)

    got(wo.at[:, 0], r_wo.at[3])
    mixed = jnp.zeros((own, width), F32)
    for p in range(NY):
        merged = []
        for c in range(2):
            logs = [lget[c, q * NY + p] for q in range(NY)]
            most = jnp.maximum(jnp.maximum(logs[0], logs[1]), jnp.maximum(logs[2], logs[3]))
            shares = [jnp.exp2(log - most) for log in logs]
            whole = (shares[0] + shares[1]) + (shares[2] + shares[3])
            total = jnp.zeros((own, nk), F32)
            for q in range(NY):
                share = shares[q] / whole
                both = jnp.where(own_lane == 0, column(share[:1]), column(share[1:]))
                total = total + both * oget[c, q * NY + p].astype(F32)
            merged.append(total.astype(BF16))
        weights = jnp.concatenate([wo[p, c].reshape(width, nk) for c in range(2)], axis=1)
        mixed = mixed + dot_t(jnp.concatenate(merged, axis=1), weights)
    out[...] = rms(mixed.astype(BF16), gain_out[...])
    logs = [lget[core, q * NY + y] for q in range(NY)]
    most = jnp.maximum(jnp.maximum(logs[0], logs[1]), jnp.maximum(logs[2], logs[3]))
    shares = [jnp.exp2(log - most) for log in logs]
    whole = (shares[0] + shares[1]) + (shares[2] + shares[3])
    log_out[...] = most * math.log(2.0) + jnp.log(whole)

    for gather in (g_up, g_uq):
        gather.drain()
    sent(up.at[pl.ds(0, 3)], s_up.at[2])
    sent(uq.at[pl.ds(0, 3)], s_uq.at[2])
    sent(wo.at[:, 0], s_wo.at[3])
    sent(tok.at[core], s_tok.at[0])
    sent(kown, s_d.at[0])
    sent(oget.at[:, pl.ds(0, 14)], s_f.at[0])
    sent(lget.at[:, pl.ds(0, 14)], s_f.at[1])

    @pl.when(core == 1)
    def _():
        g_k.drain()
        g_wr.drain()
        g_w1.drain()
        sent(wo.at[pl.ds(0, 3), 1], s_wo.at[2])
        sent(kown.at[:, pl.ds(0, 7)], s_z.at[0])
        sent(kown.at[0], s_z.at[1])
        sent(kown.at[pl.ds(0, 3), 0], s_a.at[0])

    @pl.when(core == 0)
    def _():
        g_q.drain()
        g_w0.drain()
        sent(kown.at[pl.ds(0, 3)], s_a.at[0])
        sent(wo.at[pl.ds(0, 3), 0, 0, 0], s_wo.at[2])
        sent(ql, s_q.at[1])
        sent(ql.at[pl.ds(0, 3)], s_q.at[0])


def on_device(n, ntp, tokens, doc_ids, down_q, down_k, down_r, gain_q, gain_k, up_q, up_k, up_v, out_w, gain_o):
    own, width = tokens.shape
    block = doc_ids.shape[0]
    heads = up_k.shape[1] // NOPE
    rank = down_k.shape[1]
    nq, nk, nv = up_q.shape[1], up_k.shape[1], up_v.shape[1]
    turn_in, turn_block, pick, pick_key, mix = tables(n, block, heads)
    vmem = pl.BlockSpec(memory_space=pltpu.VMEM)
    hbm = pl.BlockSpec(memory_space=pl.ANY)
    dma = lambda k: pltpu.SemaphoreType.DMA((k,))
    v = lambda *shape, dtype=BF16: pltpu.VMEM(shape, dtype)
    rows = heads * block
    scratch = [
        pltpu.VMEM((1, block), jnp.int32), v(1, rank, dtype=F32), v(1, width, dtype=F32), v(1, 256, dtype=F32), v(ROPE, 256),
        v(128, 128), v(2 * own, width), v(width // n, ROPE), v(width, 128),
        v(2, own, width), v(NZ, NX, width // n, rank), v(NZ, NX, width // n // 4, 128, dtype=F32),
        v(NY, NZ, NX, rank // n, nq), v(NY, NZ, NX, rank // n, nk + nv), v(NY, 2, NZ, NX, width // n, nv),
        v(NY, rank, nq), v(NY, rank, nk + nv), v(NY, 2 * own, rank),
        v(NX, NZ, 5, own // 2, 128), v(NX, NZ, 5, own // 2, 128), v(5, own // 2, 128),
        v(block, 256, dtype=F32), v(block, 128, dtype=F32), v(block, 128, dtype=F32), v(*pick.shape),
        v(NY, 2, rows, 256),
        v(2, 2, rows, 256, dtype=F32), v(2, 2, 256, nk), v(3, 512, nv),
        v(2, rows, 128, dtype=F32), v(2, rows, 128, dtype=F32), v(2, rows, 128, dtype=F32),
        v(NY, block, nv), v(2, NY * NY, own, nv), v(2, NY * NY, heads, block, dtype=F32),
        pltpu.SemaphoreType.REGULAR,
        dma(15), dma(1), dma(1), dma(2), dma(8), dma(2), dma(8), dma(3), dma(5), dma(3), dma(5), dma(4), dma(4),
        dma(2), dma(1), dma(1), dma(7), dma(2), dma(3), dma(1), dma(2), dma(2), dma(2),
    ]
    mixed, log_sums = pl.pallas_call(
        functools.partial(kernel, n, ntp, heads),
        out_shape=(
            jax.ShapeDtypeStruct((own, width), BF16),
            jax.ShapeDtypeStruct((heads, block), F32),
        ),
        in_specs=[hbm] * 17,
        out_specs=(vmem, vmem),
        scratch_shapes=scratch,
        compiler_params=pltpu.CompilerParams(
            collective_id=0, has_side_effects=True, vmem_limit_bytes=60 * 1024 * 1024
        ),
    )(
        tokens, doc_ids[None, :], down_q, down_k, down_r, gain_q[None, :], gain_k[None, :],
        up_q, up_k, up_v, out_w.T, gain_o[None, :],
        jnp.asarray(turn_in), jnp.asarray(turn_block[:, None, :]), jnp.asarray(pick, BF16), jnp.asarray(pick_key, BF16), jnp.asarray(mix, BF16),
    )
    return mixed, log_sums.T


def solution(mesh):
    assert mesh.shape["tp"] == 2 * NY and mesh.shape["sp"] == NX * NZ
    placed = (
        P(("sp", "tp"), None), P("sp"), P("sp", None), P("sp", None), P("sp", None), P(), P(),
        P("sp", "tp"), P("sp", "tp"), P("sp", "tp"), P("tp", "sp"), P(),
    )
    return jax.shard_map(
        functools.partial(on_device, mesh.shape["sp"], mesh.shape["tp"]),
        mesh=mesh,
        in_specs=placed,
        out_specs=(P(("sp", "tp"), None), P("sp", "tp")),
        check_vma=False,
    )
```

```python
import functools
import math

import jax
import jax.numpy as jnp
import numpy as np
from jax import lax
from jax.experimental import pallas as pl
from jax.experimental.pallas import tpu as pltpu
from jax.sharding import PartitionSpec as P

NOPE = 64
ROPE = 32
VDIM = 64
THETA = 10000.0
EPS = 1e-06
MASKED = -1e30
MESH = pl.DeviceIdType.MESH
F32 = jnp.float32
BF16 = jnp.bfloat16
NX, NY, NZ = 4, 4, 8
NEAR = (0, 1, 7, 2, 6, 3, 5, 4)
ZPOS = {rel: pos for pos, rel in enumerate(NEAR)}


def dot(a, b):
    return jnp.dot(a, b, preferred_element_type=F32)


def dot_t(a, b):
    return lax.dot_general(a, b, (((1,), (1,)), ((), ())), preferred_element_type=F32)


def rms(values, gain):
    wide = values.astype(F32)
    scale = lax.rsqrt(jnp.mean(wide * wide, axis=-1, keepdims=True) + EPS)
    return (wide * scale * gain).astype(BF16)


def tables(n, block, heads):
    half = ROPE // 2
    inverse = np.float32(THETA) ** (-np.arange(half, dtype=np.float32) / np.float32(half))
    inverse = inverse.astype(np.float32).astype(np.float64)[None, :]

    def turn(positions):
        angles = positions.astype(np.float64)[:, None] * inverse
        both = np.zeros((len(positions), 256), np.float32)
        both[:, :ROPE] = np.tile(np.cos(angles), (1, 2))
        both[:, 128 : 128 + ROPE] = np.tile(np.sin(angles), (1, 2))
        return both

    width = NOPE + ROPE
    pick = np.zeros((heads * width, heads * 384), np.float32)
    eye = np.arange(NOPE)
    rot = np.arange(ROPE)
    low = np.arange(half)
    for head in range(heads):
        pick[head * width + eye, head * 384 + (head % 2) * NOPE + eye] = 1
        pick[head * width + NOPE + rot, head * 384 + 128 + rot] = 1
        pick[head * width + NOPE + half + low, head * 384 + 256 + low] = -1
        pick[head * width + NOPE + low, head * 384 + 256 + half + low] = 1
    pick_key = np.zeros((ROPE, 256), np.float32)
    pick_key[rot, rot] = 1
    pick_key[half + low, 128 + low] = -1
    pick_key[low, 128 + half + low] = 1
    mix = np.zeros((128, 128), np.float32)
    to = np.arange(128)
    mix[32 * (to // 8 % 4) + 8 * (to // 32) + to % 8, to] = 1
    return turn(np.arange(block)), turn(np.arange(n) * block), pick, pick_key, mix


def kernel(
    n, ntp, heads,
    tokens, docs_in, down_q, down_k, down_r, gain_q, gain_k, up_q, up_k, up_v, out_wt, gain_o,
    turn_in, turn_block, pick, pick_key, mix,
    out, log_out,
    docs, gain, gain_out, turn_me, sel_key, mix_in, tok_mix, wr_in, wr_flat,
    tok, w, wr, uq, up, wo, uq_flat, up_flat, ql, kown, koth, ks, tab, kdoc, qdoc, sel, qs,
    sbuf, kbuf, vbuf, top_s, sum_s, acc_s, osend, oget, lget,
    go, loc, s_tok, r_tok, s_w, r_w, s_wr, r_wr, s_uq, r_uq, s_up, r_up, s_wo, r_wo,
    s_q, r_q, s_a, r_a, s_z, r_z, s_d, r_d, s_f, r_f,
):
    me = lax.axis_index("sp")
    t = lax.axis_index("tp")
    z, x = me // NX, lax.rem(me, NX)
    y, core = t // 2, lax.rem(t, 2)
    own, width = tokens.shape
    block = ntp * own
    rows_all = heads * block

    def wrap(v, size):
        return lax.rem(v + size, size)

    def dev(dz=0, dx=0, dy=0, c=None):
        c = core if c is None else c
        zz = wrap(z + dz, NZ) if dz else z
        xx = wrap(x + dx, NX) if dx else x
        yy = wrap(y + dy, NY) if dy else y
        return (zz * NX + xx, yy * 2 + c)

    c_dev = dev(c=1 - core)

    def rc(src, dst, s, r, device):
        return pltpu.make_async_remote_copy(
            src_ref=src, dst_ref=dst, send_sem=s, recv_sem=r, device_id=device, device_id_type=MESH
        )

    def sent(ref, s):
        rc(ref, ref, s, s, c_dev).wait_send()

    def got(ref, r):
        rc(ref, ref, r, r, c_dev).wait_recv()

    barrier = pltpu.get_barrier_semaphore()
    others = [dev(dz=d) for d in range(1, NZ)] + [dev(dx=d) for d in range(1, NX)]
    others += [dev(dz=d, c=1 - core) for d in range(1, NZ)]
    others += [dev(dy=d) for d in range(1, NY)] + [dev(dy=d, c=1 - core) for d in range(NY)]
    for device in others:
        pl.semaphore_signal(barrier, inc=1, device_id=device, device_id_type=MESH)

    @pl.when(core == 1)
    def _():
        pltpu.make_async_copy(down_k, w.at[z, x], loc.at[1]).start()
        pltpu.make_async_copy(gain_k, gain, loc.at[9]).start()

    @pl.when(core == 0)
    def _():
        pltpu.make_async_copy(down_q, w.at[z, x], loc.at[1]).start()
        pltpu.make_async_copy(gain_q, gain, loc.at[9]).start()

    nq, nk = up_q.shape[1], up_k.shape[1]
    c_w = pltpu.make_async_copy(down_k, w.at[z, x], loc.at[1])
    c_gain = pltpu.make_async_copy(gain_k, gain, loc.at[9])
    c_docs = pltpu.make_async_copy(docs_in, docs, loc.at[10])
    c_tab = pltpu.make_async_copy(turn_in, tab, loc.at[7])
    c_me = pltpu.make_async_copy(turn_block.at[me], turn_me, loc.at[11])
    c_tok = pltpu.make_async_copy(tokens, tok.at[core], loc.at[0])
    c_wr = pltpu.make_async_copy(down_r, wr_in, loc.at[2])
    c_mix = pltpu.make_async_copy(mix, mix_in, loc.at[14])
    c_uq = pltpu.make_async_copy(up_q, uq.at[0, z, x], loc.at[3])
    c_up = [
        pltpu.make_async_copy(up_k, up.at[0, z, x, :, pl.ds(0, nk)], loc.at[4]),
        pltpu.make_async_copy(up_v, up.at[0, z, x, :, pl.ds(nk, nk)], loc.at[5]),
    ]
    c_wo = pltpu.make_async_copy(out_wt, wo.at[y, core, z, x], loc.at[6])
    c_sel = pltpu.make_async_copy(pick, sel, loc.at[8])
    c_key = pltpu.make_async_copy(pick_key, sel_key, loc.at[12])
    c_out = pltpu.make_async_copy(gain_o, gain_out, loc.at[13])
    for copy in [c_docs, c_tab, c_me, c_wr, c_tok, c_uq] + c_up + [c_key, c_mix, c_wo, c_sel, c_out]:
        copy.start()

    down = lax.broadcasted_iota(jnp.int32, (block, block), 0)
    across = lax.broadcasted_iota(jnp.int32, (block, block), 1)
    c_docs.wait()
    doc_row = jnp.broadcast_to(docs[...].astype(F32), (block, block))
    doc_col = jnp.sum(jnp.where(down == across, doc_row, 0.0), axis=-1, keepdims=True)
    lane = lax.broadcasted_iota(jnp.int32, (block, 128), 1)
    in_docs = (lane >= ROPE) & (lane < ROPE + n)
    same = doc_col == (lane - ROPE).astype(F32)
    kdoc[...] = jnp.where(in_docs & same, 1.0, 0.0)
    qdoc[...] = jnp.where(in_docs & jnp.logical_not(same), MASKED, 0.0)
    c_tab.wait()
    c_me.wait()
    cos_a, sin_a = turn_me[:, :128], turn_me[:, 128:]
    cos_b, sin_b = tab[:, :128], tab[:, 128:]
    tab[:, :128] = cos_a * cos_b - sin_a * sin_b
    tab[:, 128:] = sin_a * cos_b + cos_a * sin_b

    rank = uq_flat.shape[1]
    c_wr.wait()
    wide_r = wr_in[...].astype(F32)
    wr[z, x] = jnp.concatenate([wide_r[8 * q : 8 * q + 8] for q in range(4)], axis=1)
    for copy in [c_w, c_tok, c_uq] + c_up + [c_key, c_mix, c_gain, c_wo]:
        copy.wait()
    pl.semaphore_wait(barrier, len(others))

    class Gather:
        def __init__(self, at, s, r):
            self.at, self.s, self.r = at, s, r

        def start_z(self):
            here = self.at(z, x)
            for d in reversed(NEAR[1:]):
                rc(here, here, self.s.at[0], self.r.at[0], dev(dz=d)).start()

        def start_x(self):
            got(self.at(pl.ds(0, NZ - 1), x), self.r.at[0])
            column = self.at(slice(None), x)
            for k in (2, 1, -1):
                rc(column, column, self.s.at[1], self.r.at[1], dev(dx=k)).start()

        def finish(self):
            got(self.at(pl.ds(0, NZ - 2), slice(None)), self.r.at[1])

        def drain(self):
            sent(self.at(pl.ds(0, NZ - 1), 0), self.s.at[0])
            sent(self.at(pl.ds(0, NZ - 2), slice(None)), self.s.at[1])

    class Pieces(Gather):
        def start_z(self):
            here = self.at(z, x)
            for d in reversed(NEAR[1:]):
                rc(here, here, self.s.at[0], self.r.at[d], dev(dz=d)).start()

        def pass_x(self, d):
            here = self.at(wrap(z - d, NZ), x)
            if d > 0:
                got(here, self.r.at[d])
            for k in (2, 1, -1):
                rc(here, here, self.s.at[1], self.r.at[0], dev(dx=k)).start()

        def finish(self):
            got(self.at(pl.ds(0, NZ - 2), slice(None)), self.r.at[0])

    g_k = Pieces(lambda i, j: w.at[i, j], s_w, r_w)
    g_wr = Pieces(lambda i, j: wr.at[i, j], s_wr, r_wr)
    g_q = Gather(lambda i, j: w.at[i, j], s_w, r_w)
    g_uq = Gather(lambda i, j: uq.at[0, i, j], s_uq, r_uq)
    g_up = Gather(lambda i, j: up.at[0, i, j], s_up, r_up)
    g_w0 = Gather(lambda i, j: wo.at[:, 0, i, j], s_wo, r_wo)
    g_w1 = Gather(lambda i, j: wo.at[y, 1, i, j], s_wo, r_wo)

    def wo_y():
        here = wo.at[y, 0, z, x]
        for k in (2, 1, 3):
            rc(here, here, s_wo.at[2], r_wo.at[2], dev(dy=k)).start()

    def wo_z():
        got(wo.at[pl.ds(0, 3), 0, z, x], r_wo.at[2])
        g_w0.start_z()

    def wo_last():
        @pl.when(core == 0)
        def _():
            got(wo.at[:, 0, pl.ds(0, NZ - 1), x], r_wo.at[0])
            here = wo.at[:, 0, :, x]
            rc(here, here, s_wo.at[1], r_wo.at[4], dev(dx=1)).start()
            rc(here, here, s_wo.at[1], r_wo.at[5], dev(dx=-1)).start()
            rc(here, here, s_wo.at[3], r_wo.at[3], c_dev).start()

        @pl.when(core == 1)
        def _():
            g_w1.finish()
            here = wo.at[y, 1]
            rc(here, here, s_wo.at[2], r_wo.at[4], dev(dy=1)).start()
            rc(here, here, s_wo.at[2], r_wo.at[5], dev(dy=-1)).start()
            rc(here, here, s_wo.at[3], r_wo.at[3], c_dev).start()

    def wo_far():
        low, high = pl.ds(0, NZ // 2), pl.ds(NZ // 2, NZ // 2)

        @pl.when(core == 0)
        def _():
            for d, cut, sem in ((-1, low, 4), (1, high, 5)):
                whole = wo.at[:, 0, :, wrap(x + d, NX)]
                part = wo.at[:, 0, cut, wrap(x + d, NX)]
                got(whole, r_wo.at[sem])
                rc(part, part, s_wo.at[1], r_wo.at[1], dev(dx=-d)).start()
                rc(whole, whole, s_wo.at[3], r_wo.at[3], c_dev).start()

        @pl.when(core == 1)
        def _():
            for d, cut, sem in ((-1, low, 4), (1, high, 5)):
                whole = wo.at[wrap(y + d, NY), 1]
                part = wo.at[wrap(y + d, NY), 1, cut]
                got(whole, r_wo.at[sem])
                rc(part, part, s_wo.at[2], r_wo.at[2], dev(dy=-d)).start()
                rc(whole, whole, s_wo.at[3], r_wo.at[3], c_dev).start()

    def wo_cross():
        @pl.when(core == 0)
        def _():
            here = wo.at[:, 0, :, wrap(x + 2, NX)]
            got(here, r_wo.at[1])
            rc(here, here, s_wo.at[3], r_wo.at[3], c_dev).start()

        @pl.when(core == 1)
        def _():
            here = wo.at[wrap(y + 2, NY), 1]
            got(here, r_wo.at[2])
            rc(here, here, s_wo.at[3], r_wo.at[3], c_dev).start()

    def heads_y(steps):
        for k in steps:
            rel = -k % NY
            rc(up.at[0], up.at[rel], s_up.at[2], r_up.at[1 + rel], dev(dy=k)).start()
            rc(uq.at[0], uq.at[rel], s_uq.at[2], r_uq.at[1 + rel], dev(dy=k)).start()

    def heads_far(rel):
        got(up.at[rel], r_up.at[1 + rel])
        got(uq.at[rel], r_uq.at[1 + rel])
        if rel != 2:
            cut = pl.ds(0 if rel == 3 else NZ // 2, NZ // 2)
            device = dev(dy=1 if rel == 3 else -1)
            rc(up.at[rel, cut], up.at[2, cut], s_up.at[2], r_up.at[3], device).start()
            rc(uq.at[rel, cut], uq.at[2, cut], s_uq.at[2], r_uq.at[3], device).start()

    def heads_in(rel):
        for j in range(n):
            up_flat[rel, j * 8 : (j + 1) * 8, :] = up[rel, j // NX, j % NX]
            uq_flat[rel, j * 8 : (j + 1) * 8, :] = uq[rel, j // NX, j % NX]

    here = tok.at[core]
    c_partner = rc(here, here, s_tok.at[0], r_tok.at[0], c_dev)

    @pl.when(core == 1)
    def _():
        g_k.start_z()
        g_wr.start_z()
        g_k.pass_x(0)
        g_wr.pass_x(0)
        c_partner.start()
        g_up.start_z()
        g_uq.start_z()
        g_w1.start_z()
        for d in NEAR[1:]:
            g_k.pass_x(d)
            g_wr.pass_x(d)
            if d == 1:
                pl.semaphore_signal(go, inc=1, device_id=c_dev, device_id_type=MESH)
        g_up.start_x()
        g_uq.start_x()
        got(tok.at[1 - core], r_tok.at[0])
        both_tokens = tok[...].reshape(2 * own, width)
        for j in range(width // 128):
            cut = slice(j * 128, (j + 1) * 128)
            tok_mix[:, cut] = dot(both_tokens[:, cut], mix_in[...]).astype(BF16)
        g_wr.finish()
        packed = wr[...].reshape(rank, 128)
        for q in range(4):
            turned = (pltpu.roll(packed, 128 - 32 * q, 1) if q else packed).astype(BF16)
            for j in range(width // 128):
                wr_flat[j * 128 + q * 32 : j * 128 + (q + 1) * 32, :] = turned[j * 32 : (j + 1) * 32]
        g_k.finish()

    @pl.when(core == 0)
    def _():
        c_partner.start()
        wo_y()
        g_up.start_z()
        g_uq.start_z()
        pl.semaphore_wait(go, 1)
        g_q.start_z()
        g_q.start_x()
        g_up.start_x()
        g_uq.start_x()
        wo_z()

    def project():
        raw = dot(tok[...].reshape(2 * own, width), w[...].reshape(width, w.shape[-1])).astype(BF16)
        return rms(raw, gain[...])

    @pl.when(core == 1)
    def _():
        lat = project()
        rotary = dot(tok_mix[...], wr_flat[...])[:, :ROPE].astype(BF16)
        both = dot(rotary, sel_key[...])
        rows = pl.ds(pl.multiple_of(y * (2 * own), 2 * own), 2 * own)
        turned = both[:, :128] * tab[rows, :128] + both[:, 128:] * tab[rows, 128:] + kdoc[rows, :]
        half = own // 2
        for stripe in range(2):
            first = stripe * own
            parts = [
                lat[first + s * half : first + (s + 1) * half, h * 128 : (h + 1) * 128]
                for s in range(2)
                for h in range(2)
            ]
            packed = turned[first : first + half] + pltpu.roll(turned[first + half : first + own], 64, 1)
            parts.append(packed.astype(BF16))
            for i, tile in enumerate(parts):
                if stripe == 1:
                    kown[0, 0, i] = tile
                else:
                    ks[i] = tile
        here = kown.at[0, 0]
        rc(ks, here, s_z.at[1], r_z.at[2], dev(c=0)).start()
        for k in (2, 1, 3):
            rc(here, kown.at[-k % NX, 0], s_a.at[0], r_a.at[0], dev(dx=k)).start()
        for d in (4, 1, 7, 6, 2, 3, 5):
            pos = ZPOS[-d % NZ]
            rc(ks, kown.at[0, pos], s_z.at[1], r_z.at[0 if pos < 4 else 1], dev(dz=d, c=0)).start()

    parts = ((0, 1), (1, 3), (4, 4))

    def a_send(p):
        first, length = parts[p]
        src = kown.at[0, pl.ds(first, length)]
        for k in (2, 1, 3):
            rel = -k % NX
            sem = r_a.at[0] if p == 0 else r_a.at[3 * p - 3 + rel]
            rc(src, kown.at[rel, pl.ds(first, length)], s_a.at[0], sem, dev(dx=k)).start()

    def cross(a, count, p):
        cut = pl.ds(*parts[p])
        src, dst = kown.at[pl.ds(a, count), cut], koth.at[pl.ds(a, count), cut]
        rc(src, dst, s_d.at[0], r_d.at[1 if p == 2 else 0], c_dev).start()

    def z_part(p):
        if p == 0:
            got(kown.at[0, 0], r_z.at[2])
        else:
            got(kown.at[0, pl.ds(*parts[p])], r_z.at[p - 1])
        a_send(p)
        cross(0, 1, p)

    def a_part(p):
        if p == 0:
            got(kown.at[pl.ds(1, 3), 0], r_a.at[0])
            cross(1, 3, 0)
        else:
            for rel in (1, 3, 2):
                got(kown.at[rel, pl.ds(*parts[p])], r_a.at[3 * p - 3 + rel])
                cross(rel, 1, p)

    def rows_of(h):
        cut = pl.ds(1, 3) if h == 0 else pl.ds(4, 4)
        got(kown.at[:, cut], r_z.at[h])
        cut = pl.ds(4 * h, 4)
        rc(kown.at[:, cut], koth.at[:, cut], s_d.at[0], r_d.at[h], c_dev).start()

    @pl.when(core == 0)
    def _():
        z_part(0)
        got(tok.at[1 - core], r_tok.at[0])
        z_part(1)
        g_q.finish()
        ql[y] = project()
        here = ql.at[y]
        for k in (2, 1, 3):
            for c in range(2):
                rc(here, here, s_q.at[c], r_q.at[0], dev(dy=k, c=c)).start()
        rc(here, here, s_q.at[1], r_q.at[0], dev(c=1)).start()
        z_part(2)
        g_up.finish()
        g_uq.finish()
        heads_y((1, 3))
        a_part(0)

    @pl.when(core == 1)
    def _():
        g_up.finish()
        g_uq.finish()
        heads_y((1, 3))
        got(kown.at[pl.ds(1, 3), 0], r_a.at[0])
        for d in (1, 7, 6, 4, 3, 5, 2):
            pos = ZPOS[-d % NZ]
            rc(kown.at[:, 0], kown.at[:, pos], s_z.at[0], r_z.at[0 if pos < 4 else 1], dev(dz=d)).start()
        g_w1.start_x()

    heads_in(0)

    @pl.when(core == 0)
    def _():
        a_part(1)

    @pl.when(core == 1)
    def _():
        rows_of(0)

    @pl.when(core == 1)
    def _():
        got(ql, r_q.at[0])

    @pl.when(core == 0)
    def _():
        got(ql.at[pl.ds(0, 3)], r_q.at[0])

    c_sel.wait()
    scale = 1.0 / math.sqrt(NOPE + ROPE)
    factor = scale * math.log2(math.e)

    def queries_of(rel):
        projected = dot(ql[...].reshape(block, ql.shape[-1]), uq_flat[rel]).astype(BF16)
        for head in range(heads):
            laid = dot(projected, sel[:, head * 384 : (head + 1) * 384])
            turned = (laid[:, 128:256] * tab[:, :128] + laid[:, 256:] * tab[:, 128:]) * factor + qdoc[...]
            plain = (laid[:, :128] * factor).astype(BF16)
            rows = pl.ds(head * block, block)
            qs[rel, 0, rows, :128] = plain
            qs[rel, 1, rows, :128] = plain
            qs[rel, 0, rows, 128:] = turned.astype(BF16)
            qs[rel, 1, rows, 128:] = pltpu.roll(turned, 64, 1).astype(BF16)

    def tiles(ref, h, i):
        return ref[:, 4 * h : 4 * h + 4, i].reshape(256, 128)

    def expand(j):
        ref, h, rel = groups[j]
        for s in range(2):
            lat = jnp.concatenate([tiles(ref, h, 2 * s), tiles(ref, h, 2 * s + 1)], axis=1)
            kv = dot(lat, up_flat[rel]).astype(BF16)
            kbuf[j % 2, s] = kv[:, :nk]
            vbuf[j % 3, s * 256 : (s + 1) * 256, :] = kv[:, nk:]

    def score(j):
        ref, h, rel = groups[j]
        rot = tiles(ref, h, 4)
        for s in range(2):
            sbuf[j % 2, s] = dot_t(qs[rel, s], jnp.concatenate([kbuf[j % 2, s], rot], axis=1))

    step = 128

    def weigh(j):
        par, first, pair = j % 2, j % 4 == 0, j // 4 % 2
        for r in range(0, rows_all, step):
            rows = pl.ds(r, step)
            parts = [sbuf[par, s, rows, h * 128 : (h + 1) * 128] for s in range(2) for h in range(2)]
            most = jnp.maximum(jnp.maximum(parts[0], parts[1]), jnp.maximum(parts[2], parts[3]))
            most = jnp.max(most, axis=-1, keepdims=True)
            if first:
                new = jnp.broadcast_to(most, (step, 128))
            else:
                old = top_s[pair, rows, :]
                new = jnp.maximum(old, most)
                alpha = jnp.exp2(old - new)
            weights = [jnp.exp2(p - new) for p in parts]
            total = (weights[0] + weights[1]) + (weights[2] + weights[3])
            mixed = dot(jnp.concatenate([p.astype(BF16) for p in weights], axis=1), vbuf[j % 3])
            top_s[pair, rows, :] = new
            if first:
                sum_s[pair, rows, :] = total
                acc_s[pair, rows, :] = mixed
            else:
                sum_s[pair, rows, :] = sum_s[pair, rows, :] * alpha + total
                acc_s[pair, rows, :] = acc_s[pair, rows, :] * alpha + mixed

    head_lane = lax.broadcasted_iota(jnp.int32, (block, nk), 1) // VDIM

    def close(i, rel):
        pair = i % 2
        outs, sums = [], []
        for head in range(heads):
            rows = pl.ds(head * block, block)
            weight_sum = jnp.sum(sum_s[pair, rows, :], axis=-1, keepdims=True)
            outs.append(acc_s[pair, rows, :] / weight_sum)
            log_sum = jnp.broadcast_to(top_s[pair, rows, :1] + jnp.log2(weight_sum), (block, block))
            sums.append(jnp.sum(jnp.where(down == across, log_sum, 0.0), axis=0, keepdims=True))
        osend[i] = jnp.where(head_lane == 0, outs[0], outs[1]).astype(BF16)
        slot = y * NY + wrap(y + rel, NY)
        lget[core, slot] = jnp.concatenate(sums, axis=0)
        oget[core, slot] = osend[i, pl.ds(pl.multiple_of(t * own, own), own), :]
        for k in (2, 1, 3, 0):
            for c in range(2):
                def go_to(c=c, k=k):
                    device = dev(dy=k, c=c)
                    rows = pl.ds(pl.multiple_of(device[1] * own, own), own)
                    rc(osend.at[i, rows], oget.at[core, slot], s_f.at[0], r_f.at[0], device).start()
                    rc(lget.at[core, slot], lget.at[core, slot], s_f.at[1], r_f.at[1], device).start()
                if k:
                    go_to()
                else:
                    pl.when(core != c)(go_to)

    order = (0, 1, 3, 2)
    groups = [(ref, h, rel) for rel in order for ref, h in ((kown, 0), (koth, 0), (kown, 1), (koth, 1))]
    def second_half():
        pl.when(core == 0)(lambda: a_part(2))
        pl.when(core == 1)(lambda: rows_of(1))

    events = {
        0: [lambda: queries_of(0)],
        2: [second_half, lambda: heads_far(1), lambda: heads_far(3)],
        3: [lambda: heads_in(1), wo_last],
        7: [lambda: heads_in(3)],
        11: [lambda: heads_far(2), lambda: heads_in(2)],
        14: [wo_far],
    }
    for j, (ref, h, rel) in enumerate(groups):
        for event in events.get(j, ()):
            event()
        if j == 1 or j == 3:
            got(koth.at[:, pl.ds(4 * h, 4)], r_d.at[h])
        expand(j)
        if j % 4 == 3 and j < 15:
            queries_of(groups[j + 1][2])
        if j >= 1:
            score(j - 1)
        if j >= 2:
            weigh(j - 2)
            if (j - 2) % 4 == 3:
                close((j - 2) // 4, groups[j - 2][2])
    last = len(groups) - 1
    score(last)
    weigh(last - 1)
    weigh(last)
    close(last // 4, groups[last][2])
    wo_cross()

    c_out.wait()
    got(lget.at[:, pl.ds(0, 14)], r_f.at[1])
    got(oget.at[:, pl.ds(0, 14)], r_f.at[0])
    spot = lax.broadcasted_iota(jnp.int32, (own, block), 0) + t * own
    spot = spot == lax.broadcasted_iota(jnp.int32, (own, block), 1)
    own_lane = lax.broadcasted_iota(jnp.int32, (own, nk), 1) // VDIM

    def column(row):
        return jnp.sum(jnp.where(spot, jnp.broadcast_to(row, (own, block)), 0.0), axis=-1, keepdims=True)

    got(wo.at[:, 0], r_wo.at[3])
    mixed = jnp.zeros((own, width), F32)
    for p in range(NY):
        merged = []
        for c in range(2):
            logs = [lget[c, q * NY + p] for q in range(NY)]
            most = jnp.maximum(jnp.maximum(logs[0], logs[1]), jnp.maximum(logs[2], logs[3]))
            shares = [jnp.exp2(log - most) for log in logs]
            whole = (shares[0] + shares[1]) + (shares[2] + shares[3])
            total = jnp.zeros((own, nk), F32)
            for q in range(NY):
                share = shares[q] / whole
                both = jnp.where(own_lane == 0, column(share[:1]), column(share[1:]))
                total = total + both * oget[c, q * NY + p].astype(F32)
            merged.append(total.astype(BF16))
        weights = jnp.concatenate([wo[p, c].reshape(width, nk) for c in range(2)], axis=1)
        mixed = mixed + dot_t(jnp.concatenate(merged, axis=1), weights)
    out[...] = rms(mixed.astype(BF16), gain_out[...])
    logs = [lget[core, q * NY + y] for q in range(NY)]
    most = jnp.maximum(jnp.maximum(logs[0], logs[1]), jnp.maximum(logs[2], logs[3]))
    shares = [jnp.exp2(log - most) for log in logs]
    whole = (shares[0] + shares[1]) + (shares[2] + shares[3])
    log_out[...] = most * math.log(2.0) + jnp.log(whole)

    for gather in (g_up, g_uq):
        gather.drain()
    sent(up.at[pl.ds(0, 3)], s_up.at[2])
    sent(uq.at[pl.ds(0, 3)], s_uq.at[2])
    sent(wo.at[:, 0], s_wo.at[3])
    sent(tok.at[core], s_tok.at[0])
    sent(kown, s_d.at[0])
    sent(oget.at[:, pl.ds(0, 14)], s_f.at[0])
    sent(lget.at[:, pl.ds(0, 14)], s_f.at[1])

    @pl.when(core == 1)
    def _():
        g_k.drain()
        g_wr.drain()
        g_w1.drain()
        sent(wo.at[pl.ds(0, 3), 1], s_wo.at[2])
        sent(kown.at[:, pl.ds(0, 7)], s_z.at[0])
        sent(kown.at[0], s_z.at[1])
        sent(kown.at[pl.ds(0, 3), 0], s_a.at[0])

    @pl.when(core == 0)
    def _():
        g_q.drain()
        g_w0.drain()
        sent(kown.at[pl.ds(0, 3)], s_a.at[0])
        sent(wo.at[pl.ds(0, 3), 0, 0, 0], s_wo.at[2])
        sent(ql, s_q.at[1])
        sent(ql.at[pl.ds(0, 3)], s_q.at[0])


def on_device(n, ntp, tokens, doc_ids, down_q, down_k, down_r, gain_q, gain_k, up_q, up_k, up_v, out_w, gain_o):
    own, width = tokens.shape
    block = doc_ids.shape[0]
    heads = up_k.shape[1] // NOPE
    rank = down_k.shape[1]
    nq, nk, nv = up_q.shape[1], up_k.shape[1], up_v.shape[1]
    turn_in, turn_block, pick, pick_key, mix = tables(n, block, heads)
    vmem = pl.BlockSpec(memory_space=pltpu.VMEM)
    hbm = pl.BlockSpec(memory_space=pl.ANY)
    dma = lambda k: pltpu.SemaphoreType.DMA((k,))
    v = lambda *shape, dtype=BF16: pltpu.VMEM(shape, dtype)
    rows = heads * block
    scratch = [
        pltpu.VMEM((1, block), jnp.int32), v(1, rank, dtype=F32), v(1, width, dtype=F32), v(1, 256, dtype=F32), v(ROPE, 256),
        v(128, 128), v(2 * own, width), v(width // n, ROPE), v(width, 128),
        v(2, own, width), v(NZ, NX, width // n, rank), v(NZ, NX, width // n // 4, 128, dtype=F32),
        v(NY, NZ, NX, rank // n, nq), v(NY, NZ, NX, rank // n, nk + nv), v(NY, 2, NZ, NX, width // n, nv),
        v(NY, rank, nq), v(NY, rank, nk + nv), v(NY, 2 * own, rank),
        v(NX, NZ, 5, own // 2, 128), v(NX, NZ, 5, own // 2, 128), v(5, own // 2, 128),
        v(block, 256, dtype=F32), v(block, 128, dtype=F32), v(block, 128, dtype=F32), v(*pick.shape),
        v(NY, 2, rows, 256),
        v(2, 2, rows, 256, dtype=F32), v(2, 2, 256, nk), v(3, 512, nv),
        v(2, rows, 128, dtype=F32), v(2, rows, 128, dtype=F32), v(2, rows, 128, dtype=F32),
        v(NY, block, nv), v(2, NY * NY, own, nv), v(2, NY * NY, heads, block, dtype=F32),
        pltpu.SemaphoreType.REGULAR,
        dma(15), dma(1), dma(1), dma(2), dma(8), dma(2), dma(8), dma(3), dma(5), dma(3), dma(5), dma(4), dma(6),
        dma(2), dma(1), dma(1), dma(7), dma(2), dma(3), dma(1), dma(2), dma(2), dma(2),
    ]
    mixed, log_sums = pl.pallas_call(
        functools.partial(kernel, n, ntp, heads),
        out_shape=(
            jax.ShapeDtypeStruct((own, width), BF16),
            jax.ShapeDtypeStruct((heads, block), F32),
        ),
        in_specs=[hbm] * 17,
        out_specs=(vmem, vmem),
        scratch_shapes=scratch,
        compiler_params=pltpu.CompilerParams(
            collective_id=0, has_side_effects=True, vmem_limit_bytes=60 * 1024 * 1024
        ),
    )(
        tokens, doc_ids[None, :], down_q, down_k, down_r, gain_q[None, :], gain_k[None, :],
        up_q, up_k, up_v, out_w.T, gain_o[None, :],
        jnp.asarray(turn_in), jnp.asarray(turn_block[:, None, :]), jnp.asarray(pick, BF16), jnp.asarray(pick_key, BF16), jnp.asarray(mix, BF16),
    )
    return mixed, log_sums.T


def solution(mesh):
    assert mesh.shape["tp"] == 2 * NY and mesh.shape["sp"] == NX * NZ
    placed = (
        P(("sp", "tp"), None), P("sp"), P("sp", None), P("sp", None), P("sp", None), P(), P(),
        P("sp", "tp"), P("sp", "tp"), P("sp", "tp"), P("tp", "sp"), P(),
    )
    return jax.shard_map(
        functools.partial(on_device, mesh.shape["sp"], mesh.shape["tp"]),
        mesh=mesh,
        in_specs=placed,
        out_specs=(P(("sp", "tp"), None), P("sp", "tp")),
        check_vma=False,
    )
```

```python
import functools
import math

import jax
import jax.numpy as jnp
import numpy as np
from jax import lax
from jax.experimental import pallas as pl
from jax.experimental.pallas import tpu as pltpu
from jax.sharding import PartitionSpec as P

NOPE = 64
ROPE = 32
VDIM = 64
THETA = 10000.0
EPS = 1e-06
MASKED = -1e30
MESH = pl.DeviceIdType.MESH
F32 = jnp.float32
BF16 = jnp.bfloat16
NX, NY, NZ = 4, 4, 8
NEAR = (0, 1, 7, 2, 6, 3, 5, 4)
ZPOS = {rel: pos for pos, rel in enumerate(NEAR)}


def dot(a, b):
    return jnp.dot(a, b, preferred_element_type=F32)


def dot_t(a, b):
    return lax.dot_general(a, b, (((1,), (1,)), ((), ())), preferred_element_type=F32)


def rms(values, gain):
    wide = values.astype(F32)
    scale = lax.rsqrt(jnp.mean(wide * wide, axis=-1, keepdims=True) + EPS)
    return (wide * scale * gain).astype(BF16)


def tables(n, block, heads):
    half = ROPE // 2
    inverse = np.float32(THETA) ** (-np.arange(half, dtype=np.float32) / np.float32(half))
    inverse = inverse.astype(np.float32).astype(np.float64)[None, :]

    def turn(positions):
        angles = positions.astype(np.float64)[:, None] * inverse
        both = np.zeros((len(positions), 256), np.float32)
        both[:, :ROPE] = np.tile(np.cos(angles), (1, 2))
        both[:, 128 : 128 + ROPE] = np.tile(np.sin(angles), (1, 2))
        return both

    width = NOPE + ROPE
    pick = np.zeros((heads * width, heads * 384), np.float32)
    eye = np.arange(NOPE)
    rot = np.arange(ROPE)
    low = np.arange(half)
    for head in range(heads):
        pick[head * width + eye, head * 384 + (head % 2) * NOPE + eye] = 1
        pick[head * width + NOPE + rot, head * 384 + 128 + rot] = 1
        pick[head * width + NOPE + half + low, head * 384 + 256 + low] = -1
        pick[head * width + NOPE + low, head * 384 + 256 + half + low] = 1
    pick_key = np.zeros((ROPE, 256), np.float32)
    pick_key[rot, rot] = 1
    pick_key[half + low, 128 + low] = -1
    pick_key[low, 128 + half + low] = 1
    mix = np.zeros((128, 128), np.float32)
    to = np.arange(128)
    mix[32 * (to // 8 % 4) + 8 * (to // 32) + to % 8, to] = 1
    return turn(np.arange(block)), turn(np.arange(n) * block), pick, pick_key, mix


def kernel(
    n, ntp, heads,
    tokens, docs_in, down_q, down_k, down_r, gain_q, gain_k, up_q, up_k, up_v, out_wt, gain_o,
    turn_in, turn_block, pick, pick_key, mix,
    out, log_out,
    docs, gain, gain_out, turn_me, sel_key, mix_in, tok_mix, wr_in, wr_flat,
    tok, w, wr, uq, up, wo, uq_flat, up_flat, ql, kown, koth, ks, tab, kdoc, qdoc, sel, qs,
    sbuf, kbuf, vbuf, top_s, sum_s, acc_s, osend, oget, lget,
    go, loc, s_tok, r_tok, s_w, r_w, s_wr, r_wr, s_uq, r_uq, s_up, r_up, s_wo, r_wo,
    s_q, r_q, s_a, r_a, s_z, r_z, s_d, r_d, s_f, r_f,
):
    me = lax.axis_index("sp")
    t = lax.axis_index("tp")
    z, x = me // NX, lax.rem(me, NX)
    y, core = t // 2, lax.rem(t, 2)
    own, width = tokens.shape
    block = ntp * own
    rows_all = heads * block

    def wrap(v, size):
        return lax.rem(v + size, size)

    def dev(dz=0, dx=0, dy=0, c=None):
        c = core if c is None else c
        zz = wrap(z + dz, NZ) if dz else z
        xx = wrap(x + dx, NX) if dx else x
        yy = wrap(y + dy, NY) if dy else y
        return (zz * NX + xx, yy * 2 + c)

    c_dev = dev(c=1 - core)

    def rc(src, dst, s, r, device):
        return pltpu.make_async_remote_copy(
            src_ref=src, dst_ref=dst, send_sem=s, recv_sem=r, device_id=device, device_id_type=MESH
        )

    def sent(ref, s):
        rc(ref, ref, s, s, c_dev).wait_send()

    def got(ref, r):
        rc(ref, ref, r, r, c_dev).wait_recv()

    barrier = pltpu.get_barrier_semaphore()
    others = [dev(dz=d) for d in range(1, NZ)] + [dev(dx=d) for d in range(1, NX)]
    others += [dev(dz=d, c=1 - core) for d in range(1, NZ)]
    others += [dev(dy=d) for d in range(1, NY)] + [dev(dy=d, c=1 - core) for d in range(NY)]
    for device in others:
        pl.semaphore_signal(barrier, inc=1, device_id=device, device_id_type=MESH)

    @pl.when(core == 1)
    def _():
        pltpu.make_async_copy(down_k, w.at[z, x], loc.at[1]).start()
        pltpu.make_async_copy(gain_k, gain, loc.at[9]).start()

    @pl.when(core == 0)
    def _():
        pltpu.make_async_copy(down_q, w.at[z, x], loc.at[1]).start()
        pltpu.make_async_copy(gain_q, gain, loc.at[9]).start()

    nq, nk = up_q.shape[1], up_k.shape[1]
    c_w = pltpu.make_async_copy(down_k, w.at[z, x], loc.at[1])
    c_gain = pltpu.make_async_copy(gain_k, gain, loc.at[9])
    c_docs = pltpu.make_async_copy(docs_in, docs, loc.at[10])
    c_tab = pltpu.make_async_copy(turn_in, tab, loc.at[7])
    c_me = pltpu.make_async_copy(turn_block.at[me], turn_me, loc.at[11])
    c_tok = pltpu.make_async_copy(tokens, tok.at[core], loc.at[0])
    c_wr = pltpu.make_async_copy(down_r, wr_in, loc.at[2])
    c_mix = pltpu.make_async_copy(mix, mix_in, loc.at[14])
    c_uq = pltpu.make_async_copy(up_q, uq.at[0, z, x], loc.at[3])
    c_up = [
        pltpu.make_async_copy(up_k, up.at[0, z, x, :, pl.ds(0, nk)], loc.at[4]),
        pltpu.make_async_copy(up_v, up.at[0, z, x, :, pl.ds(nk, nk)], loc.at[5]),
    ]
    c_wo = pltpu.make_async_copy(out_wt, wo.at[y, core, z, x], loc.at[6])
    c_sel = pltpu.make_async_copy(pick, sel, loc.at[8])
    c_key = pltpu.make_async_copy(pick_key, sel_key, loc.at[12])
    c_out = pltpu.make_async_copy(gain_o, gain_out, loc.at[13])
    for copy in [c_docs, c_tab, c_me, c_wr, c_tok, c_uq] + c_up + [c_key, c_mix, c_wo, c_sel, c_out]:
        copy.start()

    down = lax.broadcasted_iota(jnp.int32, (block, block), 0)
    across = lax.broadcasted_iota(jnp.int32, (block, block), 1)
    c_docs.wait()
    doc_row = jnp.broadcast_to(docs[...].astype(F32), (block, block))
    doc_col = jnp.sum(jnp.where(down == across, doc_row, 0.0), axis=-1, keepdims=True)
    lane = lax.broadcasted_iota(jnp.int32, (block, 128), 1)
    in_docs = (lane >= ROPE) & (lane < ROPE + n)
    same = doc_col == (lane - ROPE).astype(F32)
    kdoc[...] = jnp.where(in_docs & same, 1.0, 0.0)
    qdoc[...] = jnp.where(in_docs & jnp.logical_not(same), MASKED, 0.0)
    c_tab.wait()
    c_me.wait()
    cos_a, sin_a = turn_me[:, :128], turn_me[:, 128:]
    cos_b, sin_b = tab[:, :128], tab[:, 128:]
    tab[:, :128] = cos_a * cos_b - sin_a * sin_b
    tab[:, 128:] = sin_a * cos_b + cos_a * sin_b

    rank = uq_flat.shape[1]
    c_wr.wait()
    wide_r = wr_in[...].astype(F32)
    wr[z, x] = jnp.concatenate([wide_r[8 * q : 8 * q + 8] for q in range(4)], axis=1)
    for copy in [c_w, c_tok, c_uq] + c_up + [c_key, c_mix, c_gain, c_wo]:
        copy.wait()
    pl.semaphore_wait(barrier, len(others))

    class Gather:
        def __init__(self, at, s, r):
            self.at, self.s, self.r = at, s, r

        def start_z(self):
            here = self.at(z, x)
            for d in reversed(NEAR[1:]):
                rc(here, here, self.s.at[0], self.r.at[0], dev(dz=d)).start()

        def start_x(self):
            got(self.at(pl.ds(0, NZ - 1), x), self.r.at[0])
            column = self.at(slice(None), x)
            for k in (2, 1, -1):
                rc(column, column, self.s.at[1], self.r.at[1], dev(dx=k)).start()

        def finish(self):
            got(self.at(pl.ds(0, NZ - 2), slice(None)), self.r.at[1])

        def drain(self):
            sent(self.at(pl.ds(0, NZ - 1), 0), self.s.at[0])
            sent(self.at(pl.ds(0, NZ - 2), slice(None)), self.s.at[1])

    class Pieces(Gather):
        def start_z(self):
            here = self.at(z, x)
            for d in reversed(NEAR[1:]):
                rc(here, here, self.s.at[0], self.r.at[d], dev(dz=d)).start()

        def pass_x(self, d):
            here = self.at(wrap(z - d, NZ), x)
            if d > 0:
                got(here, self.r.at[d])
            for k in (2, 1, -1):
                rc(here, here, self.s.at[1], self.r.at[0], dev(dx=k)).start()

        def finish(self):
            got(self.at(pl.ds(0, NZ - 2), slice(None)), self.r.at[0])

    g_k = Pieces(lambda i, j: w.at[i, j], s_w, r_w)
    g_wr = Pieces(lambda i, j: wr.at[i, j], s_wr, r_wr)
    g_q = Gather(lambda i, j: w.at[i, j], s_w, r_w)
    g_uq = Gather(lambda i, j: uq.at[0, i, j], s_uq, r_uq)
    g_up = Gather(lambda i, j: up.at[0, i, j], s_up, r_up)
    g_w0 = Gather(lambda i, j: wo.at[:, 0, i, j], s_wo, r_wo)
    g_w1 = Gather(lambda i, j: wo.at[y, 1, i, j], s_wo, r_wo)

    def wo_y():
        here = wo.at[y, 0, z, x]
        for k in (2, 1, 3):
            rc(here, here, s_wo.at[2], r_wo.at[2], dev(dy=k)).start()

    def wo_z():
        got(wo.at[pl.ds(0, 3), 0, z, x], r_wo.at[2])
        g_w0.start_z()

    def wo_last():
        @pl.when(core == 0)
        def _():
            got(wo.at[:, 0, pl.ds(0, NZ - 1), x], r_wo.at[0])
            here = wo.at[:, 0, :, x]
            rc(here, here, s_wo.at[1], r_wo.at[4], dev(dx=1)).start()
            rc(here, here, s_wo.at[1], r_wo.at[5], dev(dx=-1)).start()
            rc(here, here, s_wo.at[3], r_wo.at[3], c_dev).start()

        @pl.when(core == 1)
        def _():
            g_w1.finish()
            here = wo.at[y, 1]
            rc(here, here, s_wo.at[2], r_wo.at[4], dev(dy=1)).start()
            rc(here, here, s_wo.at[2], r_wo.at[5], dev(dy=-1)).start()
            rc(here, here, s_wo.at[3], r_wo.at[3], c_dev).start()

    def wo_far():
        low, high = pl.ds(0, NZ // 2), pl.ds(NZ // 2, NZ // 2)

        @pl.when(core == 0)
        def _():
            for d, cut, sem in ((-1, low, 4), (1, high, 5)):
                whole = wo.at[:, 0, :, wrap(x + d, NX)]
                part = wo.at[:, 0, cut, wrap(x + d, NX)]
                got(whole, r_wo.at[sem])
                rc(part, part, s_wo.at[1], r_wo.at[1], dev(dx=-d)).start()
                rc(whole, whole, s_wo.at[3], r_wo.at[3], c_dev).start()

        @pl.when(core == 1)
        def _():
            for d, cut, sem in ((-1, low, 4), (1, high, 5)):
                whole = wo.at[wrap(y + d, NY), 1]
                part = wo.at[wrap(y + d, NY), 1, cut]
                got(whole, r_wo.at[sem])
                rc(part, part, s_wo.at[2], r_wo.at[2], dev(dy=-d)).start()
                rc(whole, whole, s_wo.at[3], r_wo.at[3], c_dev).start()

    def wo_cross():
        @pl.when(core == 0)
        def _():
            here = wo.at[:, 0, :, wrap(x + 2, NX)]
            got(here, r_wo.at[1])
            rc(here, here, s_wo.at[3], r_wo.at[3], c_dev).start()

        @pl.when(core == 1)
        def _():
            here = wo.at[wrap(y + 2, NY), 1]
            got(here, r_wo.at[2])
            rc(here, here, s_wo.at[3], r_wo.at[3], c_dev).start()

    def heads_y(steps):
        for k in steps:
            rel = -k % NY
            rc(up.at[0], up.at[rel], s_up.at[2], r_up.at[1 + rel], dev(dy=k)).start()
            rc(uq.at[0], uq.at[rel], s_uq.at[2], r_uq.at[1 + rel], dev(dy=k)).start()

    def heads_far(rel):
        got(up.at[rel], r_up.at[1 + rel])
        got(uq.at[rel], r_uq.at[1 + rel])
        if rel != 2:
            cut = pl.ds(0 if rel == 3 else NZ // 2, NZ // 2)
            device = dev(dy=1 if rel == 3 else -1)
            rc(up.at[rel, cut], up.at[2, cut], s_up.at[2], r_up.at[3], device).start()
            rc(uq.at[rel, cut], uq.at[2, cut], s_uq.at[2], r_uq.at[3], device).start()

    def heads_in(rel):
        for j in range(n):
            up_flat[rel, j * 8 : (j + 1) * 8, :] = up[rel, j // NX, j % NX]
            uq_flat[rel, j * 8 : (j + 1) * 8, :] = uq[rel, j // NX, j % NX]

    here = tok.at[core]
    c_partner = rc(here, here, s_tok.at[0], r_tok.at[0], c_dev)

    @pl.when(core == 1)
    def _():
        g_k.start_z()
        g_wr.start_z()
        g_k.pass_x(0)
        g_wr.pass_x(0)
        c_partner.start()
        g_up.start_z()
        g_uq.start_z()
        for d in NEAR[1:]:
            g_k.pass_x(d)
            g_wr.pass_x(d)
            if d == 1:
                pl.semaphore_signal(go, inc=1, device_id=c_dev, device_id_type=MESH)
        g_w1.start_z()
        g_up.start_x()
        g_uq.start_x()
        got(tok.at[1 - core], r_tok.at[0])
        both_tokens = tok[...].reshape(2 * own, width)
        for j in range(width // 128):
            cut = slice(j * 128, (j + 1) * 128)
            tok_mix[:, cut] = dot(both_tokens[:, cut], mix_in[...]).astype(BF16)
        g_wr.finish()
        packed = wr[...].reshape(rank, 128)
        for q in range(4):
            turned = (pltpu.roll(packed, 128 - 32 * q, 1) if q else packed).astype(BF16)
            for j in range(width // 128):
                wr_flat[j * 128 + q * 32 : j * 128 + (q + 1) * 32, :] = turned[j * 32 : (j + 1) * 32]
        g_k.finish()

    @pl.when(core == 0)
    def _():
        c_partner.start()
        wo_y()
        g_up.start_z()
        g_uq.start_z()
        pl.semaphore_wait(go, 1)
        g_q.start_z()
        g_q.start_x()
        g_up.start_x()
        g_uq.start_x()
        wo_z()

    def project():
        raw = dot(tok[...].reshape(2 * own, width), w[...].reshape(width, w.shape[-1])).astype(BF16)
        return rms(raw, gain[...])

    @pl.when(core == 1)
    def _():
        lat = project()
        rotary = dot(tok_mix[...], wr_flat[...])[:, :ROPE].astype(BF16)
        both = dot(rotary, sel_key[...])
        rows = pl.ds(pl.multiple_of(y * (2 * own), 2 * own), 2 * own)
        turned = both[:, :128] * tab[rows, :128] + both[:, 128:] * tab[rows, 128:] + kdoc[rows, :]
        half = own // 2
        for stripe in range(2):
            first = stripe * own
            parts = [
                lat[first + s * half : first + (s + 1) * half, h * 128 : (h + 1) * 128]
                for s in range(2)
                for h in range(2)
            ]
            packed = turned[first : first + half] + pltpu.roll(turned[first + half : first + own], 64, 1)
            parts.append(packed.astype(BF16))
            for i, tile in enumerate(parts):
                if stripe == 1:
                    kown[0, 0, i] = tile
                else:
                    ks[i] = tile
        here = kown.at[0, 0]
        rc(ks, here, s_z.at[1], r_z.at[2], dev(c=0)).start()
        for k in (2, 1, 3):
            rc(here, kown.at[-k % NX, 0], s_a.at[0], r_a.at[0], dev(dx=k)).start()
        for d in (4, 1, 7, 6, 2, 3, 5):
            pos = ZPOS[-d % NZ]
            rc(ks, kown.at[0, pos], s_z.at[1], r_z.at[0 if pos < 4 else 1], dev(dz=d, c=0)).start()

    parts = ((0, 1), (1, 3), (4, 4))

    def a_send(p):
        first, length = parts[p]
        src = kown.at[0, pl.ds(first, length)]
        for k in (2, 1, 3):
            rel = -k % NX
            sem = r_a.at[0] if p == 0 else r_a.at[3 * p - 3 + rel]
            rc(src, kown.at[rel, pl.ds(first, length)], s_a.at[0], sem, dev(dx=k)).start()

    def cross(a, count, p):
        cut = pl.ds(*parts[p])
        src, dst = kown.at[pl.ds(a, count), cut], koth.at[pl.ds(a, count), cut]
        rc(src, dst, s_d.at[0], r_d.at[1 if p == 2 else 0], c_dev).start()

    def z_part(p):
        if p == 0:
            got(kown.at[0, 0], r_z.at[2])
        else:
            got(kown.at[0, pl.ds(*parts[p])], r_z.at[p - 1])
        a_send(p)
        cross(0, 1, p)

    def a_part(p):
        if p == 0:
            got(kown.at[pl.ds(1, 3), 0], r_a.at[0])
            cross(1, 3, 0)
        else:
            for rel in (1, 3, 2):
                got(kown.at[rel, pl.ds(*parts[p])], r_a.at[3 * p - 3 + rel])
                cross(rel, 1, p)

    def rows_of(h):
        cut = pl.ds(1, 3) if h == 0 else pl.ds(4, 4)
        got(kown.at[:, cut], r_z.at[h])
        cut = pl.ds(4 * h, 4)
        rc(kown.at[:, cut], koth.at[:, cut], s_d.at[0], r_d.at[h], c_dev).start()

    @pl.when(core == 0)
    def _():
        z_part(0)
        got(tok.at[1 - core], r_tok.at[0])
        z_part(1)
        g_q.finish()
        ql[y] = project()
        here = ql.at[y]
        for k in (2, 1, 3):
            for c in range(2):
                rc(here, here, s_q.at[c], r_q.at[0], dev(dy=k, c=c)).start()
        rc(here, here, s_q.at[1], r_q.at[0], dev(c=1)).start()
        z_part(2)
        g_up.finish()
        g_uq.finish()
        heads_y((1, 3))
        a_part(0)

    @pl.when(core == 1)
    def _():
        g_up.finish()
        g_uq.finish()
        heads_y((1, 3))
        got(kown.at[pl.ds(1, 3), 0], r_a.at[0])
        for d in (1, 7, 6, 4, 3, 5, 2):
            pos = ZPOS[-d % NZ]
            rc(kown.at[:, 0], kown.at[:, pos], s_z.at[0], r_z.at[0 if pos < 4 else 1], dev(dz=d)).start()
        g_w1.start_x()

    heads_in(0)

    @pl.when(core == 0)
    def _():
        a_part(1)

    @pl.when(core == 1)
    def _():
        rows_of(0)

    @pl.when(core == 1)
    def _():
        got(ql, r_q.at[0])

    @pl.when(core == 0)
    def _():
        got(ql.at[pl.ds(0, 3)], r_q.at[0])

    c_sel.wait()
    scale = 1.0 / math.sqrt(NOPE + ROPE)
    factor = scale * math.log2(math.e)

    def queries_of(rel):
        projected = dot(ql[...].reshape(block, ql.shape[-1]), uq_flat[rel]).astype(BF16)
        for head in range(heads):
            laid = dot(projected, sel[:, head * 384 : (head + 1) * 384])
            turned = (laid[:, 128:256] * tab[:, :128] + laid[:, 256:] * tab[:, 128:]) * factor + qdoc[...]
            plain = (laid[:, :128] * factor).astype(BF16)
            rows = pl.ds(head * block, block)
            qs[rel, 0, rows, :128] = plain
            qs[rel, 1, rows, :128] = plain
            qs[rel, 0, rows, 128:] = turned.astype(BF16)
            qs[rel, 1, rows, 128:] = pltpu.roll(turned, 64, 1).astype(BF16)

    def tiles(ref, h, i):
        return ref[:, 4 * h : 4 * h + 4, i].reshape(256, 128)

    def expand(j):
        ref, h, rel = groups[j]
        for s in range(2):
            lat = jnp.concatenate([tiles(ref, h, 2 * s), tiles(ref, h, 2 * s + 1)], axis=1)
            kv = dot(lat, up_flat[rel]).astype(BF16)
            kbuf[j % 2, s] = kv[:, :nk]
            vbuf[j % 3, s * 256 : (s + 1) * 256, :] = kv[:, nk:]

    def score(j):
        ref, h, rel = groups[j]
        rot = tiles(ref, h, 4)
        for s in range(2):
            sbuf[j % 2, s] = dot_t(qs[rel, s], jnp.concatenate([kbuf[j % 2, s], rot], axis=1))

    step = 128

    def weigh(j):
        par, first, pair = j % 2, j % 4 == 0, j // 4 % 2
        for r in range(0, rows_all, step):
            rows = pl.ds(r, step)
            parts = [sbuf[par, s, rows, h * 128 : (h + 1) * 128] for s in range(2) for h in range(2)]
            most = jnp.maximum(jnp.maximum(parts[0], parts[1]), jnp.maximum(parts[2], parts[3]))
            most = jnp.max(most, axis=-1, keepdims=True)
            if first:
                new = jnp.broadcast_to(most, (step, 128))
            else:
                old = top_s[pair, rows, :]
                new = jnp.maximum(old, most)
                alpha = jnp.exp2(old - new)
            weights = [jnp.exp2(p - new) for p in parts]
            total = (weights[0] + weights[1]) + (weights[2] + weights[3])
            mixed = dot(jnp.concatenate([p.astype(BF16) for p in weights], axis=1), vbuf[j % 3])
            top_s[pair, rows, :] = new
            if first:
                sum_s[pair, rows, :] = total
                acc_s[pair, rows, :] = mixed
            else:
                sum_s[pair, rows, :] = sum_s[pair, rows, :] * alpha + total
                acc_s[pair, rows, :] = acc_s[pair, rows, :] * alpha + mixed

    head_lane = lax.broadcasted_iota(jnp.int32, (block, nk), 1) // VDIM

    def close(i, rel):
        pair = i % 2
        outs, sums = [], []
        for head in range(heads):
            rows = pl.ds(head * block, block)
            weight_sum = jnp.sum(sum_s[pair, rows, :], axis=-1, keepdims=True)
            outs.append(acc_s[pair, rows, :] / weight_sum)
            log_sum = jnp.broadcast_to(top_s[pair, rows, :1] + jnp.log2(weight_sum), (block, block))
            sums.append(jnp.sum(jnp.where(down == across, log_sum, 0.0), axis=0, keepdims=True))
        osend[i] = jnp.where(head_lane == 0, outs[0], outs[1]).astype(BF16)
        slot = y * NY + wrap(y + rel, NY)
        lget[core, slot] = jnp.concatenate(sums, axis=0)
        oget[core, slot] = osend[i, pl.ds(pl.multiple_of(t * own, own), own), :]
        for k in (2, 1, 3, 0):
            for c in range(2):
                def go_to(c=c, k=k):
                    device = dev(dy=k, c=c)
                    rows = pl.ds(pl.multiple_of(device[1] * own, own), own)
                    rc(osend.at[i, rows], oget.at[core, slot], s_f.at[0], r_f.at[0], device).start()
                    rc(lget.at[core, slot], lget.at[core, slot], s_f.at[1], r_f.at[1], device).start()
                if k:
                    go_to()
                else:
                    pl.when(core != c)(go_to)

    order = (0, 1, 3, 2)
    groups = [(ref, h, rel) for rel in order for ref, h in ((kown, 0), (koth, 0), (kown, 1), (koth, 1))]
    def second_half():
        pl.when(core == 0)(lambda: a_part(2))
        pl.when(core == 1)(lambda: rows_of(1))

    events = {
        0: [lambda: queries_of(0)],
        2: [second_half, lambda: heads_far(1), lambda: heads_far(3)],
        3: [lambda: heads_in(1), wo_last],
        7: [lambda: heads_in(3)],
        11: [lambda: heads_far(2), lambda: heads_in(2)],
        14: [wo_far],
    }
    for j, (ref, h, rel) in enumerate(groups):
        for event in events.get(j, ()):
            event()
        if j == 1 or j == 3:
            got(koth.at[:, pl.ds(4 * h, 4)], r_d.at[h])
        expand(j)
        if j % 4 == 3 and j < 15:
            queries_of(groups[j + 1][2])
        if j >= 1:
            score(j - 1)
        if j >= 2:
            weigh(j - 2)
            if (j - 2) % 4 == 3:
                close((j - 2) // 4, groups[j - 2][2])
    last = len(groups) - 1
    score(last)
    weigh(last - 1)
    weigh(last)
    close(last // 4, groups[last][2])
    wo_cross()

    c_out.wait()
    got(lget.at[:, pl.ds(0, 14)], r_f.at[1])
    got(oget.at[:, pl.ds(0, 14)], r_f.at[0])
    spot = lax.broadcasted_iota(jnp.int32, (own, block), 0) + t * own
    spot = spot == lax.broadcasted_iota(jnp.int32, (own, block), 1)
    own_lane = lax.broadcasted_iota(jnp.int32, (own, nk), 1) // VDIM

    def column(row):
        return jnp.sum(jnp.where(spot, jnp.broadcast_to(row, (own, block)), 0.0), axis=-1, keepdims=True)

    got(wo.at[:, 0], r_wo.at[3])
    mixed = jnp.zeros((own, width), F32)
    for p in range(NY):
        merged = []
        for c in range(2):
            logs = [lget[c, q * NY + p] for q in range(NY)]
            most = jnp.maximum(jnp.maximum(logs[0], logs[1]), jnp.maximum(logs[2], logs[3]))
            shares = [jnp.exp2(log - most) for log in logs]
            whole = (shares[0] + shares[1]) + (shares[2] + shares[3])
            total = jnp.zeros((own, nk), F32)
            for q in range(NY):
                share = shares[q] / whole
                both = jnp.where(own_lane == 0, column(share[:1]), column(share[1:]))
                total = total + both * oget[c, q * NY + p].astype(F32)
            merged.append(total.astype(BF16))
        weights = jnp.concatenate([wo[p, c].reshape(width, nk) for c in range(2)], axis=1)
        mixed = mixed + dot_t(jnp.concatenate(merged, axis=1), weights)
    out[...] = rms(mixed.astype(BF16), gain_out[...])
    logs = [lget[core, q * NY + y] for q in range(NY)]
    most = jnp.maximum(jnp.maximum(logs[0], logs[1]), jnp.maximum(logs[2], logs[3]))
    shares = [jnp.exp2(log - most) for log in logs]
    whole = (shares[0] + shares[1]) + (shares[2] + shares[3])
    log_out[...] = most * math.log(2.0) + jnp.log(whole)

    for gather in (g_up, g_uq):
        gather.drain()
    sent(up.at[pl.ds(0, 3)], s_up.at[2])
    sent(uq.at[pl.ds(0, 3)], s_uq.at[2])
    sent(wo.at[:, 0], s_wo.at[3])
    sent(tok.at[core], s_tok.at[0])
    sent(kown, s_d.at[0])
    sent(oget.at[:, pl.ds(0, 14)], s_f.at[0])
    sent(lget.at[:, pl.ds(0, 14)], s_f.at[1])

    @pl.when(core == 1)
    def _():
        g_k.drain()
        g_wr.drain()
        g_w1.drain()
        sent(wo.at[pl.ds(0, 3), 1], s_wo.at[2])
        sent(kown.at[:, pl.ds(0, 7)], s_z.at[0])
        sent(kown.at[0], s_z.at[1])
        sent(kown.at[pl.ds(0, 3), 0], s_a.at[0])

    @pl.when(core == 0)
    def _():
        g_q.drain()
        g_w0.drain()
        sent(kown.at[pl.ds(0, 3)], s_a.at[0])
        sent(wo.at[pl.ds(0, 3), 0, 0, 0], s_wo.at[2])
        sent(ql, s_q.at[1])
        sent(ql.at[pl.ds(0, 3)], s_q.at[0])


def on_device(n, ntp, tokens, doc_ids, down_q, down_k, down_r, gain_q, gain_k, up_q, up_k, up_v, out_w, gain_o):
    own, width = tokens.shape
    block = doc_ids.shape[0]
    heads = up_k.shape[1] // NOPE
    rank = down_k.shape[1]
    nq, nk, nv = up_q.shape[1], up_k.shape[1], up_v.shape[1]
    turn_in, turn_block, pick, pick_key, mix = tables(n, block, heads)
    vmem = pl.BlockSpec(memory_space=pltpu.VMEM)
    hbm = pl.BlockSpec(memory_space=pl.ANY)
    dma = lambda k: pltpu.SemaphoreType.DMA((k,))
    v = lambda *shape, dtype=BF16: pltpu.VMEM(shape, dtype)
    rows = heads * block
    scratch = [
        pltpu.VMEM((1, block), jnp.int32), v(1, rank, dtype=F32), v(1, width, dtype=F32), v(1, 256, dtype=F32), v(ROPE, 256),
        v(128, 128), v(2 * own, width), v(width // n, ROPE), v(width, 128),
        v(2, own, width), v(NZ, NX, width // n, rank), v(NZ, NX, width // n // 4, 128, dtype=F32),
        v(NY, NZ, NX, rank // n, nq), v(NY, NZ, NX, rank // n, nk + nv), v(NY, 2, NZ, NX, width // n, nv),
        v(NY, rank, nq), v(NY, rank, nk + nv), v(NY, 2 * own, rank),
        v(NX, NZ, 5, own // 2, 128), v(NX, NZ, 5, own // 2, 128), v(5, own // 2, 128),
        v(block, 256, dtype=F32), v(block, 128, dtype=F32), v(block, 128, dtype=F32), v(*pick.shape),
        v(NY, 2, rows, 256),
        v(2, 2, rows, 256, dtype=F32), v(2, 2, 256, nk), v(3, 512, nv),
        v(2, rows, 128, dtype=F32), v(2, rows, 128, dtype=F32), v(2, rows, 128, dtype=F32),
        v(NY, block, nv), v(2, NY * NY, own, nv), v(2, NY * NY, heads, block, dtype=F32),
        pltpu.SemaphoreType.REGULAR,
        dma(15), dma(1), dma(1), dma(2), dma(8), dma(2), dma(8), dma(3), dma(5), dma(3), dma(5), dma(4), dma(6),
        dma(2), dma(1), dma(1), dma(7), dma(2), dma(3), dma(1), dma(2), dma(2), dma(2),
    ]
    mixed, log_sums = pl.pallas_call(
        functools.partial(kernel, n, ntp, heads),
        out_shape=(
            jax.ShapeDtypeStruct((own, width), BF16),
            jax.ShapeDtypeStruct((heads, block), F32),
        ),
        in_specs=[hbm] * 17,
        out_specs=(vmem, vmem),
        scratch_shapes=scratch,
        compiler_params=pltpu.CompilerParams(
            collective_id=0, has_side_effects=True, vmem_limit_bytes=60 * 1024 * 1024
        ),
    )(
        tokens, doc_ids[None, :], down_q, down_k, down_r, gain_q[None, :], gain_k[None, :],
        up_q, up_k, up_v, out_w.T, gain_o[None, :],
        jnp.asarray(turn_in), jnp.asarray(turn_block[:, None, :]), jnp.asarray(pick, BF16), jnp.asarray(pick_key, BF16), jnp.asarray(mix, BF16),
    )
    return mixed, log_sums.T


def solution(mesh):
    assert mesh.shape["tp"] == 2 * NY and mesh.shape["sp"] == NX * NZ
    placed = (
        P(("sp", "tp"), None), P("sp"), P("sp", None), P("sp", None), P("sp", None), P(), P(),
        P("sp", "tp"), P("sp", "tp"), P("sp", "tp"), P("tp", "sp"), P(),
    )
    return jax.shard_map(
        functools.partial(on_device, mesh.shape["sp"], mesh.shape["tp"]),
        mesh=mesh,
        in_specs=placed,
        out_specs=(P(("sp", "tp"), None), P("sp", "tp")),
        check_vma=False,
    )
```

```python
import functools
import math

import jax
import jax.numpy as jnp
import numpy as np
from jax import lax
from jax.experimental import pallas as pl
from jax.experimental.pallas import tpu as pltpu
from jax.sharding import PartitionSpec as P

NOPE = 64
ROPE = 32
VDIM = 64
THETA = 10000.0
EPS = 1e-06
MASKED = -1e30
MESH = pl.DeviceIdType.MESH
F32 = jnp.float32
BF16 = jnp.bfloat16
NX, NY, NZ = 4, 4, 8
NEAR = (0, 1, 7, 2, 6, 3, 5, 4)
ZPOS = {rel: pos for pos, rel in enumerate(NEAR)}


def dot(a, b):
    return jnp.dot(a, b, preferred_element_type=F32)


def dot_t(a, b):
    return lax.dot_general(a, b, (((1,), (1,)), ((), ())), preferred_element_type=F32)


def rms(values, gain):
    wide = values.astype(F32)
    scale = lax.rsqrt(jnp.mean(wide * wide, axis=-1, keepdims=True) + EPS)
    return (wide * scale * gain).astype(BF16)


def tables(n, block, heads):
    half = ROPE // 2
    inverse = np.float32(THETA) ** (-np.arange(half, dtype=np.float32) / np.float32(half))
    inverse = inverse.astype(np.float32).astype(np.float64)[None, :]

    def turn(positions):
        angles = positions.astype(np.float64)[:, None] * inverse
        both = np.zeros((len(positions), 256), np.float32)
        both[:, :ROPE] = np.tile(np.cos(angles), (1, 2))
        both[:, 128 : 128 + ROPE] = np.tile(np.sin(angles), (1, 2))
        return both

    width = NOPE + ROPE
    pick = np.zeros((heads * width, heads * 384), np.float32)
    eye = np.arange(NOPE)
    rot = np.arange(ROPE)
    low = np.arange(half)
    for head in range(heads):
        pick[head * width + eye, head * 384 + (head % 2) * NOPE + eye] = 1
        pick[head * width + NOPE + rot, head * 384 + 128 + rot] = 1
        pick[head * width + NOPE + half + low, head * 384 + 256 + low] = -1
        pick[head * width + NOPE + low, head * 384 + 256 + half + low] = 1
    pick_key = np.zeros((ROPE, 256), np.float32)
    pick_key[rot, rot] = 1
    pick_key[half + low, 128 + low] = -1
    pick_key[low, 128 + half + low] = 1
    mix = np.zeros((128, 128), np.float32)
    to = np.arange(128)
    mix[32 * (to // 8 % 4) + 8 * (to // 32) + to % 8, to] = 1
    return turn(np.arange(block)), turn(np.arange(n) * block), pick, pick_key, mix


def kernel(
    n, ntp, heads,
    tokens, docs_in, down_q, down_k, down_r, gain_q, gain_k, up_q, up_k, up_v, out_wt, gain_o,
    turn_in, turn_block, pick, pick_key, mix,
    out, log_out,
    docs, gain, gain_out, turn_me, sel_key, mix_in, tok_mix, wr_in, wr_flat,
    tok, w, wr, uq, up, wo, uq_flat, up_flat, ql, kown, koth, ks, tab, kdoc, qdoc, sel, qs,
    sbuf, kbuf, vbuf, top_s, sum_s, acc_s, osend, oget, lget,
    go, loc, s_tok, r_tok, s_w, r_w, s_wr, r_wr, s_uq, r_uq, s_up, r_up, s_wo, r_wo,
    s_q, r_q, s_a, r_a, s_z, r_z, s_d, r_d, s_f, r_f,
):
    me = lax.axis_index("sp")
    t = lax.axis_index("tp")
    z, x = me // NX, lax.rem(me, NX)
    y, core = t // 2, lax.rem(t, 2)
    own, width = tokens.shape
    block = ntp * own
    rows_all = heads * block

    def wrap(v, size):
        return lax.rem(v + size, size)

    def dev(dz=0, dx=0, dy=0, c=None):
        c = core if c is None else c
        zz = wrap(z + dz, NZ) if dz else z
        xx = wrap(x + dx, NX) if dx else x
        yy = wrap(y + dy, NY) if dy else y
        return (zz * NX + xx, yy * 2 + c)

    c_dev = dev(c=1 - core)

    def rc(src, dst, s, r, device):
        return pltpu.make_async_remote_copy(
            src_ref=src, dst_ref=dst, send_sem=s, recv_sem=r, device_id=device, device_id_type=MESH
        )

    def sent(ref, s):
        rc(ref, ref, s, s, c_dev).wait_send()

    def got(ref, r):
        rc(ref, ref, r, r, c_dev).wait_recv()

    barrier = pltpu.get_barrier_semaphore()
    others = [dev(dz=d) for d in range(1, NZ)] + [dev(dx=d) for d in range(1, NX)]
    others += [dev(dz=d, c=1 - core) for d in range(1, NZ)]
    others += [dev(dy=d) for d in range(1, NY)] + [dev(dy=d, c=1 - core) for d in range(NY)]
    for device in others:
        pl.semaphore_signal(barrier, inc=1, device_id=device, device_id_type=MESH)

    @pl.when(core == 1)
    def _():
        pltpu.make_async_copy(down_k, w.at[z, x], loc.at[1]).start()
        pltpu.make_async_copy(gain_k, gain, loc.at[9]).start()

    @pl.when(core == 0)
    def _():
        pltpu.make_async_copy(down_q, w.at[z, x], loc.at[1]).start()
        pltpu.make_async_copy(gain_q, gain, loc.at[9]).start()

    nq, nk = up_q.shape[1], up_k.shape[1]
    c_w = pltpu.make_async_copy(down_k, w.at[z, x], loc.at[1])
    c_gain = pltpu.make_async_copy(gain_k, gain, loc.at[9])
    c_docs = pltpu.make_async_copy(docs_in, docs, loc.at[10])
    c_tab = pltpu.make_async_copy(turn_in, tab, loc.at[7])
    c_me = pltpu.make_async_copy(turn_block.at[me], turn_me, loc.at[11])
    c_tok = pltpu.make_async_copy(tokens, tok.at[core], loc.at[0])
    c_wr = pltpu.make_async_copy(down_r, wr_in, loc.at[2])
    c_mix = pltpu.make_async_copy(mix, mix_in, loc.at[14])
    c_uq = pltpu.make_async_copy(up_q, uq.at[0, z, x], loc.at[3])
    c_up = [
        pltpu.make_async_copy(up_k, up.at[0, z, x, :, pl.ds(0, nk)], loc.at[4]),
        pltpu.make_async_copy(up_v, up.at[0, z, x, :, pl.ds(nk, nk)], loc.at[5]),
    ]
    c_wo = pltpu.make_async_copy(out_wt, wo.at[y, core, z, x], loc.at[6])
    c_sel = pltpu.make_async_copy(pick, sel, loc.at[8])
    c_key = pltpu.make_async_copy(pick_key, sel_key, loc.at[12])
    c_out = pltpu.make_async_copy(gain_o, gain_out, loc.at[13])
    for copy in [c_docs, c_tab, c_me, c_wr, c_tok, c_uq] + c_up + [c_key, c_mix, c_wo, c_sel, c_out]:
        copy.start()

    down = lax.broadcasted_iota(jnp.int32, (block, block), 0)
    across = lax.broadcasted_iota(jnp.int32, (block, block), 1)
    c_docs.wait()
    doc_row = jnp.broadcast_to(docs[...].astype(F32), (block, block))
    doc_col = jnp.sum(jnp.where(down == across, doc_row, 0.0), axis=-1, keepdims=True)
    lane = lax.broadcasted_iota(jnp.int32, (block, 128), 1)
    in_docs = (lane >= ROPE) & (lane < ROPE + n)
    same = doc_col == (lane - ROPE).astype(F32)
    kdoc[...] = jnp.where(in_docs & same, 1.0, 0.0)
    qdoc[...] = jnp.where(in_docs & jnp.logical_not(same), MASKED, 0.0)
    c_tab.wait()
    c_me.wait()
    cos_a, sin_a = turn_me[:, :128], turn_me[:, 128:]
    cos_b, sin_b = tab[:, :128], tab[:, 128:]
    tab[:, :128] = cos_a * cos_b - sin_a * sin_b
    tab[:, 128:] = sin_a * cos_b + cos_a * sin_b

    rank = uq_flat.shape[1]
    c_wr.wait()
    wide_r = wr_in[...].astype(F32)
    wr[z, x] = jnp.concatenate([wide_r[8 * q : 8 * q + 8] for q in range(4)], axis=1)
    for copy in [c_w, c_tok, c_uq] + c_up + [c_key, c_mix, c_gain, c_wo]:
        copy.wait()
    pl.semaphore_wait(barrier, len(others))

    class Gather:
        def __init__(self, at, s, r):
            self.at, self.s, self.r = at, s, r

        def start_z(self):
            here = self.at(z, x)
            for d in reversed(NEAR[1:]):
                rc(here, here, self.s.at[0], self.r.at[0], dev(dz=d)).start()

        def start_x(self):
            got(self.at(pl.ds(0, NZ - 1), x), self.r.at[0])
            column = self.at(slice(None), x)
            for k in (2, 1, -1):
                rc(column, column, self.s.at[1], self.r.at[1], dev(dx=k)).start()

        def finish(self):
            got(self.at(pl.ds(0, NZ - 2), slice(None)), self.r.at[1])

        def drain(self):
            sent(self.at(pl.ds(0, NZ - 1), 0), self.s.at[0])
            sent(self.at(pl.ds(0, NZ - 2), slice(None)), self.s.at[1])

    class Pieces(Gather):
        def start_z(self):
            here = self.at(z, x)
            for d in reversed(NEAR[1:]):
                rc(here, here, self.s.at[0], self.r.at[d], dev(dz=d)).start()

        def pass_x(self, d):
            here = self.at(wrap(z - d, NZ), x)
            if d > 0:
                got(here, self.r.at[d])
            for k in (2, 1, -1):
                rc(here, here, self.s.at[1], self.r.at[0], dev(dx=k)).start()

        def finish(self):
            got(self.at(pl.ds(0, NZ - 2), slice(None)), self.r.at[0])

    g_k = Pieces(lambda i, j: w.at[i, j], s_w, r_w)
    g_wr = Pieces(lambda i, j: wr.at[i, j], s_wr, r_wr)
    g_q = Gather(lambda i, j: w.at[i, j], s_w, r_w)
    g_uq = Gather(lambda i, j: uq.at[0, i, j], s_uq, r_uq)
    g_up = Gather(lambda i, j: up.at[0, i, j], s_up, r_up)
    g_w0 = Gather(lambda i, j: wo.at[:, 0, i, j], s_wo, r_wo)
    g_w1 = Gather(lambda i, j: wo.at[y, 1, i, j], s_wo, r_wo)

    def wo_y():
        here = wo.at[y, 0, z, x]
        for k in (2, 1, 3):
            rc(here, here, s_wo.at[2], r_wo.at[2], dev(dy=k)).start()

    def wo_z():
        got(wo.at[pl.ds(0, 3), 0, z, x], r_wo.at[2])
        g_w0.start_z()

    def wo_last():
        @pl.when(core == 0)
        def _():
            got(wo.at[:, 0, pl.ds(0, NZ - 1), x], r_wo.at[0])
            here = wo.at[:, 0, :, x]
            rc(here, here, s_wo.at[1], r_wo.at[4], dev(dx=1)).start()
            rc(here, here, s_wo.at[1], r_wo.at[5], dev(dx=-1)).start()
            rc(here, here, s_wo.at[3], r_wo.at[3], c_dev).start()

        @pl.when(core == 1)
        def _():
            g_w1.finish()
            here = wo.at[y, 1]
            rc(here, here, s_wo.at[2], r_wo.at[4], dev(dy=1)).start()
            rc(here, here, s_wo.at[2], r_wo.at[5], dev(dy=-1)).start()
            rc(here, here, s_wo.at[3], r_wo.at[3], c_dev).start()

    def wo_far():
        low, high = pl.ds(0, NZ // 2), pl.ds(NZ // 2, NZ // 2)

        @pl.when(core == 0)
        def _():
            for d, cut, sem in ((-1, low, 4), (1, high, 5)):
                whole = wo.at[:, 0, :, wrap(x + d, NX)]
                part = wo.at[:, 0, cut, wrap(x + d, NX)]
                got(whole, r_wo.at[sem])
                rc(part, part, s_wo.at[1], r_wo.at[1], dev(dx=-d)).start()
                rc(whole, whole, s_wo.at[3], r_wo.at[3], c_dev).start()

        @pl.when(core == 1)
        def _():
            for d, cut, sem in ((-1, low, 4), (1, high, 5)):
                whole = wo.at[wrap(y + d, NY), 1]
                part = wo.at[wrap(y + d, NY), 1, cut]
                got(whole, r_wo.at[sem])
                rc(part, part, s_wo.at[2], r_wo.at[2], dev(dy=-d)).start()
                rc(whole, whole, s_wo.at[3], r_wo.at[3], c_dev).start()

    def wo_cross():
        @pl.when(core == 0)
        def _():
            here = wo.at[:, 0, :, wrap(x + 2, NX)]
            got(here, r_wo.at[1])
            rc(here, here, s_wo.at[3], r_wo.at[3], c_dev).start()

        @pl.when(core == 1)
        def _():
            here = wo.at[wrap(y + 2, NY), 1]
            got(here, r_wo.at[2])
            rc(here, here, s_wo.at[3], r_wo.at[3], c_dev).start()

    def heads_y(g, ref, s, r):
        g.finish()
        for k in (1, 3):
            rel = -k % NY
            rc(ref.at[0], ref.at[rel], s.at[2], r.at[1 + rel], dev(dy=k)).start()

    def heads_far(rel):
        got(up.at[rel], r_up.at[1 + rel])
        got(uq.at[rel], r_uq.at[1 + rel])
        if rel != 2:
            cut = pl.ds(0 if rel == 3 else NZ // 2, NZ // 2)
            device = dev(dy=1 if rel == 3 else -1)
            rc(up.at[rel, cut], up.at[2, cut], s_up.at[2], r_up.at[3], device).start()
            rc(uq.at[rel, cut], uq.at[2, cut], s_uq.at[2], r_uq.at[3], device).start()

    def heads_in(rel):
        for j in range(n):
            up_flat[rel, j * 8 : (j + 1) * 8, :] = up[rel, j // NX, j % NX]
            uq_flat[rel, j * 8 : (j + 1) * 8, :] = uq[rel, j // NX, j % NX]

    here = tok.at[core]
    c_partner = rc(here, here, s_tok.at[0], r_tok.at[0], c_dev)

    @pl.when(core == 1)
    def _():
        g_k.start_z()
        g_wr.start_z()
        g_k.pass_x(0)
        g_wr.pass_x(0)
        c_partner.start()
        g_up.start_z()
        g_uq.start_z()
        for d in NEAR[1:]:
            g_k.pass_x(d)
            g_wr.pass_x(d)
            if d == 1:
                pl.semaphore_signal(go, inc=1, device_id=c_dev, device_id_type=MESH)
        g_w1.start_z()
        g_up.start_x()
        g_uq.start_x()
        got(tok.at[1 - core], r_tok.at[0])
        both_tokens = tok[...].reshape(2 * own, width)
        for j in range(width // 128):
            cut = slice(j * 128, (j + 1) * 128)
            tok_mix[:, cut] = dot(both_tokens[:, cut], mix_in[...]).astype(BF16)
        g_wr.finish()
        packed = wr[...].reshape(rank, 128)
        for q in range(4):
            turned = (pltpu.roll(packed, 128 - 32 * q, 1) if q else packed).astype(BF16)
            for j in range(width // 128):
                wr_flat[j * 128 + q * 32 : j * 128 + (q + 1) * 32, :] = turned[j * 32 : (j + 1) * 32]
        g_k.finish()

    @pl.when(core == 0)
    def _():
        c_partner.start()
        wo_y()
        g_up.start_z()
        g_uq.start_z()
        pl.semaphore_wait(go, 1)
        g_q.start_z()
        g_q.start_x()
        g_up.start_x()
        g_uq.start_x()
        wo_z()

    def project():
        raw = dot(tok[...].reshape(2 * own, width), w[...].reshape(width, w.shape[-1])).astype(BF16)
        return rms(raw, gain[...])

    @pl.when(core == 1)
    def _():
        lat = project()
        rotary = dot(tok_mix[...], wr_flat[...])[:, :ROPE].astype(BF16)
        both = dot(rotary, sel_key[...])
        rows = pl.ds(pl.multiple_of(y * (2 * own), 2 * own), 2 * own)
        turned = both[:, :128] * tab[rows, :128] + both[:, 128:] * tab[rows, 128:] + kdoc[rows, :]
        half = own // 2
        for stripe in range(2):
            first = stripe * own
            parts = [
                lat[first + s * half : first + (s + 1) * half, h * 128 : (h + 1) * 128]
                for s in range(2)
                for h in range(2)
            ]
            packed = turned[first : first + half] + pltpu.roll(turned[first + half : first + own], 64, 1)
            parts.append(packed.astype(BF16))
            for i, tile in enumerate(parts):
                if stripe == 1:
                    kown[0, 0, i] = tile
                else:
                    ks[i] = tile
        here = kown.at[0, 0]
        rc(ks, here, s_z.at[1], r_z.at[2], dev(c=0)).start()
        for k in (2, 1, 3):
            rc(here, kown.at[-k % NX, 0], s_a.at[0], r_a.at[0], dev(dx=k)).start()
        for d in (4, 1, 7, 6, 2, 3, 5):
            pos = ZPOS[-d % NZ]
            rc(ks, kown.at[0, pos], s_z.at[1], r_z.at[0 if pos < 4 else 1], dev(dz=d, c=0)).start()

    parts = ((0, 1), (1, 3), (4, 4))

    def a_send(p):
        first, length = parts[p]
        src = kown.at[0, pl.ds(first, length)]
        for k in (2, 1, 3):
            rel = -k % NX
            sem = r_a.at[0] if p == 0 else r_a.at[3 * p - 3 + rel]
            rc(src, kown.at[rel, pl.ds(first, length)], s_a.at[0], sem, dev(dx=k)).start()

    def cross(a, count, p):
        cut = pl.ds(*parts[p])
        src, dst = kown.at[pl.ds(a, count), cut], koth.at[pl.ds(a, count), cut]
        rc(src, dst, s_d.at[0], r_d.at[1 if p == 2 else 0], c_dev).start()

    def z_part(p):
        if p == 0:
            got(kown.at[0, 0], r_z.at[2])
        else:
            got(kown.at[0, pl.ds(*parts[p])], r_z.at[p - 1])
        a_send(p)
        cross(0, 1, p)

    def a_part(p):
        if p == 0:
            got(kown.at[pl.ds(1, 3), 0], r_a.at[0])
            cross(1, 3, 0)
        else:
            for rel in (1, 3, 2):
                got(kown.at[rel, pl.ds(*parts[p])], r_a.at[3 * p - 3 + rel])
                cross(rel, 1, p)

    def rows_of(h):
        cut = pl.ds(1, 3) if h == 0 else pl.ds(4, 4)
        got(kown.at[:, cut], r_z.at[h])
        cut = pl.ds(4 * h, 4)
        rc(kown.at[:, cut], koth.at[:, cut], s_d.at[0], r_d.at[h], c_dev).start()

    @pl.when(core == 0)
    def _():
        z_part(0)
        got(tok.at[1 - core], r_tok.at[0])
        z_part(1)
        g_q.finish()
        ql[y] = project()
        here = ql.at[y]
        for k in (2, 1, 3):
            for c in range(2):
                rc(here, here, s_q.at[c], r_q.at[0], dev(dy=k, c=c)).start()
        rc(here, here, s_q.at[1], r_q.at[0], dev(c=1)).start()
        z_part(2)
        heads_y(g_up, up, s_up, r_up)
        heads_y(g_uq, uq, s_uq, r_uq)
        a_part(0)

    @pl.when(core == 1)
    def _():
        heads_y(g_up, up, s_up, r_up)
        heads_y(g_uq, uq, s_uq, r_uq)
        got(kown.at[pl.ds(1, 3), 0], r_a.at[0])
        for d in (1, 7, 6, 4, 3, 5, 2):
            pos = ZPOS[-d % NZ]
            rc(kown.at[:, 0], kown.at[:, pos], s_z.at[0], r_z.at[0 if pos < 4 else 1], dev(dz=d)).start()
        g_w1.start_x()

    heads_in(0)

    @pl.when(core == 0)
    def _():
        a_part(1)

    @pl.when(core == 1)
    def _():
        rows_of(0)

    @pl.when(core == 1)
    def _():
        got(ql, r_q.at[0])

    @pl.when(core == 0)
    def _():
        got(ql.at[pl.ds(0, 3)], r_q.at[0])

    c_sel.wait()
    scale = 1.0 / math.sqrt(NOPE + ROPE)
    factor = scale * math.log2(math.e)

    def queries_of(rel):
        projected = dot(ql[...].reshape(block, ql.shape[-1]), uq_flat[rel]).astype(BF16)
        for head in range(heads):
            laid = dot(projected, sel[:, head * 384 : (head + 1) * 384])
            turned = (laid[:, 128:256] * tab[:, :128] + laid[:, 256:] * tab[:, 128:]) * factor + qdoc[...]
            plain = (laid[:, :128] * factor).astype(BF16)
            rows = pl.ds(head * block, block)
            qs[rel, 0, rows, :128] = plain
            qs[rel, 1, rows, :128] = plain
            qs[rel, 0, rows, 128:] = turned.astype(BF16)
            qs[rel, 1, rows, 128:] = pltpu.roll(turned, 64, 1).astype(BF16)

    def tiles(ref, h, i):
        return ref[:, 4 * h : 4 * h + 4, i].reshape(256, 128)

    def expand(j):
        ref, h, rel = groups[j]
        for s in range(2):
            lat = jnp.concatenate([tiles(ref, h, 2 * s), tiles(ref, h, 2 * s + 1)], axis=1)
            kv = dot(lat, up_flat[rel]).astype(BF16)
            kbuf[j % 2, s] = kv[:, :nk]
            vbuf[j % 3, s * 256 : (s + 1) * 256, :] = kv[:, nk:]

    def score(j):
        ref, h, rel = groups[j]
        rot = tiles(ref, h, 4)
        for s in range(2):
            sbuf[j % 2, s] = dot_t(qs[rel, s], jnp.concatenate([kbuf[j % 2, s], rot], axis=1))

    step = 128

    def weigh(j):
        par, first, pair = j % 2, j % 4 == 0, j // 4 % 2
        for r in range(0, rows_all, step):
            rows = pl.ds(r, step)
            parts = [sbuf[par, s, rows, h * 128 : (h + 1) * 128] for s in range(2) for h in range(2)]
            most = jnp.maximum(jnp.maximum(parts[0], parts[1]), jnp.maximum(parts[2], parts[3]))
            most = jnp.max(most, axis=-1, keepdims=True)
            if first:
                new = jnp.broadcast_to(most, (step, 128))
            else:
                old = top_s[pair, rows, :]
                new = jnp.maximum(old, most)
                alpha = jnp.exp2(old - new)
            weights = [jnp.exp2(p - new) for p in parts]
            total = (weights[0] + weights[1]) + (weights[2] + weights[3])
            mixed = dot(jnp.concatenate([p.astype(BF16) for p in weights], axis=1), vbuf[j % 3])
            top_s[pair, rows, :] = new
            if first:
                sum_s[pair, rows, :] = total
                acc_s[pair, rows, :] = mixed
            else:
                sum_s[pair, rows, :] = sum_s[pair, rows, :] * alpha + total
                acc_s[pair, rows, :] = acc_s[pair, rows, :] * alpha + mixed

    head_lane = lax.broadcasted_iota(jnp.int32, (block, nk), 1) // VDIM

    def close(i, rel):
        pair = i % 2
        outs, sums = [], []
        for head in range(heads):
            rows = pl.ds(head * block, block)
            weight_sum = jnp.sum(sum_s[pair, rows, :], axis=-1, keepdims=True)
            outs.append(acc_s[pair, rows, :] / weight_sum)
            log_sum = jnp.broadcast_to(top_s[pair, rows, :1] + jnp.log2(weight_sum), (block, block))
            sums.append(jnp.sum(jnp.where(down == across, log_sum, 0.0), axis=0, keepdims=True))
        osend[i] = jnp.where(head_lane == 0, outs[0], outs[1]).astype(BF16)
        slot = y * NY + wrap(y + rel, NY)
        lget[core, slot] = jnp.concatenate(sums, axis=0)
        oget[core, slot] = osend[i, pl.ds(pl.multiple_of(t * own, own), own), :]
        for k in (2, 1, 3, 0):
            for c in range(2):
                def go_to(c=c, k=k):
                    device = dev(dy=k, c=c)
                    rows = pl.ds(pl.multiple_of(device[1] * own, own), own)
                    rc(osend.at[i, rows], oget.at[core, slot], s_f.at[0], r_f.at[0], device).start()
                    rc(lget.at[core, slot], lget.at[core, slot], s_f.at[1], r_f.at[1], device).start()
                if k:
                    go_to()
                else:
                    pl.when(core != c)(go_to)

    order = (0, 1, 3, 2)
    groups = [(ref, h, rel) for rel in order for ref, h in ((kown, 0), (koth, 0), (kown, 1), (koth, 1))]
    def second_half():
        pl.when(core == 0)(lambda: a_part(2))
        pl.when(core == 1)(lambda: rows_of(1))

    events = {
        0: [lambda: queries_of(0)],
        2: [second_half, lambda: heads_far(1), lambda: heads_far(3)],
        3: [lambda: heads_in(1), wo_last],
        7: [lambda: heads_in(3)],
        11: [lambda: heads_far(2), lambda: heads_in(2)],
        14: [wo_far],
    }
    for j, (ref, h, rel) in enumerate(groups):
        for event in events.get(j, ()):
            event()
        if j == 1 or j == 3:
            got(koth.at[:, pl.ds(4 * h, 4)], r_d.at[h])
        expand(j)
        if j % 4 == 3 and j < 15:
            queries_of(groups[j + 1][2])
        if j >= 1:
            score(j - 1)
        if j >= 2:
            weigh(j - 2)
            if (j - 2) % 4 == 3:
                close((j - 2) // 4, groups[j - 2][2])
    last = len(groups) - 1
    score(last)
    weigh(last - 1)
    weigh(last)
    close(last // 4, groups[last][2])
    wo_cross()

    c_out.wait()
    got(lget.at[:, pl.ds(0, 14)], r_f.at[1])
    got(oget.at[:, pl.ds(0, 14)], r_f.at[0])
    spot = lax.broadcasted_iota(jnp.int32, (own, block), 0) + t * own
    spot = spot == lax.broadcasted_iota(jnp.int32, (own, block), 1)
    own_lane = lax.broadcasted_iota(jnp.int32, (own, nk), 1) // VDIM

    def column(row):
        return jnp.sum(jnp.where(spot, jnp.broadcast_to(row, (own, block)), 0.0), axis=-1, keepdims=True)

    got(wo.at[:, 0], r_wo.at[3])
    mixed = jnp.zeros((own, width), F32)
    for p in range(NY):
        merged = []
        for c in range(2):
            logs = [lget[c, q * NY + p] for q in range(NY)]
            most = jnp.maximum(jnp.maximum(logs[0], logs[1]), jnp.maximum(logs[2], logs[3]))
            shares = [jnp.exp2(log - most) for log in logs]
            whole = (shares[0] + shares[1]) + (shares[2] + shares[3])
            total = jnp.zeros((own, nk), F32)
            for q in range(NY):
                share = shares[q] / whole
                both = jnp.where(own_lane == 0, column(share[:1]), column(share[1:]))
                total = total + both * oget[c, q * NY + p].astype(F32)
            merged.append(total.astype(BF16))
        weights = jnp.concatenate([wo[p, c].reshape(width, nk) for c in range(2)], axis=1)
        mixed = mixed + dot_t(jnp.concatenate(merged, axis=1), weights)
    out[...] = rms(mixed.astype(BF16), gain_out[...])
    logs = [lget[core, q * NY + y] for q in range(NY)]
    most = jnp.maximum(jnp.maximum(logs[0], logs[1]), jnp.maximum(logs[2], logs[3]))
    shares = [jnp.exp2(log - most) for log in logs]
    whole = (shares[0] + shares[1]) + (shares[2] + shares[3])
    log_out[...] = most * math.log(2.0) + jnp.log(whole)

    for gather in (g_up, g_uq):
        gather.drain()
    sent(up.at[pl.ds(0, 3)], s_up.at[2])
    sent(uq.at[pl.ds(0, 3)], s_uq.at[2])
    sent(wo.at[:, 0], s_wo.at[3])
    sent(tok.at[core], s_tok.at[0])
    sent(kown, s_d.at[0])
    sent(oget.at[:, pl.ds(0, 14)], s_f.at[0])
    sent(lget.at[:, pl.ds(0, 14)], s_f.at[1])

    @pl.when(core == 1)
    def _():
        g_k.drain()
        g_wr.drain()
        g_w1.drain()
        sent(wo.at[pl.ds(0, 3), 1], s_wo.at[2])
        sent(kown.at[:, pl.ds(0, 7)], s_z.at[0])
        sent(kown.at[0], s_z.at[1])
        sent(kown.at[pl.ds(0, 3), 0], s_a.at[0])

    @pl.when(core == 0)
    def _():
        g_q.drain()
        g_w0.drain()
        sent(kown.at[pl.ds(0, 3)], s_a.at[0])
        sent(wo.at[pl.ds(0, 3), 0, 0, 0], s_wo.at[2])
        sent(ql, s_q.at[1])
        sent(ql.at[pl.ds(0, 3)], s_q.at[0])


def on_device(n, ntp, tokens, doc_ids, down_q, down_k, down_r, gain_q, gain_k, up_q, up_k, up_v, out_w, gain_o):
    own, width = tokens.shape
    block = doc_ids.shape[0]
    heads = up_k.shape[1] // NOPE
    rank = down_k.shape[1]
    nq, nk, nv = up_q.shape[1], up_k.shape[1], up_v.shape[1]
    turn_in, turn_block, pick, pick_key, mix = tables(n, block, heads)
    vmem = pl.BlockSpec(memory_space=pltpu.VMEM)
    hbm = pl.BlockSpec(memory_space=pl.ANY)
    dma = lambda k: pltpu.SemaphoreType.DMA((k,))
    v = lambda *shape, dtype=BF16: pltpu.VMEM(shape, dtype)
    rows = heads * block
    scratch = [
        pltpu.VMEM((1, block), jnp.int32), v(1, rank, dtype=F32), v(1, width, dtype=F32), v(1, 256, dtype=F32), v(ROPE, 256),
        v(128, 128), v(2 * own, width), v(width // n, ROPE), v(width, 128),
        v(2, own, width), v(NZ, NX, width // n, rank), v(NZ, NX, width // n // 4, 128, dtype=F32),
        v(NY, NZ, NX, rank // n, nq), v(NY, NZ, NX, rank // n, nk + nv), v(NY, 2, NZ, NX, width // n, nv),
        v(NY, rank, nq), v(NY, rank, nk + nv), v(NY, 2 * own, rank),
        v(NX, NZ, 5, own // 2, 128), v(NX, NZ, 5, own // 2, 128), v(5, own // 2, 128),
        v(block, 256, dtype=F32), v(block, 128, dtype=F32), v(block, 128, dtype=F32), v(*pick.shape),
        v(NY, 2, rows, 256),
        v(2, 2, rows, 256, dtype=F32), v(2, 2, 256, nk), v(3, 512, nv),
        v(2, rows, 128, dtype=F32), v(2, rows, 128, dtype=F32), v(2, rows, 128, dtype=F32),
        v(NY, block, nv), v(2, NY * NY, own, nv), v(2, NY * NY, heads, block, dtype=F32),
        pltpu.SemaphoreType.REGULAR,
        dma(15), dma(1), dma(1), dma(2), dma(8), dma(2), dma(8), dma(3), dma(5), dma(3), dma(5), dma(4), dma(6),
        dma(2), dma(1), dma(1), dma(7), dma(2), dma(3), dma(1), dma(2), dma(2), dma(2),
    ]
    mixed, log_sums = pl.pallas_call(
        functools.partial(kernel, n, ntp, heads),
        out_shape=(
            jax.ShapeDtypeStruct((own, width), BF16),
            jax.ShapeDtypeStruct((heads, block), F32),
        ),
        in_specs=[hbm] * 17,
        out_specs=(vmem, vmem),
        scratch_shapes=scratch,
        compiler_params=pltpu.CompilerParams(
            collective_id=0, has_side_effects=True, vmem_limit_bytes=60 * 1024 * 1024
        ),
    )(
        tokens, doc_ids[None, :], down_q, down_k, down_r, gain_q[None, :], gain_k[None, :],
        up_q, up_k, up_v, out_w.T, gain_o[None, :],
        jnp.asarray(turn_in), jnp.asarray(turn_block[:, None, :]), jnp.asarray(pick, BF16), jnp.asarray(pick_key, BF16), jnp.asarray(mix, BF16),
    )
    return mixed, log_sums.T


def solution(mesh):
    assert mesh.shape["tp"] == 2 * NY and mesh.shape["sp"] == NX * NZ
    placed = (
        P(("sp", "tp"), None), P("sp"), P("sp", None), P("sp", None), P("sp", None), P(), P(),
        P("sp", "tp"), P("sp", "tp"), P("sp", "tp"), P("tp", "sp"), P(),
    )
    return jax.shard_map(
        functools.partial(on_device, mesh.shape["sp"], mesh.shape["tp"]),
        mesh=mesh,
        in_specs=placed,
        out_specs=(P(("sp", "tp"), None), P("sp", "tp")),
        check_vma=False,
    )
```
